256 devices in a mesh: sp: 64 (over z, y, core), tp: 4 (over x).
Axes of the slice: x: 4, y: 4, z: 8, core: 2. Of those that a mesh axis runs over, the one named last changes fastest.
Arguments:
- residual: bfloat16 [8192, 2048], P(('sp', 'tp')), may hold values from -6 to 6
- query_content: bfloat16 [8192, 1024], P('sp', 'tp'), may hold values from -400 to 400
- query_rotary: bfloat16 [8192, 384], P('sp', 'tp'), may hold values from -16 to 16
- key_latent: bfloat16 [8192, 512], P('sp'), may hold values from -6 to 6
- rotary_key: bfloat16 [8192, 32], P('sp'), may hold values from -6 to 6
- latent_gain: float32 [512], replicated, may hold values from 0.1 to 1.9
- key_weight: bfloat16 [512, 1024], P(None, 'tp'), may hold values from -0.25 to 0.25
- value_weight: bfloat16 [512, 1024], P(None, 'tp'), may hold values from -0.25 to 0.25
- output_gain: float32 [1024], P('tp'), may hold values from 0.1 to 1.9
- output_weight: bfloat16 [1024, 2048], P('tp'), may hold values from -0.1875 to 0.1875
- mixer_gain: float32 [2048], replicated, may hold values from 0.1 to 1.9
- gate_weight: bfloat16 [2048, 5632], P('sp', 'tp'), may hold values from -0.125 to 0.125
- up_weight: bfloat16 [2048, 5632], P('sp', 'tp'), may hold values from -0.125 to 0.125
- down_weight: bfloat16 [5632, 2048], P('tp', 'sp'), may hold values from -0.078125 to 0.078125
Outputs:
- layer_out: bfloat16 [8192, 2048], P(('sp', 'tp'))
The draws below stay inside these ranges and needn't reach their ends.
All inputs are finite; a program needn't handle non-finite values.
Results may differ from the reference program's by a relative error of at most 0.015.
Values may be sent and summed in bfloat16 or wider, within the bound.
A program may use at most 128 MiB of HBM per device.

```python
import math
import jax
import jax.numpy as jnp
from jax import lax

D = 2048
FF = 5632
LATENT = 512
NARROW_HEADS = 8
WIDE_HEADS = 4
NARROW_DIM = 64
WIDE_DIM = 128
ROT_DIM = 32
TOKENS = 8192
CONTENT = 1024
ROTARY = 384
NARROW_DEV = 2
WIDE_DEV = 1
N_TP = 4


def draw_query_content(key, part):
    first_key = jax.random.fold_in(key, 0)
    width = NARROW_HEADS * NARROW_DIM + WIDE_HEADS * WIDE_DIM
    normal = jax.random.normal(first_key, (TOKENS, width), jnp.float32) * 2.5
    return jnp.clip(normal, -20.0, 20.0).astype(jnp.bfloat16)


def levels(stream_key, dims, shards, low, high):
    factor_of = 1.0
    for axis_at, blocks in shards:
        draws = jax.random.uniform(jax.random.fold_in(jax.random.fold_in(stream_key, 6), axis_at), (blocks,), jnp.float32, low / len(shards), high / len(shards))
        factor_of = factor_of * jnp.repeat(jnp.exp(draws), dims[axis_at] // blocks).reshape((-1,) + (1,) * (len(dims) - 1 - axis_at))
    return factor_of


def gaussian(rng, shape, deviation, most, pieces=(), kind=jnp.bfloat16):
    values = deviation * jax.random.normal(rng, shape, jnp.float32)
    if pieces:
        values = values * levels(rng, shape, pieces, -0.22, 0.18)
    return jnp.clip(values, -most, most).astype(kind)


def setup_inputs(seed: int = 0) -> dict:
    streams_of = jax.random.split(jax.random.key(seed), 15)
    residual = gaussian(streams_of[0], (TOKENS, D), 1.0, 6.0, ((0, 256),))
    query_content = draw_query_content(jax.random.fold_in(streams_of[14], 71), 0)
    query_rotary = gaussian(streams_of[2], (TOKENS, ROTARY), 2.5, 16.0, ((0, 64), (1, 4)))
    key_latent = gaussian(streams_of[3], (TOKENS, LATENT), 1.0, 6.0, ((0, 64),))
    rotary_key = gaussian(streams_of[4], (TOKENS, ROT_DIM), 1.0, 6.0, ((0, 64),))
    latent_gain = jnp.clip(1.0 + 0.18 * jax.random.normal(streams_of[5], (LATENT,), jnp.float32), 0.1, 1.9)
    key_weight = gaussian(streams_of[6], (LATENT, CONTENT), LATENT ** -0.5, 0.25, ((1, 4),))
    value_weight = gaussian(streams_of[7], (LATENT, CONTENT), LATENT ** -0.5, 0.25, ((1, 4),))
    output_gain = jnp.clip(1.0 + 0.18 * jax.random.normal(streams_of[8], (CONTENT,), jnp.float32), 0.1, 1.9)
    output_weight = gaussian(streams_of[9], (CONTENT, D), CONTENT ** -0.5, 0.1875, ((0, 4),))
    mixer_gain = jnp.clip(1.0 + 0.18 * jax.random.normal(streams_of[10], (D,), jnp.float32), 0.1, 1.9)
    gate_weight = gaussian(streams_of[11], (D, FF), D ** -0.5, 0.125, ((0, 64), (1, 4)))
    up_weight = gaussian(streams_of[12], (D, FF), D ** -0.5, 0.125, ((0, 64), (1, 4)))
    down_weight = gaussian(streams_of[13], (FF, D), FF ** -0.5, 0.078125, ((0, 4), (1, 64)))
    return {"residual": residual, "query_content": query_content, "query_rotary": query_rotary, "key_latent": key_latent, "rotary_key": rotary_key, "latent_gain": latent_gain, "key_weight": key_weight, "value_weight": value_weight, "output_gain": output_gain, "output_weight": output_weight, "mixer_gain": mixer_gain, "gate_weight": gate_weight, "up_weight": up_weight, "down_weight": down_weight}


epsilon = 1e-06
rope_base = 500000.0

def stored(values):
    return lax.optimization_barrier(values.astype(jnp.bfloat16))

def normalize(values):
    values = values.astype(jnp.float32)
    return values * lax.rsqrt(lax.optimization_barrier(jnp.mean(values * values, axis=-1, keepdims=True)) + epsilon)

def rotate(values, positions):
    half_width = values.shape[-1] // 2
    inverse = 1.0 / jnp.power(rope_base, jnp.arange(0, 2 * half_width, 2, dtype=jnp.float32) / (2 * half_width))
    angles = positions.astype(jnp.float32)[:, None] * inverse[None, :]
    table_shape = (angles.shape[0],) + (1,) * (values.ndim - 2) + (half_width,)
    cosine_table = jnp.cos(angles).reshape(table_shape)
    sine_table = jnp.sin(angles).reshape(table_shape)
    first_half = values[..., :half_width]
    second_half = values[..., half_width:]
    return jnp.concatenate([first_half * cosine_table - second_half * sine_table, second_half * cosine_table + first_half * sine_table], axis=-1)

def split_groups(whole, narrow_size, wide_size):
    row_count = whole.shape[0]
    blocks = whole.reshape(row_count, N_TP, -1)
    narrow_cols = NARROW_DEV * narrow_size
    narrow = blocks[:, :, :narrow_cols].reshape(row_count, N_TP * NARROW_DEV, narrow_size)
    wide = blocks[:, :, narrow_cols:].reshape(row_count, N_TP * WIDE_DEV, wide_size)
    return (narrow, wide)

def join_groups(narrow, wide):
    row_count = narrow.shape[0]
    return jnp.concatenate([narrow.reshape(row_count, N_TP, -1), wide.reshape(row_count, N_TP, -1)], axis=2).reshape(row_count, -1)

def attend(query_part, rotary_part, key_part, rotary_keys, value_part, factor):
    key_float = key_part.astype(jnp.float32)
    rotary_float = rotary_keys.astype(jnp.float32)
    value_float = value_part.astype(jnp.float32)
    row_count = query_part.shape[0]
    block_rows = math.gcd(512, row_count)

    def one_block(offset):
        query_block = lax.dynamic_slice_in_dim(query_part, offset, block_rows, 0).astype(jnp.float32)
        rotary_block = lax.dynamic_slice_in_dim(rotary_part, offset, block_rows, 0).astype(jnp.float32)
        scores = (jnp.einsum('qhd,khd->hqk', query_block, key_float) + jnp.einsum('qhd,kd->hqk', rotary_block, rotary_float)) * factor
        largest = lax.optimization_barrier(jnp.max(scores, axis=-1, keepdims=True))
        powers = jnp.exp(scores - largest)
        totals = lax.optimization_barrier(jnp.sum(powers, axis=-1))
        weights = stored(powers).astype(jnp.float32)
        summed = jnp.einsum('hqk,khd->qhd', weights, value_float)
        return summed / jnp.transpose(totals)[:, :, None]
    offsets = jnp.arange(0, row_count, block_rows, dtype=jnp.int32)
    result = lax.map(one_block, offsets)
    return result.reshape(row_count, result.shape[2], result.shape[3])

def reference(residual, query_content, query_rotary, key_latent, rotary_key, latent_gain, key_weight, value_weight, output_gain, output_weight, mixer_gain, gate_weight, up_weight, down_weight):
    row_count = key_latent.shape[0]
    positions = jnp.arange(row_count, dtype=jnp.int32)
    latent = stored(normalize(key_latent) * latent_gain.astype(jnp.float32))
    key_content = stored(jnp.dot(latent, key_weight, preferred_element_type=jnp.float32))
    value_rows = stored(jnp.dot(latent, value_weight, preferred_element_type=jnp.float32))
    rot_keys = stored(rotate(rotary_key.astype(jnp.float32), positions))
    turned = rotate(query_rotary.astype(jnp.float32).reshape(row_count, -1, ROT_DIM), positions)
    rot_queries = stored(turned).reshape(row_count, -1)
    query_narrow, query_wide = split_groups(query_content, NARROW_DIM, WIDE_DIM)
    rotary_narrow, rotary_wide = split_groups(rot_queries, ROT_DIM, ROT_DIM)
    key_narrow, key_wide = split_groups(key_content, NARROW_DIM, WIDE_DIM)
    value_narrow, value_wide = split_groups(value_rows, NARROW_DIM, WIDE_DIM)
    out_narrow = attend(query_narrow, rotary_narrow, key_narrow, rot_keys, value_narrow, (NARROW_DIM + ROT_DIM) ** (-0.5))
    out_wide = attend(query_wide, rotary_wide, key_wide, rot_keys, value_wide, (WIDE_DIM + ROT_DIM) ** (-0.5))
    mixed = stored(join_groups(normalize(out_narrow), normalize(out_wide)) * output_gain.astype(jnp.float32))
    projected = jnp.dot(mixed, output_weight, preferred_element_type=jnp.float32)
    middle = stored(residual.astype(jnp.float32) + projected)
    normed = stored(normalize(middle) * mixer_gain.astype(jnp.float32))
    gate_sums = jnp.dot(normed, gate_weight, preferred_element_type=jnp.float32)
    up_sums = jnp.dot(normed, up_weight, preferred_element_type=jnp.float32)
    hidden = stored(jax.nn.silu(gate_sums) * up_sums)
    block_width = FF // N_TP
    channel_out = jnp.zeros((row_count, D), jnp.float32)
    for block_index in range(N_TP):
        columns = hidden[:, block_index * block_width:(block_index + 1) * block_width]
        weight_rows = down_weight[block_index * block_width:(block_index + 1) * block_width]
        channel_out = channel_out + stored(jnp.dot(columns, weight_rows, preferred_element_type=jnp.float32)).astype(jnp.float32)
    return (middle.astype(jnp.float32) + channel_out).astype(jnp.bfloat16)
```

```python
import functools

import jax
import jax.numpy as jnp
from jax import lax
from jax.experimental import pallas as pl
from jax.experimental.pallas import tpu as pltpu
from jax.sharding import PartitionSpec as P

NY = 4
ROT_DIM = 32
EPS = 1e-06
ROPE_BASE = 500000.0
LOG2E = 1.4426950408889634
MESH = pl.DeviceIdType.MESH
F32 = jnp.float32
BF16 = jnp.bfloat16


def dot(a, b):
    return lax.dot_general(a, b, (((1,), (0,)), ((), ())), preferred_element_type=F32)


def dot_nt(a, b):
    return lax.dot_general(a, b, (((1,), (1,)), ((), ())), preferred_element_type=F32)


def hops(n):
    both = list(range(1, (n - 1) // 2 + 1))
    return both, (n // 2 if n % 2 == 0 and n > 1 else None)


def kernel(
    NZ,
    NX,
    scales,
    cos_ref,
    sin_ref,
    qc_ref,
    qr_ref,
    lat_ref,
    rk_ref,
    lgain_ref,
    kw_ref,
    vw_ref,
    ogain_ref,
    mgain_ref,
    resid_hbm,
    ow_hbm,
    gate_hbm,
    up_hbm,
    down_hbm,
    out_ref,
    w,
    kv,
    qall,
    qx,
    acc,
    mrow,
    lrow,
    osend,
    orecv,
    ssend,
    srecv,
    mixed,
    wo,
    resid,
    mid,
    normed,
    accg,
    accu,
    hid,
    part,
    rsum,
    loc_sem,
    kv_s,
    kv_r,
    kvp_s,
    kvp_r,
    q_s,
    q_r,
    o_s,
    o_r,
    st_s,
    st_r,
    mx_s,
    mx_r,
    wo_s,
    wo_r,
    wop_s,
    wop_r,
    re_s,
    re_r,
    rs_s,
    rs_r,
    w_s1,
    w_s2,
    wp_s,
    w_r1,
    w_r2,
    wp_r,
):
    sp = lax.axis_index("sp")
    x = lax.axis_index("tp")
    c = sp % 2
    y = (sp // 2) % NY
    z = sp // (2 * NY)
    T = qc_ref.shape[0]
    R = resid.shape[1]
    D = resid.shape[2]
    pend = []

    def dev(zz=None, yy=None, cc=None, xx=None):
        zz = z if zz is None else (zz + 2 * NZ) % NZ
        yy = y if yy is None else (yy + 2 * NY) % NY
        cc = c if cc is None else cc
        xx = x if xx is None else (xx + 2 * NX) % NX
        return ((zz * NY + yy) * 2 + cc, xx)

    def send(src, dst, ssem, rsem, device, keep=True):
        d = pltpu.make_async_remote_copy(
            src_ref=src, dst_ref=dst, send_sem=ssem, recv_sem=rsem, device_id=device, device_id_type=MESH
        )
        d.start()
        if keep:
            pend.append(d)

    def arrived(ref, sem):
        pltpu.make_async_copy(ref, ref, sem).wait()

    def core0(f):
        pl.when(c == 0)(f)

    def core1(f):
        pl.when(c == 1)(f)

    partner = dev(cc=1 - c)
    dirc = 1 - 2 * c
    zboth, zlast = hops(NZ)
    yboth, ylast = hops(NY)
    xboth, xlast = hops(NX)

    loc = [
        pltpu.make_async_copy(resid_hbm, resid.at[x], loc_sem.at[0]),
        pltpu.make_async_copy(ow_hbm, wo.at[x], loc_sem.at[1]),
        pltpu.make_async_copy(gate_hbm, w.at[0, z, y, c], loc_sem.at[2]),
        pltpu.make_async_copy(up_hbm, w.at[1, z, y, c], loc_sem.at[3]),
        pltpu.make_async_copy(down_hbm, w.at[2, z, y, c], loc_sem.at[4]),
    ]
    for d in loc:
        d.start()

    barrier = pltpu.get_barrier_semaphore()
    peers = [partner]
    peers += [dev(zz=z + 1)] + ([dev(zz=z - 1)] if NZ > 2 else [])
    peers += [dev(yy=y + k) for k in range(1, NY)]
    peers += [dev(xx=x + k) for k in range(1, NX)]
    for p in peers:
        pl.semaphore_signal(barrier, inc=1, device_id=p, device_id_type=MESH)

    lane_q = lax.broadcasted_iota(jnp.int32, (qr_ref.shape[1], 128), 1)
    row_q = lax.broadcasted_iota(jnp.int32, (qr_ref.shape[1], 128), 0)
    half = ROT_DIM // 2
    swapped_q = jnp.where(lane_q % ROT_DIM < half, lane_q + half, lane_q - half)
    qr = qr_ref[...]
    q_same = dot(qr, (row_q == lane_q).astype(BF16))
    q_swap = dot(qr, (row_q == swapped_q).astype(BF16))
    cos = cos_ref[...]
    sin = sin_ref[...]
    qall[0, :, 0:128] = qc_ref[:, 0:128]
    qall[0, :, 128:256] = (q_same * cos + q_swap * sin).astype(BF16)
    qall[0, :, 256:384] = qc_ref[:, 128:256]

    lane_k = lax.broadcasted_iota(jnp.int32, (ROT_DIM, 128), 1)
    row_k = lax.broadcasted_iota(jnp.int32, (ROT_DIM, 128), 0)
    lane_in = lane_k % ROT_DIM
    swapped_k = jnp.where(lane_in < half, lane_in + half, lane_in - half)
    rk = rk_ref[...]
    k_same = dot(rk, (row_k == lane_in).astype(BF16))
    k_swap = dot(rk, (row_k == swapped_k).astype(BF16))
    lat = lat_ref[...].astype(F32)
    lat = lat * lax.rsqrt(jnp.mean(lat * lat, axis=-1, keepdims=True) + EPS)
    lat = (lat * lgain_ref[...]).astype(BF16)
    keys = dot(lat, kw_ref[...]).astype(BF16)
    vals = jnp.transpose(dot(lat, vw_ref[...])).astype(BF16)
    kv[0, c, :, 0:128] = keys[:, 0:128]
    kv[0, c, :, 128:256] = (k_same * cos + k_swap * sin).astype(BF16)
    kv[0, c, :, 256:384] = keys[:, 128:256]
    kv[0, c, :, 384:512] = vals[0:128, :]
    kv[0, c, :, 512:640] = vals[128:256, :]

    pl.semaphore_wait(barrier, len(peers))

    def kv_copy(src_slot, dst_slot, device):
        send(kv.at[src_slot, c], kv.at[dst_slot, c], kv_s.at[dst_slot], kv_r.at[dst_slot], device)

    def kv_partner(slot):
        send(kv.at[slot, c], kv.at[slot, c], kvp_s.at[slot], kvp_r.at[slot], partner)

    def kv_send(r):
        if r in zboth:
            kv_copy(2 * r - 3 if r > 1 else 0, 2 * r - 1, dev(zz=z + 1))
            kv_copy(2 * r - 2 if r > 1 else 0, 2 * r, dev(zz=z - 1))
        elif r == zlast:
            kv_copy((2 * r - 3 + c) if r > 1 else 0, NZ - 1, dev(zz=z + dirc))

    def slots_of(n, r):
        if r == 0:
            return [0]
        return [2 * r - 1, 2 * r] if r <= (n - 1) // 2 else [n - 1]

    def offset_of(n, slot):
        if slot == 0:
            return 0
        return slot_r(n, slot) if slot % 2 == 0 else -slot_r(n, slot)

    def slot_r(n, slot):
        return (slot + 1) // 2

    def zpos(slot):
        return (z + offset_of(NZ, slot) + 2 * NZ) % NZ

    def ypos(slot):
        return (y + offset_of(NY, slot) + 2 * NY) % NY

    kv_send(1)
    kv_partner(0)
    for k in range(1, NY):
        send(qall.at[0], qall.at[NY - k], q_s.at[k], q_r.at[NY - k], dev(yy=y + k))

    for d in loc:
        d.wait()

    def wo_send(r):
        if r in xboth:
            send(wo.at[(x - r + 1 + NX) % NX, c], wo.at[(x - r + 1 + NX) % NX, c], wo_s.at[2 * r - 1], wo_r.at[2 * r - 1], dev(xx=x + 1))
            send(wo.at[(x + r - 1) % NX, c], wo.at[(x + r - 1) % NX, c], wo_s.at[2 * r], wo_r.at[2 * r], dev(xx=x - 1))
        elif r == xlast:
            p = (x - dirc * (r - 1) + 2 * NX) % NX
            send(wo.at[p, c], wo.at[p, c], wo_s.at[NX - 1], wo_r.at[NX - 1], dev(xx=x + dirc))

    def wo_wait(r):
        for slot in slots_of(NX, r):
            p = (x + offset_of(NX, slot) + 2 * NX) % NX
            arrived(wo.at[p, c], wo_r.at[slot])
            send(wo.at[p, c], wo.at[p, c], wop_s.at[slot], wop_r.at[slot], partner)

    for k in range(1, NX):
        send(resid.at[x], resid.at[x], re_s.at[k], re_r.at[NX - k], dev(xx=x + k))
    if NX > 1:
        wo_send(1)

    def zdir(m):
        return dirc * (1 - 2 * (m % 2))

    def ring_y(m, zz, cc, r, ssem, rsems):
        if r in yboth:
            a, b = (y - r + 1 + NY) % NY, (y + r - 1) % NY
            send(w.at[m, zz, a, cc], w.at[m, zz, a, cc], ssem, rsems(2 * r - 1), dev(yy=y + 1), False)
            send(w.at[m, zz, b, cc], w.at[m, zz, b, cc], ssem, rsems(2 * r), dev(yy=y - 1), False)
        elif r == ylast:
            p = (y - zdir(m) * (r - 1) + 2 * NY) % NY
            send(w.at[m, zz, p, cc], w.at[m, zz, p, cc], ssem, rsems(NY - 1), dev(yy=y + zdir(m)), False)

    def ring_z(m, view, r, ssem, rsems):
        if r in zboth:
            a, b = (z - r + 1 + NZ) % NZ, (z + r - 1) % NZ
            send(view(a), view(a), ssem, rsems(2 * r - 1), dev(zz=z + 1), False)
            send(view(b), view(b), ssem, rsems(2 * r), dev(zz=z - 1), False)
        elif r == zlast:
            p = (z - zdir(m) * (r - 1) + 2 * NZ) % NZ
            send(view(p), view(p), ssem, rsems(NZ - 1), dev(zz=z + zdir(m)), False)

    def a1_send(m, r):
        ring_y(m, z, 0, r, w_s1.at[m], lambda s: w_r1.at[m, s])

    def a1_wait(m, r):
        for slot in slots_of(NY, r):
            arrived(w.at[m, z, ypos(slot), 0], w_r1.at[m, slot])

    def a_block(m, zz):
        return w.at[m, zz, :, 0]

    def a2_send(m, r):
        ring_z(m, lambda p: a_block(m, p), r, w_s2.at[m], lambda s: w_r2.at[m, s, 0])

    def a_partner(m, slot):
        p = zpos(slot)
        send(a_block(m, p), a_block(m, p), wp_s.at[m], wp_r.at[m, slot], partner, False)

    def a2_wait(m, r):
        for slot in slots_of(NZ, r):
            arrived(a_block(m, zpos(slot)), w_r2.at[m, slot, 0])

    def b1_send(m, r):
        ring_z(m, lambda p: w.at[m, p, y, 1], r, w_s1.at[m], lambda s: w_r1.at[m, s])

    def b1_wait(m, r):
        for slot in slots_of(NZ, r):
            arrived(w.at[m, zpos(slot), y, 1], w_r1.at[m, slot])

    def b2_send(m, slot, r):
        ring_y(m, zpos(slot), 1, r, w_s2.at[m], lambda s: w_r2.at[m, slot, s])

    def b_partner(m, slot, yslot):
        p = w.at[m, zpos(slot), ypos(yslot), 1]
        send(p, p, wp_s.at[m], wp_r.at[m, slot], partner, False)

    def b2_wait(m, slot, r):
        for yslot in slots_of(NY, r):
            arrived(w.at[m, zpos(slot), ypos(yslot), 1], w_r2.at[m, slot, yslot])
            b_partner(m, slot, yslot)

    RZ = NZ // 2
    RY = NY // 2

    def y_start():
        @core0
        def _():
            for m in range(3):
                a1_send(m, 1)

    def y_more(r):
        @core0
        def _():
            for m in range(3):
                a1_wait(m, r)
                if r < RY:
                    a1_send(m, r + 1)

    def z_start():
        @core0
        def _():
            for m in range(3):
                a2_send(m, 1)
            for m in range(3):
                a_partner(m, 0)

        @core1
        def _():
            for m in range(3):
                b1_send(m, 1)
            for m in range(3):
                b2_send(m, 0, 1)
                b_partner(m, 0, 0)

    def tick(r, ms=(0, 1, 2)):
        @core0
        def _():
            for m in ms:
                if r <= RZ:
                    a2_wait(m, r)
                    if r < RZ:
                        a2_send(m, r + 1)
                    for slot in slots_of(NZ, r):
                        a_partner(m, slot)

        @core1
        def _():
            for m in ms:
                if r <= RZ:
                    b1_wait(m, r)
                    if r < RZ:
                        b1_send(m, r + 1)
                    for slot in slots_of(NZ, r):
                        b2_send(m, slot, 1)
                        b_partner(m, slot, 0)
                for k in range(1, RY + 1):
                    if 0 <= r - k <= RZ:
                        for slot in slots_of(NZ, r - k):
                            b2_wait(m, slot, k)
                            if k < RY:
                                b2_send(m, slot, k + 1)

    y_start()

    lane = lax.broadcasted_iota(jnp.int32, (T, 256), 1)
    own0 = (lane < 64) | ((lane >= 128) & (lane < 160))
    own1 = ((lane >= 64) & (lane < 128)) | ((lane >= 160) & (lane < 192))
    own2 = ((lane >= 64) & (lane < 96)) | (lane >= 128)

    def spread(k):
        narrow = qall[k, :, 0:256]
        wide = qall[k, :, 128:384]
        zero = jnp.zeros_like(narrow)
        qx[0, k * T : (k + 1) * T, :] = jnp.where(own0, narrow, zero)
        qx[1, k * T : (k + 1) * T, :] = jnp.where(own1, narrow, zero)
        qx[2, k * T : (k + 1) * T, :] = jnp.where(own2, wide, zero)

    spread(0)
    mrow[...] = jnp.full_like(mrow, -1e30)
    lrow[...] = jnp.zeros_like(lrow)
    acc[...] = jnp.zeros_like(acc)
    for k in range(1, NY):
        arrived(qall.at[k], q_r.at[k])
        spread(k)

    QB = min(256, NY * T)
    head_rows = ((0, 64), (64, 128), (128, 256))

    def attend(first, count):
        nk = count * 2 * T
        k_narrow = kv[first : first + count, :, :, 0:256].reshape(nk, 256)
        k_wide = kv[first : first + count, :, :, 128:384].reshape(nk, 256)

        def values(h):
            lo, hi = ((384, 512), (384, 512), (512, 640))[h]
            r0, r1 = ((0, 64), (64, 128), (0, 128))[h]
            return jnp.concatenate(
                [kv[first + s, cc, r0:r1, lo:hi] for s in range(count) for cc in range(2)], axis=1
            )

        def block(b, carry):
            cols = pl.ds(pl.multiple_of(b * QB, QB), QB)
            for h in range(3):
                s = dot_nt(k_narrow if h < 2 else k_wide, qx[h, cols, :]) * (scales[h] * LOG2E)
                old = mrow[h : h + 1, cols]
                new = jnp.maximum(old, jnp.max(s, axis=0, keepdims=True))
                shrink = jnp.exp2(old - new)
                p = jnp.exp2(s - new)
                lrow[h : h + 1, cols] = lrow[h : h + 1, cols] * shrink + jnp.sum(p, axis=0, keepdims=True)
                mrow[h : h + 1, cols] = new
                r0, r1 = head_rows[h]
                acc[r0:r1, cols] = acc[r0:r1, cols] * shrink + dot(values(h), p.astype(BF16))
            return carry

        lax.fori_loop(0, NY * T // QB, block, 0)

    arrived(kv.at[0, 1 - c], kvp_r.at[0])
    attend(0, 1)
    y_more(1)
    if NX > 1:
        wo_wait(1)
        if 1 < NX // 2:
            wo_send(2)
    for r in range(1, RZ + 1):
        ring = slots_of(NZ, r)
        for slot in ring:
            arrived(kv.at[slot, c], kv_r.at[slot])
        if r < RZ:
            kv_send(r + 1)
        for slot in ring:
            kv_partner(slot)
        if r == max(RZ - 1, 1):
            for k in range(2, RY + 1):
                y_more(k)
            z_start()
        for slot in ring:
            arrived(kv.at[slot, 1 - c], kvp_r.at[slot])
        attend(ring[0], len(ring))

    for k in range(NY):
        cols = slice(k * T, (k + 1) * T)
        osend[k] = acc[:, cols].astype(BF16)
        ssend[k, 0:3] = mrow[0:3, cols]
        ssend[k, 3:6] = lrow[0:3, cols]
        ssend[k, 6:8] = jnp.zeros((2, T), F32)
    for k in range(1, NY):
        send(osend.at[k], orecv.at[NY - k], o_s.at[k], o_r.at[NY - k], dev(yy=y + k))
        send(ssend.at[k], srecv.at[NY - k], st_s.at[k], st_r.at[NY - k], dev(yy=y + k))
    for r in range(2, NX // 2 + 1):
        wo_wait(r)
        if r < NX // 2:
            wo_send(r + 1)
    for k in range(1, NY):
        arrived(orecv.at[k], o_r.at[k])
        arrived(srecv.at[k], st_r.at[k])
    ms = [ssend[0, 0:3]] + [srecv[k, 0:3] for k in range(1, NY)]
    ls = [ssend[0, 3:6]] + [srecv[k, 3:6] for k in range(1, NY)]
    top = functools.reduce(jnp.maximum, ms)
    ws = [jnp.exp2(m - top) for m in ms]
    total = sum(a * b for a, b in zip(ws, ls))
    outs = []
    for h in range(3):
        r0, r1 = head_rows[h]
        o = acc[r0:r1, 0:T] * ws[0][h : h + 1]
        for k in range(1, NY):
            o = o + orecv[k, r0:r1].astype(F32) * ws[k][h : h + 1]
        o = o / total[h : h + 1]
        outs.append(o * lax.rsqrt(jnp.mean(o * o, axis=0, keepdims=True) + EPS))
    heads = jnp.transpose(jnp.concatenate(outs, axis=0))
    mixed[x] = (heads * ogain_ref[...]).astype(BF16)
    for k in range(1, NX):
        send(mixed.at[x], mixed.at[x], mx_s.at[k], mx_r.at[NX - k], dev(xx=x + k))
    tick(1)
    for k in range(1, NX):
        p = (x + k) % NX
        arrived(mixed.at[p], mx_r.at[k])
        arrived(resid.at[p], re_r.at[k])
    for slot in range(1, NX):
        arrived(wo.at[(x + offset_of(NX, slot) + 2 * NX) % NX, 1 - c], wop_r.at[slot])
    mixed_all = jnp.concatenate([mixed[k] for k in range(NX)], axis=1)

    def project(n, squares):
        cols = pl.ds(pl.multiple_of(n * 256, 256), 256)
        s = dot(mixed_all, wo[:, :, :, cols].reshape(NX * 256, 256))
        s = (s + resid[:, :, cols].reshape(T, 256).astype(F32)).astype(BF16)
        mid[n] = s
        s = s.astype(F32)
        return squares + jnp.sum(s * s, axis=1, keepdims=True)

    squares = lax.fori_loop(0, D // 256, project, jnp.zeros((T, 1), F32))
    factor = lax.rsqrt(squares / D + EPS)

    def scale(n, carry):
        cols = pl.ds(pl.multiple_of(n * 256, 256), 256)
        normed[n] = (mid[n].astype(F32) * factor * mgain_ref[:, cols]).astype(BF16)
        return carry

    lax.fori_loop(0, D // 256, scale, 0)

    def from_partner(m, slot):
        arrived(w.at[m, zpos(slot), :, 1 - c], wp_r.at[m, slot])

    accg[...] = jnp.zeros_like(accg)
    accu[...] = jnp.zeros_like(accu)
    F = accg.shape[1]

    def widen(k):
        for slot in slots_of(NZ, k):
            from_partner(0, slot)
            from_partner(1, slot)
        ring = slots_of(NZ, k)

        def one(i, carry):
            step = 0 if k == 0 else (k if len(ring) == 1 else (2 * i - 1) * k)
            p = (z + step + 2 * NZ) % NZ
            n = normed[p]
            accg[...] += dot(n, w[0, p].reshape(256, F))
            accu[...] += dot(n, w[1, p].reshape(256, F))
            return carry

        lax.fori_loop(0, len(ring), one, 0)

    for r in range(2, RZ + RY + 1):
        tick(r)
        if r >= RY:
            widen(r - RY)
    for m in (2,):
        for slot in range(NZ):
            from_partner(m, slot)
    g = accg[...]
    hid[...] = (g / (1.0 + jnp.exp(-g)) * accu[...]).astype(BF16)
    GROUPS = rs_r.shape[0]
    per = NZ // GROUPS

    def narrow(n, carry):
        s = dot_nt(hid[...], w[2, n].reshape(256, F)).astype(BF16)
        part[n] = s.reshape(NX, R, 256)
        return carry

    for gr in range(GROUPS):
        lax.fori_loop(gr * per, (gr + 1) * per, narrow, 0)
        rows = pl.ds(gr * per, per)
        for k in range(1, NX):
            p = (x + k) % NX
            send(part.at[rows, p], rsum.at[NX - k, rows], rs_s.at[gr, k], rs_r.at[gr, NX - k], dev(xx=x + k))
    for gr in range(GROUPS):
        rows = pl.ds(gr * per, per)
        for k in range(1, NX):
            arrived(rsum.at[k, rows], rs_r.at[gr, k])
        for n in range(gr * per, (gr + 1) * per):
            s = part[n, x].astype(F32)
            for k in range(1, NX):
                s = s + rsum[k, n].astype(F32)
            s = s + mid[n, pl.ds(pl.multiple_of(x * R, R), R), :].astype(F32)
            out_ref[:, n * 256 : (n + 1) * 256] = s.astype(BF16)

    for d in pend:
        d.wait_send()

    @core0
    def _():
        for m in range(3):
            arrived(w.at[m, 0, pl.ds(0, NY - 1), 0], w_s1.at[m])
            arrived(w.at[m, pl.ds(0, NZ - 1), :, 0], w_s2.at[m])
            arrived(w.at[m, :, :, 0], wp_s.at[m])

    @core1
    def _():
        for m in range(3):
            arrived(w.at[m, pl.ds(0, NZ - 1), 0, 1], w_s1.at[m])
            arrived(w.at[m, :, pl.ds(0, NY - 1), 1], w_s2.at[m])
            arrived(w.at[m, :, :, 1], wp_s.at[m])


def on_device(
    NZ,
    NX,
    residual,
    query_content,
    query_rotary,
    key_latent,
    rotary_key,
    latent_gain,
    key_weight,
    value_weight,
    output_gain,
    output_weight,
    mixer_gain,
    gate_weight,
    up_weight,
    down_weight,
):
    T = key_latent.shape[0]
    R, D = residual.shape
    F = gate_weight.shape[1]
    positions = lax.axis_index("sp") * T + lax.iota(jnp.int32, T)
    lanes = jnp.arange(128) % ROT_DIM
    half = ROT_DIM // 2
    power = 2.0 * (lanes % half).astype(F32) / ROT_DIM
    inverse = 1.0 / jnp.power(ROPE_BASE, power)
    angles = positions.astype(F32)[:, None] * inverse[None, :]
    cos = jnp.cos(angles)
    sin = jnp.where(lanes[None, :] < half, -jnp.sin(angles), jnp.sin(angles))
    vm = pl.BlockSpec(memory_space=pltpu.VMEM)
    hbm = pl.BlockSpec(memory_space=pl.ANY)
    V = pltpu.VMEM
    S = pltpu.SemaphoreType.DMA
    scales = ((64 + ROT_DIM) ** -0.5,) * 2 + ((128 + ROT_DIM) ** -0.5,)
    return pl.pallas_call(
        functools.partial(kernel, NZ, NX, scales),
        out_shape=jax.ShapeDtypeStruct((R, D), BF16),
        in_specs=[vm] * 11 + [hbm] * 5,
        out_specs=vm,
        scratch_shapes=[
            V((3, NZ, NY, 2, R, F), BF16),
            V((NZ, 2, T, 640), BF16),
            V((NY, T, 384), BF16),
            V((3, NY * T, 256), BF16),
            V((256, NY * T), F32),
            V((8, NY * T), F32),
            V((8, NY * T), F32),
            V((NY, 256, T), BF16),
            V((NY, 256, T), BF16),
            V((NY, 8, T), F32),
            V((NY, 8, T), F32),
            V((NX, T, 256), BF16),
            V((NX, 2, 128, D), BF16),
            V((NX, R, D), BF16),
            V((NZ, T, 256), BF16),
            V((NZ, T, 256), BF16),
            V((T, F), F32),
            V((T, F), F32),
            V((T, F), BF16),
            V((NZ, NX, R, 256), BF16),
            V((NX, NZ, R, 256), BF16),
            S((5,)),
            S((NZ,)),
            S((NZ,)),
            S((NZ,)),
            S((NZ,)),
            S((NY,)),
            S((NY,)),
            S((NY,)),
            S((NY,)),
            S((NY,)),
            S((NY,)),
            S((NX,)),
            S((NX,)),
            S((NX,)),
            S((NX,)),
            S((NX,)),
            S((NX,)),
            S((NX,)),
            S((NX,)),
            S((NZ // 2, NX)),
            S((NZ // 2, NX)),
            S((3,)),
            S((3,)),
            S((3,)),
            S((3, NZ)),
            S((3, NZ, NY)),
            S((3, NZ)),
        ],
        compiler_params=pltpu.CompilerParams(
            collective_id=0, has_side_effects=True, vmem_limit_bytes=60 * 1024 * 1024
        ),
    )(
        cos,
        sin,
        query_content,
        query_rotary,
        key_latent,
        rotary_key,
        latent_gain[None, :],
        key_weight,
        value_weight,
        output_gain[None, :],
        mixer_gain[None, :],
        residual,
        output_weight.reshape(2, 128, D),
        gate_weight,
        up_weight,
        down_weight.T,
    )


def solution(mesh):
    placed = (
        P(("sp", "tp"), None),
        P("sp", "tp"),
        P("sp", "tp"),
        P("sp", None),
        P("sp", None),
        P(),
        P(None, "tp"),
        P(None, "tp"),
        P("tp"),
        P("tp", None),
        P(),
        P("sp", "tp"),
        P("sp", "tp"),
        P("tp", "sp"),
    )
    NZ = mesh.shape["sp"] // (2 * NY)
    NX = mesh.shape["tp"]
    return jax.shard_map(
        functools.partial(on_device, NZ, NX),
        mesh=mesh,
        in_specs=placed,
        out_specs=P(("sp", "tp"), None),
        check_vma=False,
    )
```

```python
import contextlib
import functools

import jax
import jax.numpy as jnp
from jax import lax
from jax.experimental import pallas as pl
from jax.experimental.pallas import tpu as pltpu
from jax.sharding import PartitionSpec as P

NY = 4
ROT_DIM = 32
EPS = 1e-06
ROPE_BASE = 500000.0
LOG2E = 1.4426950408889634
MESH = pl.DeviceIdType.MESH
F32 = jnp.float32
BF16 = jnp.bfloat16


def dot(a, b):
    return lax.dot_general(a, b, (((1,), (0,)), ((), ())), preferred_element_type=F32)


def dot_nt(a, b):
    return lax.dot_general(a, b, (((1,), (1,)), ((), ())), preferred_element_type=F32)


def hops(n):
    both = list(range(1, (n - 1) // 2 + 1))
    return both, (n // 2 if n % 2 == 0 and n > 1 else None)


def kernel(
    NZ,
    NX,
    scales,
    cos_ref,
    sin_ref,
    ogain_ref,
    mgain_ref,
    lgain_ref,
    lat_hbm,
    kw_hbm,
    vw_hbm,
    qc_hbm,
    qr_hbm,
    rk_hbm,
    resid_hbm,
    ow_hbm,
    gate_hbm,
    up_hbm,
    down_hbm,
    out_ref,
    lat_ref,
    kw_ref,
    vw_ref,
    qc_ref,
    qr_ref,
    rk_ref,
    w,
    kv,
    qall,
    qx,
    acc,
    mrow,
    lrow,
    osend,
    orecv,
    ssend,
    srecv,
    mixed,
    wo,
    resid,
    mid,
    normed,
    accg,
    accu,
    hid,
    part,
    rsum,
    loc_sem,
    kv_s,
    kv_r,
    kvp_s,
    kvp_r,
    q_s,
    q_r,
    o_s,
    o_r,
    st_s,
    st_r,
    mx_s,
    mx_r,
    wo_s,
    wo_r,
    wop_s,
    wop_r,
    re_s,
    re_r,
    rs_s,
    rs_r,
    w_s1,
    w_s2,
    wp_s,
    w_r1,
    w_r2,
    wp_r,
):
    sp = lax.axis_index("sp")
    x = lax.axis_index("tp")
    c = sp % 2
    y = (sp // 2) % NY
    z = sp // (2 * NY)
    T = qc_ref.shape[0]
    R = resid.shape[1]
    D = resid.shape[2]
    phases = contextlib.ExitStack()

    def phase(name):
        phases.close()
        phases.enter_context(jax.named_scope(name))

    pend = []

    def dev(zz=None, yy=None, cc=None, xx=None):
        zz = z if zz is None else (zz + 2 * NZ) % NZ
        yy = y if yy is None else (yy + 2 * NY) % NY
        cc = c if cc is None else cc
        xx = x if xx is None else (xx + 2 * NX) % NX
        return ((zz * NY + yy) * 2 + cc, xx)

    def send(src, dst, ssem, rsem, device, keep=True):
        d = pltpu.make_async_remote_copy(
            src_ref=src, dst_ref=dst, send_sem=ssem, recv_sem=rsem, device_id=device, device_id_type=MESH
        )
        d.start()
        if keep:
            pend.append(d)

    def arrived(ref, sem):
        pltpu.make_async_copy(ref, ref, sem).wait()

    def core0(f):
        pl.when(c == 0)(f)

    def core1(f):
        pl.when(c == 1)(f)

    partner = dev(cc=1 - c)
    dirc = 1 - 2 * c
    zboth, zlast = hops(NZ)
    yboth, ylast = hops(NY)
    xboth, xlast = hops(NX)

    barrier = pltpu.get_barrier_semaphore()
    peers = [partner]
    peers += [dev(zz=z + 1)] + ([dev(zz=z - 1)] if NZ > 2 else [])
    peers += [dev(yy=y + k) for k in range(1, NY)]
    peers += [dev(xx=x + k) for k in range(1, NX)]
    for p in peers:
        pl.semaphore_signal(barrier, inc=1, device_id=p, device_id_type=MESH)

    def local(pairs, first):
        copies = [
            pltpu.make_async_copy(a, b, loc_sem.at[first + k]) for k, (a, b) in enumerate(pairs)
        ]
        for d in copies:
            d.start()
        return copies

    small = local(
        [(lat_hbm, lat_ref), (kw_hbm, kw_ref), (vw_hbm, vw_ref), (qc_hbm, qc_ref), (qr_hbm, qr_ref), (rk_hbm, rk_ref)],
        0,
    )
    loc = local(
        [
            (gate_hbm, w.at[0, z, y, c]),
            (up_hbm, w.at[1, z, y, c]),
            (down_hbm, w.at[2, z, y, c]),
            (ow_hbm, wo.at[x]),
            (resid_hbm, resid.at[x]),
        ],
        6,
    )

    phase("qkv")
    for d in small:
        d.wait()
    half = ROT_DIM // 2
    cos = cos_ref[...]
    sin = sin_ref[...]

    def turned(ref, count):
        rows = []
        for h in range(count):
            a = ref[h * ROT_DIM : h * ROT_DIM + half, :].astype(F32)
            b = ref[h * ROT_DIM + half : (h + 1) * ROT_DIM, :].astype(F32)
            rows += [a * cos - b * sin, b * cos + a * sin]
        return rows

    lat = lat_ref[...].astype(F32)
    lat = lat * lax.rsqrt(jnp.mean(lat * lat, axis=-1, keepdims=True) + EPS)
    lat = (lat * lgain_ref[...]).astype(BF16)
    keys = dot(lat, kw_ref[...]).astype(BF16)
    vals = jnp.transpose(dot(lat, vw_ref[...])).astype(BF16)
    kv[0, c, :, 0:128] = keys[:, 0:128]
    kv[0, c, :, 128:256] = jnp.transpose(jnp.concatenate(turned(rk_ref, 1) * 4, axis=0)).astype(BF16)
    kv[0, c, :, 256:384] = keys[:, 128:256]
    kv[0, c, :, 384:512] = vals[0:128, :]
    kv[0, c, :, 512:640] = vals[128:256, :]

    turned_q = turned(qr_ref, 3) + [jnp.zeros((ROT_DIM, T), F32)]
    qall[0, :, 0:128] = qc_ref[:, 0:128]
    qall[0, :, 128:256] = jnp.transpose(jnp.concatenate(turned_q, axis=0)).astype(BF16)
    qall[0, :, 256:384] = qc_ref[:, 128:256]

    phase("barrier")
    pl.semaphore_wait(barrier, len(peers))

    def kv_copy(src_slot, dst_slot, device):
        send(kv.at[src_slot, c], kv.at[dst_slot, c], kv_s.at[dst_slot], kv_r.at[dst_slot], device)

    def kv_partner(slot):
        send(kv.at[slot, c], kv.at[slot, c], kvp_s.at[slot], kvp_r.at[slot], partner)

    def kv_send(r):
        if r in zboth:
            kv_copy(2 * r - 3 if r > 1 else 0, 2 * r - 1, dev(zz=z + 1))
            kv_copy(2 * r - 2 if r > 1 else 0, 2 * r, dev(zz=z - 1))
        elif r == zlast:
            kv_copy((2 * r - 3 + c) if r > 1 else 0, NZ - 1, dev(zz=z + dirc))

    def slots_of(n, r):
        if r == 0:
            return [0]
        return [2 * r - 1, 2 * r] if r <= (n - 1) // 2 else [n - 1]

    def offset_of(n, slot):
        if slot == 0:
            return 0
        return slot_r(n, slot) if slot % 2 == 0 else -slot_r(n, slot)

    def slot_r(n, slot):
        return (slot + 1) // 2

    def zpos(slot):
        return (z + offset_of(NZ, slot) + 2 * NZ) % NZ

    def ypos(slot):
        return (y + offset_of(NY, slot) + 2 * NY) % NY

    def wo_send(r):
        if r in xboth:
            send(wo.at[(x - r + 1 + NX) % NX, c], wo.at[(x - r + 1 + NX) % NX, c], wo_s.at[2 * r - 1], wo_r.at[2 * r - 1], dev(xx=x + 1))
            send(wo.at[(x + r - 1) % NX, c], wo.at[(x + r - 1) % NX, c], wo_s.at[2 * r], wo_r.at[2 * r], dev(xx=x - 1))
        elif r == xlast:
            p = (x - dirc * (r - 1) + 2 * NX) % NX
            send(wo.at[p, c], wo.at[p, c], wo_s.at[NX - 1], wo_r.at[NX - 1], dev(xx=x + dirc))

    def wo_wait(r):
        for slot in slots_of(NX, r):
            p = (x + offset_of(NX, slot) + 2 * NX) % NX
            arrived(wo.at[p, c], wo_r.at[slot])
            send(wo.at[p, c], wo.at[p, c], wop_s.at[slot], wop_r.at[slot], partner)

    def zdir(m):
        return dirc * (1 - 2 * (m % 2))

    def ring_y(m, zz, cc, r, ssem, rsems):
        if r in yboth:
            a, b = (y - r + 1 + NY) % NY, (y + r - 1) % NY
            send(w.at[m, zz, a, cc], w.at[m, zz, a, cc], ssem, rsems(2 * r - 1), dev(yy=y + 1), False)
            send(w.at[m, zz, b, cc], w.at[m, zz, b, cc], ssem, rsems(2 * r), dev(yy=y - 1), False)
        elif r == ylast:
            p = (y - zdir(m) * (r - 1) + 2 * NY) % NY
            send(w.at[m, zz, p, cc], w.at[m, zz, p, cc], ssem, rsems(NY - 1), dev(yy=y + zdir(m)), False)

    def ring_z(m, view, r, ssem, rsems):
        if r in zboth:
            a, b = (z - r + 1 + NZ) % NZ, (z + r - 1) % NZ
            send(view(a), view(a), ssem, rsems(2 * r - 1), dev(zz=z + 1), False)
            send(view(b), view(b), ssem, rsems(2 * r), dev(zz=z - 1), False)
        elif r == zlast:
            p = (z - zdir(m) * (r - 1) + 2 * NZ) % NZ
            send(view(p), view(p), ssem, rsems(NZ - 1), dev(zz=z + zdir(m)), False)

    def a1_send(m, r):
        ring_y(m, z, 0, r, w_s1.at[m], lambda s: w_r1.at[m, s])

    def a1_wait(m, r):
        for slot in slots_of(NY, r):
            arrived(w.at[m, z, ypos(slot), 0], w_r1.at[m, slot])

    def a_block(m, zz):
        return w.at[m, zz, :, 0]

    def a2_send(m, r):
        ring_z(m, lambda p: a_block(m, p), r, w_s2.at[m], lambda s: w_r2.at[m, s, 0])

    def a_partner(m, slot):
        p = zpos(slot)
        send(a_block(m, p), a_block(m, p), wp_s.at[m], wp_r.at[m, slot], partner, False)

    def a2_wait(m, r):
        for slot in slots_of(NZ, r):
            arrived(a_block(m, zpos(slot)), w_r2.at[m, slot, 0])

    def b1_send(m, r):
        ring_z(m, lambda p: w.at[m, p, y, c], r, w_s1.at[m], lambda s: w_r1.at[m, s])

    def b1_wait(m, r):
        for slot in slots_of(NZ, r):
            arrived(w.at[m, zpos(slot), y, c], w_r1.at[m, slot])

    def b2_send(m, slot, r):
        ring_y(m, zpos(slot), c, r, w_s2.at[m], lambda s: w_r2.at[m, slot, s])

    def b_partner(m, slot, yslot):
        p = w.at[m, zpos(slot), ypos(yslot), c]
        send(p, p, wp_s.at[m], wp_r.at[m, slot], partner, False)

    RZ = NZ // 2
    RY = NY // 2

    def b_start(m):
        b1_send(m, 1)
        b2_send(m, 0, 1)
        b_partner(m, 0, 0)

    def b_z(m, r):
        b1_wait(m, r)
        if r < RZ:
            b1_send(m, r + 1)
        for slot in slots_of(NZ, r):
            b2_send(m, slot, 1)
            b_partner(m, slot, 0)

    def b_y(m, r, k):
        for slot in slots_of(NZ, r):
            for yslot in slots_of(NY, k):
                arrived(w.at[m, zpos(slot), ypos(yslot), c], w_r2.at[m, slot, yslot])
            if k < RY:
                b2_send(m, slot, k + 1)
            for yslot in slots_of(NY, k):
                b_partner(m, slot, yslot)

    def a_y(m, k):
        a1_wait(m, k)
        if k < RY:
            a1_send(m, k + 1)

    def a_z(m, r):
        a2_wait(m, r)
        if r < RZ:
            a2_send(m, r + 1)
        for slot in slots_of(NZ, r):
            a_partner(m, slot)

    def on(core, *steps):
        def run():
            for f, *a in steps:
                f(*a)

        if core is None:
            run()
        else:
            pl.when(c == core)(run)

    def both01(f, *a):
        return [(f, 0, *a), (f, 1, *a)]

    phase("send0")
    kv_send(1)
    kv_partner(0)
    for k in range(1, NY):
        send(qall.at[0], qall.at[NY - k], q_s.at[k], q_r.at[NY - k], dev(yy=y + k))
    for d in loc:
        d.wait()
    on(0, *both01(a1_send, 1))
    on(1, *both01(b_start))
    wo_send(1)
    for k in range(1, NX):
        send(resid.at[x], resid.at[x], re_s.at[k], re_r.at[NX - k], dev(xx=x + k))

    lane = lax.broadcasted_iota(jnp.int32, (T, 256), 1)
    own0 = (lane < 64) | ((lane >= 128) & (lane < 160))
    own1 = ((lane >= 64) & (lane < 128)) | ((lane >= 160) & (lane < 192))
    own2 = ((lane >= 64) & (lane < 96)) | (lane >= 128)

    def spread(k):
        narrow = qall[k, :, 0:256]
        wide = qall[k, :, 128:384]
        zero = jnp.zeros_like(narrow)
        qx[0, k * T : (k + 1) * T, :] = jnp.where(own0, narrow, zero)
        qx[1, k * T : (k + 1) * T, :] = jnp.where(own1, narrow, zero)
        qx[2, k * T : (k + 1) * T, :] = jnp.where(own2, wide, zero)

    def kv_wait(r):
        phase(f"kvw#r={r}")
        for slot in slots_of(NZ, r):
            arrived(kv.at[slot, c], kv_r.at[slot])
        if r < RZ:
            kv_send(r + 1)
        for slot in slots_of(NZ, r):
            kv_partner(slot)

    phase("spread0")
    spread(0)
    mrow[...] = jnp.full_like(mrow, -1e30)
    lrow[...] = jnp.zeros_like(lrow)
    acc[...] = jnp.zeros_like(acc)
    kv_wait(1)
    phase("g1")
    on(1, *both01(b_z, 1))
    on(0, *both01(a_y, 1))
    phase("qwait")
    for k in range(1, NY):
        arrived(qall.at[k], q_r.at[k])
        spread(k)

    QB = min(256, NY * T)
    head_rows = ((0, 64), (64, 128), (128, 256))

    def attend(first, count):
        nk = count * 2 * T
        k_narrow = kv[first : first + count, :, :, 0:256].reshape(nk, 256)
        k_wide = kv[first : first + count, :, :, 128:384].reshape(nk, 256)

        def values(h):
            lo, hi = ((384, 512), (384, 512), (512, 640))[h]
            r0, r1 = ((0, 64), (64, 128), (0, 128))[h]
            return jnp.concatenate(
                [kv[first + s, cc, r0:r1, lo:hi] for s in range(count) for cc in range(2)], axis=1
            )

        def block(b, carry):
            cols = pl.ds(pl.multiple_of(b * QB, QB), QB)
            for h in range(3):
                s = dot_nt(k_narrow if h < 2 else k_wide, qx[h, cols, :]) * (scales[h] * LOG2E)
                old = mrow[h : h + 1, cols]
                new = jnp.maximum(old, jnp.max(s, axis=0, keepdims=True))
                shrink = jnp.exp2(old - new)
                p = jnp.exp2(s - new)
                lrow[h : h + 1, cols] = lrow[h : h + 1, cols] * shrink + jnp.sum(p, axis=0, keepdims=True)
                mrow[h : h + 1, cols] = new
                r0, r1 = head_rows[h]
                acc[r0:r1, cols] = acc[r0:r1, cols] * shrink + dot(values(h), p.astype(BF16))
            return carry

        lax.fori_loop(0, NY * T // QB, block, 0)

    def att(r):
        phase(f"attw#r={r}")
        ring = slots_of(NZ, r)
        for slot in ring:
            arrived(kv.at[slot, 1 - c], kvp_r.at[slot])
        phase(f"att#r={r}")
        attend(ring[0], len(ring))

    att(0)
    kv_wait(2)
    phase("g2")
    on(0, *both01(a_y, 2), (a2_send, 0, 1), (a_partner, 0, 0), (a_partner, 1, 0))
    on(1, *both01(b_y, 0, 1))
    on(None, (b_start, 2))
    att(1)
    kv_wait(3)
    phase("g3")
    on(0, (a2_send, 1, 1))
    on(1, *both01(b_z, 2), *both01(b_y, 0, 2), *both01(b_y, 1, 1))
    on(None, (b_z, 2, 1))
    att(2)
    kv_wait(4)
    phase("g4")
    on(0, *both01(a_z, 1))
    on(1, *both01(b_y, 1, 2), *both01(b_y, 2, 1))
    on(None, (b_y, 2, 0, 1))
    att(3)
    phase("g5")
    on(1, *both01(b_z, 3))
    on(None, (b_z, 2, 2), (b_y, 2, 0, 2), (b_y, 2, 1, 1))
    att(4)

    phase("osend")
    for k in range(NY):
        cols = slice(k * T, (k + 1) * T)
        osend[k] = acc[:, cols].astype(BF16)
        ssend[k, 0:3] = mrow[0:3, cols]
        ssend[k, 3:6] = lrow[0:3, cols]
        ssend[k, 6:8] = jnp.zeros((2, T), F32)
    for k in range(1, NY):
        send(osend.at[k], orecv.at[NY - k], o_s.at[k], o_r.at[NY - k], dev(yy=y + k))
        send(ssend.at[k], srecv.at[NY - k], st_s.at[k], st_r.at[NY - k], dev(yy=y + k))
    phase("g6")
    on(1, *both01(b_y, 2, 2), *both01(b_y, 3, 1))
    wo_wait(1)
    wo_send(2)
    phase("owait")
    for k in range(1, NY):
        arrived(orecv.at[k], o_r.at[k])
        arrived(srecv.at[k], st_r.at[k])
    phase("merge")
    ms = [ssend[0, 0:3]] + [srecv[k, 0:3] for k in range(1, NY)]
    ls = [ssend[0, 3:6]] + [srecv[k, 3:6] for k in range(1, NY)]
    top = functools.reduce(jnp.maximum, ms)
    ws = [jnp.exp2(m - top) for m in ms]
    total = sum(a * b for a, b in zip(ws, ls))
    outs = []
    for h in range(3):
        r0, r1 = head_rows[h]
        o = acc[r0:r1, 0:T] * ws[0][h : h + 1]
        for k in range(1, NY):
            o = o + orecv[k, r0:r1].astype(F32) * ws[k][h : h + 1]
        o = o / total[h : h + 1]
        outs.append(o * lax.rsqrt(jnp.mean(o * o, axis=0, keepdims=True) + EPS))
    heads = jnp.transpose(jnp.concatenate(outs, axis=0))
    mixed[x] = (heads * ogain_ref[...]).astype(BF16)
    for k in range(1, NX):
        send(mixed.at[x], mixed.at[x], mx_s.at[k], mx_r.at[NX - k], dev(xx=x + k))
    phase("g7")
    on(0, *both01(a_z, 2))
    on(1, *both01(b_z, 4), *both01(b_y, 3, 2))
    on(None, (b_z, 2, 3), (b_y, 2, 1, 2), (b_y, 2, 2, 1))
    wo_wait(2)
    phase("mixw")
    for k in range(1, NX):
        p = (x + k) % NX
        arrived(mixed.at[p], mx_r.at[k])
        arrived(resid.at[p], re_r.at[k])
    for slot in range(1, NX):
        arrived(wo.at[(x + offset_of(NX, slot) + 2 * NX) % NX, 1 - c], wop_r.at[slot])
    phase("proj")
    mixed_all = jnp.concatenate([mixed[k] for k in range(NX)], axis=1)

    def project(n, squares):
        cols = pl.ds(pl.multiple_of(n * 256, 256), 256)
        s = dot(mixed_all, wo[:, :, :, cols].reshape(NX * 256, 256))
        s = (s + resid[:, :, cols].reshape(T, 256).astype(F32)).astype(BF16)
        mid[n] = s
        s = s.astype(F32)
        return squares + jnp.sum(s * s, axis=1, keepdims=True)

    squares = lax.fori_loop(0, D // 256, project, jnp.zeros((T, 1), F32))
    factor = lax.rsqrt(squares / D + EPS)

    def scale(n, carry):
        cols = pl.ds(pl.multiple_of(n * 256, 256), 256)
        normed[n] = (mid[n].astype(F32) * factor * mgain_ref[:, cols]).astype(BF16)
        return carry

    lax.fori_loop(0, D // 256, scale, 0)

    phase("mlp0")
    def from_partner(m, slot):
        arrived(w.at[m, zpos(slot), :, 1 - c], wp_r.at[m, slot])

    accg[...] = jnp.zeros_like(accg)
    accu[...] = jnp.zeros_like(accu)
    F = accg.shape[1]

    def widen(k):
        for slot in slots_of(NZ, k):
            from_partner(0, slot)
            from_partner(1, slot)
        ring = slots_of(NZ, k)

        def one(i, carry):
            step = 0 if k == 0 else (k if len(ring) == 1 else (2 * i - 1) * k)
            p = (z + step + 2 * NZ) % NZ
            n = normed[p]
            accg[...] += dot(n, w[0, p].reshape(256, F))
            accu[...] += dot(n, w[1, p].reshape(256, F))
            return carry

        lax.fori_loop(0, len(ring), one, 0)

    phase("widen01")
    widen(0)
    widen(1)
    phase("g8")
    on(0, *both01(a_z, 3))
    on(1, *both01(b_y, 4, 1))
    on(None, (b_z, 2, 4), (b_y, 2, 2, 2), (b_y, 2, 3, 1))
    phase("widen2")
    widen(2)
    phase("g9")
    on(0, *both01(a_z, 4))
    on(1, *both01(b_y, 4, 2))
    phase("widen34")
    widen(3)
    widen(4)
    phase("silu")
    g = accg[...]
    hid[...] = (g / (1.0 + jnp.exp(-g)) * accu[...]).astype(BF16)

    def narrow(slot, carry):
        p = (z + ((slot + 1) // 2) * (1 - 2 * (slot % 2)) + 2 * NZ) % NZ
        s = dot_nt(hid[...], w[2, p].reshape(256, F)).astype(BF16)
        part[slot] = s.reshape(NX, R, 256)
        return carry

    def down(first, count):
        for slot in range(first, first + count):
            from_partner(2, slot)
        lax.fori_loop(first, first + count, narrow, 0)

    def sums_send(gr):
        rows = pl.ds(2 * gr, 2)
        for k in range(1, NX):
            p = (x + k) % NX
            send(part.at[rows, p], rsum.at[NX - k, rows], rs_s.at[gr, k], rs_r.at[gr, NX - k], dev(xx=x + k))

    phase("down0")
    down(0, 4)
    sums_send(0)
    sums_send(1)
    phase("g10")
    on(None, (b_y, 2, 3, 2), (b_y, 2, 4, 1))
    phase("down4")
    down(4, 2)
    sums_send(2)
    phase("g11")
    on(None, (b_y, 2, 4, 2))
    phase("down6")
    down(6, 2)
    sums_send(3)
    phase("final")
    for gr in range(NZ // 2):
        rows = pl.ds(2 * gr, 2)
        for k in range(1, NX):
            arrived(rsum.at[k, rows], rs_r.at[gr, k])
        for slot in (2 * gr, 2 * gr + 1):
            p = zpos(slot)
            s = part[slot, x].astype(F32)
            for k in range(1, NX):
                s = s + rsum[k, slot].astype(F32)
            s = s + mid[p, pl.ds(pl.multiple_of(x * R, R), R), :].astype(F32)
            out_ref[:, pl.ds(pl.multiple_of(p * 256, 256), 256)] = s.astype(BF16)

    phase("sendw")
    for d in pend:
        d.wait_send()

    def sent_a(m):
        arrived(w.at[m, 0, pl.ds(0, NY - 1), 0], w_s1.at[m])
        arrived(w.at[m, pl.ds(0, NZ - 1), :, 0], w_s2.at[m])
        arrived(w.at[m, :, :, 0], wp_s.at[m])

    def sent_b(m):
        arrived(w.at[m, pl.ds(0, NZ - 1), 0, 1], w_s1.at[m])
        arrived(w.at[m, :, pl.ds(0, NY - 1), 1], w_s2.at[m])
        arrived(w.at[m, :, :, 1], wp_s.at[m])

    on(0, (sent_a, 0), (sent_a, 1))
    on(1, (sent_b, 0), (sent_b, 1))
    on(None, (sent_b, 2))

    phases.close()


def on_device(
    NZ,
    NX,
    residual,
    query_content,
    query_rotary,
    key_latent,
    rotary_key,
    latent_gain,
    key_weight,
    value_weight,
    output_gain,
    output_weight,
    mixer_gain,
    gate_weight,
    up_weight,
    down_weight,
):
    T = key_latent.shape[0]
    R, D = residual.shape
    F = gate_weight.shape[1]
    positions = lax.axis_index("sp") * T + lax.iota(jnp.int32, T)
    power = jnp.arange(0, ROT_DIM, 2, dtype=F32) / ROT_DIM
    inverse = 1.0 / jnp.power(ROPE_BASE, power)
    angles = positions.astype(F32)[None, :] * inverse[:, None]
    cos = jnp.cos(angles)
    sin = jnp.sin(angles)
    vm = pl.BlockSpec(memory_space=pltpu.VMEM)
    hbm = pl.BlockSpec(memory_space=pl.ANY)
    V = pltpu.VMEM
    S = pltpu.SemaphoreType.DMA
    scales = ((64 + ROT_DIM) ** -0.5,) * 2 + ((128 + ROT_DIM) ** -0.5,)
    return pl.pallas_call(
        functools.partial(kernel, NZ, NX, scales),
        out_shape=jax.ShapeDtypeStruct((R, D), BF16),
        in_specs=[vm] * 5 + [hbm] * 11,
        out_specs=vm,
        scratch_shapes=[
            V((T, key_latent.shape[1]), BF16),
            V(key_weight.shape, BF16),
            V(value_weight.shape, BF16),
            V((T, 256), BF16),
            V((query_rotary.shape[1], T), BF16),
            V((ROT_DIM, T), BF16),
            V((3, NZ, NY, 2, R, F), BF16),
            V((NZ, 2, T, 640), BF16),
            V((NY, T, 384), BF16),
            V((3, NY * T, 256), BF16),
            V((256, NY * T), F32),
            V((8, NY * T), F32),
            V((8, NY * T), F32),
            V((NY, 256, T), BF16),
            V((NY, 256, T), BF16),
            V((NY, 8, T), F32),
            V((NY, 8, T), F32),
            V((NX, T, 256), BF16),
            V((NX, 2, 128, D), BF16),
            V((NX, R, D), BF16),
            V((NZ, T, 256), BF16),
            V((NZ, T, 256), BF16),
            V((T, F), F32),
            V((T, F), F32),
            V((T, F), BF16),
            V((NZ, NX, R, 256), BF16),
            V((NX, NZ, R, 256), BF16),
            S((11,)),
            S((NZ,)),
            S((NZ,)),
            S((NZ,)),
            S((NZ,)),
            S((NY,)),
            S((NY,)),
            S((NY,)),
            S((NY,)),
            S((NY,)),
            S((NY,)),
            S((NX,)),
            S((NX,)),
            S((NX,)),
            S((NX,)),
            S((NX,)),
            S((NX,)),
            S((NX,)),
            S((NX,)),
            S((NZ // 2, NX)),
            S((NZ // 2, NX)),
            S((3,)),
            S((3,)),
            S((3,)),
            S((3, NZ)),
            S((3, NZ, NY)),
            S((3, NZ)),
        ],
        compiler_params=pltpu.CompilerParams(
            collective_id=0, has_side_effects=True, vmem_limit_bytes=60 * 1024 * 1024
        ),
    )(
        cos,
        sin,
        output_gain[None, :],
        mixer_gain[None, :],
        latent_gain[None, :],
        key_latent,
        key_weight,
        value_weight,
        query_content,
        query_rotary.T,
        rotary_key.T,
        residual,
        output_weight.reshape(2, 128, D),
        gate_weight,
        up_weight,
        down_weight.T,
    )


def solution(mesh):
    placed = (
        P(("sp", "tp"), None),
        P("sp", "tp"),
        P("sp", "tp"),
        P("sp", None),
        P("sp", None),
        P(),
        P(None, "tp"),
        P(None, "tp"),
        P("tp"),
        P("tp", None),
        P(),
        P("sp", "tp"),
        P("sp", "tp"),
        P("tp", "sp"),
    )
    NZ = mesh.shape["sp"] // (2 * NY)
    NX = mesh.shape["tp"]
    return jax.shard_map(
        functools.partial(on_device, NZ, NX),
        mesh=mesh,
        in_specs=placed,
        out_specs=P(("sp", "tp"), None),
        check_vma=False,
    )
```

```python
import contextlib
import functools

import jax
import jax.numpy as jnp
from jax import lax
from jax.experimental import pallas as pl
from jax.experimental.pallas import tpu as pltpu
from jax.sharding import PartitionSpec as P

NY = 4
ROT_DIM = 32
EPS = 1e-06
ROPE_BASE = 500000.0
LOG2E = 1.4426950408889634
MESH = pl.DeviceIdType.MESH
F32 = jnp.float32
BF16 = jnp.bfloat16

PARTS = (
    "kvw1",
    "q1",
    "q2",
    "att0",
    "kvw2",
    "att1",
    "kvw3",
    "att2",
    "kvw4",
    "att3",
    "att4",
    "owait",
    "mixw",
    "widen0",
    "widen1",
    "widen2",
    "widen3",
    "widen4",
    "hid",
    "down0",
    "down1",
    "down2",
    "down3",
    "down4",
    "final",
)
PLAN = (
    (
        (("ast", 0), ("by0", 2), ("ast", 1), ("bz0", 2),),
        (),
        (("zz", 2, 1), ("zy", 2, 1),),
        (("ay", 1, 1),),
        (("wo0",),),
        (("y", 2, 1, 1), ("ay", 1, 2),),
        (),
        (("y", 2, 0, 1), ("re",), ("az0", 1),),
        (("ay", 0, 1), ("zz", 2, 2), ("zy", 2, 2),),
        (("ay", 0, 2), ("az0", 0),),
        (("wo1",), ("az", 1, 1),),
        (("az", 0, 1), ("az", 1, 2), ("wo2",),),
        (("az", 0, 2), ("y", 2, 2, 1),),
        (),
        (("y", 2, 0, 2), ("zz", 2, 3), ("zy", 2, 3),),
        (("az", 1, 3),),
        (("y", 2, 2, 2), ("az", 0, 3),),
        (("zz", 2, 4), ("zy", 2, 4), ("y", 2, 3, 1), ("az", 1, 4), ("az", 0, 4),),
        (("y", 2, 1, 2),),
        (),
        (),
        (("y", 2, 4, 1),),
        (("y", 2, 3, 2),),
        (("y", 2, 4, 2),),
        (),
    ),
    (
        (("bz0", 0), ("bz0", 1), ("by0", 2), ("bz0", 2), ("wo0",), ("by0", 1),),
        (),
        (("by0", 0), ("zz", 1, 1), ("zy", 1, 1), ("zz", 0, 1), ("zy", 0, 1),),
        (("re",),),
        (("y", 2, 0, 1), ("y", 1, 0, 1),),
        (("wo1",),),
        (("zz", 0, 2), ("zy", 0, 2), ("zz", 2, 1), ("zy", 2, 1),),
        (("zz", 2, 2), ("zy", 2, 2),),
        (("y", 0, 0, 1),),
        (("y", 1, 1, 1), ("y", 2, 1, 1),),
        (("zz", 1, 2), ("zy", 1, 2),),
        (("y", 2, 0, 2), ("zz", 0, 3), ("zy", 0, 3), ("zz", 0, 4), ("zy", 0, 4), ("y", 0, 1, 1),),
        (("y", 2, 2, 1), ("y", 1, 2, 1), ("y", 0, 2, 1), ("zz", 1, 3), ("zy", 1, 3), ("zz", 1, 4), ("zy", 1, 4), ("wo2",),),
        (("y", 0, 3, 1), ("y", 0, 4, 1), ("y", 1, 3, 1), ("y", 1, 0, 2), ("y", 0, 0, 2),),
        (("y", 0, 1, 2), ("y", 1, 1, 2),),
        (("y", 1, 4, 1), ("y", 1, 2, 2), ("y", 0, 2, 2),),
        (("y", 2, 2, 2), ("y", 2, 1, 2), ("zz", 2, 3), ("zy", 2, 3), ("zz", 2, 4), ("zy", 2, 4), ("y", 0, 3, 2), ("y", 1, 3, 2),),
        (("y", 2, 3, 1), ("y", 0, 4, 2), ("y", 1, 4, 2),),
        (("y", 2, 4, 1),),
        (),
        (("y", 2, 3, 2),),
        (),
        (),
        (("y", 2, 4, 2),),
        (),
    ),
)


def dot(a, b):
    return lax.dot_general(a, b, (((1,), (0,)), ((), ())), preferred_element_type=F32)


def dot_nt(a, b):
    return lax.dot_general(a, b, (((1,), (1,)), ((), ())), preferred_element_type=F32)


def hops(n):
    both = list(range(1, (n - 1) // 2 + 1))
    return both, (n // 2 if n % 2 == 0 and n > 1 else None)


def kernel(
    NZ,
    NX,
    scales,
    cos_ref,
    sin_ref,
    ogain_ref,
    mgain_ref,
    lgain_ref,
    lat_hbm,
    kw_hbm,
    vw_hbm,
    qc_hbm,
    qr_hbm,
    rk_hbm,
    resid_hbm,
    ow_hbm,
    gate_hbm,
    up_hbm,
    down_hbm,
    out_ref,
    lat_ref,
    kw_ref,
    vw_ref,
    qc_ref,
    qr_ref,
    rk_ref,
    w,
    kv,
    qall,
    qx,
    acc,
    mrow,
    lrow,
    osend,
    orecv,
    ssend,
    srecv,
    mixed,
    wo,
    resid,
    mid,
    normed,
    accg,
    accu,
    hid,
    part,
    rsum,
    loc_sem,
    kv_s,
    kv_r,
    kvp_s,
    kvp_r,
    q_s,
    q_r,
    o_s,
    o_r,
    st_s,
    st_r,
    mx_s,
    mx_r,
    wo_s,
    wo_r,
    wop_s,
    wop_r,
    re_s,
    re_r,
    rs_s,
    rs_r,
    w_s1,
    w_s2,
    wp_s,
    w_r1,
    w_r2,
    wp_r,
):
    sp = lax.axis_index("sp")
    x = lax.axis_index("tp")
    c = sp % 2
    y = (sp // 2) % NY
    z = sp // (2 * NY)
    T = qc_ref.shape[0]
    R = resid.shape[1]
    D = resid.shape[2]
    phases = contextlib.ExitStack()

    def phase(name):
        phases.close()
        phases.enter_context(jax.named_scope(name))

    pend = []

    def dev(zz=None, yy=None, cc=None, xx=None):
        zz = z if zz is None else (zz + 2 * NZ) % NZ
        yy = y if yy is None else (yy + 2 * NY) % NY
        cc = c if cc is None else cc
        xx = x if xx is None else (xx + 2 * NX) % NX
        return ((zz * NY + yy) * 2 + cc, xx)

    def send(src, dst, ssem, rsem, device, keep=True):
        d = pltpu.make_async_remote_copy(
            src_ref=src, dst_ref=dst, send_sem=ssem, recv_sem=rsem, device_id=device, device_id_type=MESH
        )
        d.start()
        if keep:
            pend.append(d)

    def arrived(ref, sem):
        pltpu.make_async_copy(ref, ref, sem).wait()

    partner = dev(cc=1 - c)
    dirc = 1 - 2 * c
    zboth, zlast = hops(NZ)
    yboth, ylast = hops(NY)
    xboth, xlast = hops(NX)

    barrier = pltpu.get_barrier_semaphore()
    peers = [partner]
    peers += [dev(zz=z + 1)] + ([dev(zz=z - 1)] if NZ > 2 else [])
    peers += [dev(yy=y + k) for k in range(1, NY)]
    peers += [dev(xx=x + k) for k in range(1, NX)]
    for p in peers:
        pl.semaphore_signal(barrier, inc=1, device_id=p, device_id_type=MESH)

    def local(pairs, first):
        copies = [
            pltpu.make_async_copy(a, b, loc_sem.at[first + k]) for k, (a, b) in enumerate(pairs)
        ]
        for d in copies:
            d.start()
        return copies

    small = local(
        [(lat_hbm, lat_ref), (kw_hbm, kw_ref), (vw_hbm, vw_ref), (qc_hbm, qc_ref), (qr_hbm, qr_ref), (rk_hbm, rk_ref)],
        0,
    )
    loc = local(
        [
            (gate_hbm, w.at[0, z, y, c]),
            (up_hbm, w.at[1, z, y, c]),
            (down_hbm, w.at[2, z, y, c]),
            (ow_hbm, wo.at[x]),
            (resid_hbm, resid.at[x]),
        ],
        6,
    )

    phase("qkv")
    for d in small:
        d.wait()
    half = ROT_DIM // 2
    cos = cos_ref[...]
    sin = sin_ref[...]

    def turned(ref, count):
        rows = []
        for h in range(count):
            a = ref[h * ROT_DIM : h * ROT_DIM + half, :].astype(F32)
            b = ref[h * ROT_DIM + half : (h + 1) * ROT_DIM, :].astype(F32)
            rows += [a * cos - b * sin, b * cos + a * sin]
        return rows

    lat = lat_ref[...].astype(F32)
    lat = lat * lax.rsqrt(jnp.mean(lat * lat, axis=-1, keepdims=True) + EPS)
    lat = (lat * lgain_ref[...]).astype(BF16)
    keys = dot(lat, kw_ref[...]).astype(BF16)
    vals = jnp.transpose(dot(lat, vw_ref[...])).astype(BF16)
    kv[0, c, :, 0:128] = keys[:, 0:128]
    kv[0, c, :, 128:256] = jnp.transpose(jnp.concatenate(turned(rk_ref, 1) * 4, axis=0)).astype(BF16)
    kv[0, c, :, 256:384] = keys[:, 128:256]
    kv[0, c, :, 384:512] = vals[0:128, :]
    kv[0, c, :, 512:640] = vals[128:256, :]

    turned_q = turned(qr_ref, 3) + [jnp.zeros((ROT_DIM, T), F32)]
    qall[0, :, 0:128] = qc_ref[:, 0:128]
    qall[0, :, 128:256] = jnp.transpose(jnp.concatenate(turned_q, axis=0)).astype(BF16)
    qall[0, :, 256:384] = qc_ref[:, 128:256]

    phase("barrier")
    pl.semaphore_wait(barrier, len(peers))

    def kv_copy(src_slot, dst_slot, device):
        send(kv.at[src_slot, c], kv.at[dst_slot, c], kv_s.at[dst_slot], kv_r.at[dst_slot], device)

    def kv_partner(slot):
        send(kv.at[slot, c], kv.at[slot, c], kvp_s.at[slot], kvp_r.at[slot], partner)

    def kv_send(r):
        if r in zboth:
            kv_copy(2 * r - 3 if r > 1 else 0, 2 * r - 1, dev(zz=z + 1))
            kv_copy(2 * r - 2 if r > 1 else 0, 2 * r, dev(zz=z - 1))
        elif r == zlast:
            kv_copy((2 * r - 3 + c) if r > 1 else 0, NZ - 1, dev(zz=z + dirc))

    def slots_of(n, r):
        if r == 0:
            return [0]
        return [2 * r - 1, 2 * r] if r <= (n - 1) // 2 else [n - 1]

    def offset_of(n, slot):
        if slot == 0:
            return 0
        return slot_r(n, slot) if slot % 2 == 0 else -slot_r(n, slot)

    def slot_r(n, slot):
        return (slot + 1) // 2

    def zpos(slot):
        return (z + offset_of(NZ, slot) + 2 * NZ) % NZ

    def ypos(slot):
        return (y + offset_of(NY, slot) + 2 * NY) % NY

    def wo_send(r):
        if r in xboth:
            send(wo.at[(x - r + 1 + NX) % NX, c], wo.at[(x - r + 1 + NX) % NX, c], wo_s.at[2 * r - 1], wo_r.at[2 * r - 1], dev(xx=x + 1), False)
            send(wo.at[(x + r - 1) % NX, c], wo.at[(x + r - 1) % NX, c], wo_s.at[2 * r], wo_r.at[2 * r], dev(xx=x - 1), False)
        elif r == xlast:
            p = (x - dirc * (r - 1) + 2 * NX) % NX
            send(wo.at[p, c], wo.at[p, c], wo_s.at[NX - 1], wo_r.at[NX - 1], dev(xx=x + dirc), False)

    def wo_wait(r):
        for slot in slots_of(NX, r):
            p = (x + offset_of(NX, slot) + 2 * NX) % NX
            arrived(wo.at[p, c], wo_r.at[slot])
            send(wo.at[p, c], wo.at[p, c], wop_s.at[slot], wop_r.at[slot], partner, False)

    def zdir(m):
        return dirc * (1 - 2 * (m % 2))

    def ring_y(m, zz, cc, r, ssem, rsems):
        if r in yboth:
            a, b = (y - r + 1 + NY) % NY, (y + r - 1) % NY
            send(w.at[m, zz, a, cc], w.at[m, zz, a, cc], ssem, rsems(2 * r - 1), dev(yy=y + 1), False)
            send(w.at[m, zz, b, cc], w.at[m, zz, b, cc], ssem, rsems(2 * r), dev(yy=y - 1), False)
        elif r == ylast:
            p = (y - zdir(m) * (r - 1) + 2 * NY) % NY
            send(w.at[m, zz, p, cc], w.at[m, zz, p, cc], ssem, rsems(NY - 1), dev(yy=y + zdir(m)), False)

    def ring_z(m, view, r, ssem, rsems):
        if r in zboth:
            a, b = (z - r + 1 + NZ) % NZ, (z + r - 1) % NZ
            send(view(a), view(a), ssem, rsems(2 * r - 1), dev(zz=z + 1), False)
            send(view(b), view(b), ssem, rsems(2 * r), dev(zz=z - 1), False)
        elif r == zlast:
            p = (z - zdir(m) * (r - 1) + 2 * NZ) % NZ
            send(view(p), view(p), ssem, rsems(NZ - 1), dev(zz=z + zdir(m)), False)

    def a1_send(m, r):
        ring_y(m, z, 0, r, w_s1.at[m], lambda s: w_r1.at[m, s])

    def a1_wait(m, r):
        for slot in slots_of(NY, r):
            arrived(w.at[m, z, ypos(slot), 0], w_r1.at[m, slot])

    def a_block(m, zz):
        return w.at[m, zz, :, 0]

    def a2_send(m, r):
        ring_z(m, lambda p: a_block(m, p), r, w_s2.at[m], lambda s: w_r2.at[m, s, 0])

    def a_partner(m, slot):
        p = zpos(slot)
        send(a_block(m, p), a_block(m, p), wp_s.at[m], wp_r.at[m, slot], partner, False)

    def a2_wait(m, r):
        for slot in slots_of(NZ, r):
            arrived(a_block(m, zpos(slot)), w_r2.at[m, slot, 0])

    def b1_send(m, r):
        ring_z(m, lambda p: w.at[m, p, y, c], r, w_s1.at[m], lambda s: w_r1.at[m, s])

    def b1_wait(m, r):
        for slot in slots_of(NZ, r):
            arrived(w.at[m, zpos(slot), y, c], w_r1.at[m, slot])

    def b2_send(m, slot, r):
        ring_y(m, zpos(slot), c, r, w_s2.at[m], lambda s: w_r2.at[m, slot, s])

    def b_partner(m, slot, yslot):
        p = w.at[m, zpos(slot), ypos(yslot), c]
        send(p, p, wp_s.at[m], wp_r.at[m, slot], partner, False)

    RZ = NZ // 2
    RY = NY // 2

    def b_first_y(m):
        b2_send(m, 0, 1)
        b_partner(m, 0, 0)

    def b_z(m, r):
        b1_wait(m, r)
        if r < RZ:
            b1_send(m, r + 1)

    def b_zy(m, r):
        for slot in slots_of(NZ, r):
            b2_send(m, slot, 1)
            b_partner(m, slot, 0)

    def b_y(m, r, k):
        for slot in slots_of(NZ, r):
            for yslot in slots_of(NY, k):
                arrived(w.at[m, zpos(slot), ypos(yslot), c], w_r2.at[m, slot, yslot])
            if k < RY:
                b2_send(m, slot, k + 1)
            for yslot in slots_of(NY, k):
                b_partner(m, slot, yslot)

    def a_y(m, k):
        a1_wait(m, k)
        if k < RY:
            a1_send(m, k + 1)

    def a_z(m, r):
        a2_wait(m, r)
        if r < RZ:
            a2_send(m, r + 1)
        for slot in slots_of(NZ, r):
            a_partner(m, slot)

    def a_first_z(m):
        a2_send(m, 1)
        a_partner(m, 0)

    def resid_send():
        for k in range(1, NX):
            send(resid.at[x], resid.at[x], re_s.at[k], re_r.at[NX - k], dev(xx=x + k), False)

    def wo_pass(r):
        wo_wait(r)
        if r < NX // 2:
            wo_send(r + 1)

    steps = {
        "ast": lambda m: a1_send(m, 1),
        "ay": a_y,
        "az0": a_first_z,
        "az": a_z,
        "bz0": lambda m: b1_send(m, 1),
        "by0": b_first_y,
        "zz": b_z,
        "zy": b_zy,
        "y": b_y,
        "wo0": lambda: wo_send(1),
        "wo1": lambda: wo_pass(1),
        "wo2": lambda: wo_pass(2),
        "re": resid_send,
    }

    def on(core, *todo):
        def run():
            for f, *a in todo:
                steps[f](*a)

        pl.when(c == core)(run)

    def gap(name):
        phase("g_" + name)
        at = PARTS.index(name)
        for core in (0, 1):
            if PLAN[core][at]:
                on(core, *PLAN[core][at])

    phase("send0")

    def q_send(r):
        if r in yboth:
            left = 0 if r == 1 else offset_of(NY, 2 * r - 3) % NY
            right = 0 if r == 1 else offset_of(NY, 2 * r - 2) % NY
            send(qall.at[left], qall.at[(-r) % NY], q_s.at[2 * r - 1], q_r.at[2 * r - 1], dev(yy=y + 1))
            send(qall.at[right], qall.at[r], q_s.at[2 * r], q_r.at[2 * r], dev(yy=y - 1))
        elif r == ylast:
            member = 0 if r == 1 else (-dirc * (r - 1) + NY) % NY
            send(qall.at[member], qall.at[r], q_s.at[NY - 1], q_r.at[NY - 1], dev(yy=y + dirc))

    kv_send(1)
    kv_partner(0)
    q_send(1)
    for d in loc:
        d.wait()

    lane = lax.broadcasted_iota(jnp.int32, (T, 256), 1)
    own0 = (lane < 64) | ((lane >= 128) & (lane < 160))
    own1 = ((lane >= 64) & (lane < 128)) | ((lane >= 160) & (lane < 192))
    own2 = ((lane >= 64) & (lane < 96)) | (lane >= 128)

    def spread(k):
        narrow = qall[k, :, 0:256]
        wide = qall[k, :, 128:384]
        zero = jnp.zeros_like(narrow)
        qx[0, k * T : (k + 1) * T, :] = jnp.where(own0, narrow, zero)
        qx[1, k * T : (k + 1) * T, :] = jnp.where(own1, narrow, zero)
        qx[2, k * T : (k + 1) * T, :] = jnp.where(own2, wide, zero)

    def kv_wait(r):
        phase(f"kvw#r={r}")
        for slot in slots_of(NZ, r):
            arrived(kv.at[slot, c], kv_r.at[slot])
        if r < RZ:
            kv_send(r + 1)
        for slot in slots_of(NZ, r):
            kv_partner(slot)

    phase("spread0")
    spread(0)
    mrow[...] = jnp.full_like(mrow, -1e30)
    lrow[...] = jnp.zeros_like(lrow)
    acc[...] = jnp.zeros_like(acc)
    def q_wait(r):
        phase(f"qw#r={r}")
        for slot in slots_of(NY, r):
            arrived(qall.at[offset_of(NY, slot) % NY], q_r.at[slot])
        if r < RY:
            q_send(r + 1)
        for slot in slots_of(NY, r):
            spread(offset_of(NY, slot) % NY)

    gap("kvw1")
    kv_wait(1)
    gap("q1")
    q_wait(1)
    gap("q2")
    for r in range(2, RY + 1):
        q_wait(r)

    QB = min(256, NY * T)
    head_rows = ((0, 64), (64, 128), (128, 256))

    def attend(first, count):
        nk = count * 2 * T
        k_narrow = kv[first : first + count, :, :, 0:256].reshape(nk, 256)
        k_wide = kv[first : first + count, :, :, 128:384].reshape(nk, 256)

        def values(h):
            lo, hi = ((384, 512), (384, 512), (512, 640))[h]
            r0, r1 = ((0, 64), (64, 128), (0, 128))[h]
            return jnp.concatenate(
                [kv[first + s, cc, r0:r1, lo:hi] for s in range(count) for cc in range(2)], axis=1
            )

        def block(b, carry):
            cols = pl.ds(pl.multiple_of(b * QB, QB), QB)
            for h in range(3):
                s = dot_nt(k_narrow if h < 2 else k_wide, qx[h, cols, :]) * (scales[h] * LOG2E)
                old = mrow[h : h + 1, cols]
                new = jnp.maximum(old, jnp.max(s, axis=0, keepdims=True))
                shrink = jnp.exp2(old - new)
                p = jnp.exp2(s - new)
                lrow[h : h + 1, cols] = lrow[h : h + 1, cols] * shrink + jnp.sum(p, axis=0, keepdims=True)
                mrow[h : h + 1, cols] = new
                r0, r1 = head_rows[h]
                acc[r0:r1, cols] = acc[r0:r1, cols] * shrink + dot(values(h), p.astype(BF16))
            return carry

        lax.fori_loop(0, NY * T // QB, block, 0)

    def att(r):
        phase(f"attw#r={r}")
        ring = slots_of(NZ, r)
        for slot in ring:
            arrived(kv.at[slot, 1 - c], kvp_r.at[slot])
        phase(f"att#r={r}")
        attend(ring[0], len(ring))

    gap("att0")
    att(0)
    for r in range(1, RZ + 1):
        if r < RZ:
            gap(f"kvw{r + 1}")
            kv_wait(r + 1)
        gap(f"att{r}")
        att(r)

    phase("osend")
    for k in range(NY):
        cols = slice(k * T, (k + 1) * T)
        osend[k] = acc[:, cols].astype(BF16)
        ssend[k, 0:3] = mrow[0:3, cols]
        ssend[k, 3:6] = lrow[0:3, cols]
        ssend[k, 6:8] = jnp.zeros((2, T), F32)
    for k in range(1, NY):
        send(osend.at[k], orecv.at[NY - k], o_s.at[k], o_r.at[NY - k], dev(yy=y + k))
        send(ssend.at[k], srecv.at[NY - k], st_s.at[k], st_r.at[NY - k], dev(yy=y + k))
    gap("owait")
    phase("owait")
    for k in range(1, NY):
        arrived(orecv.at[k], o_r.at[k])
        arrived(srecv.at[k], st_r.at[k])
    phase("merge")
    ms = [ssend[0, 0:3]] + [srecv[k, 0:3] for k in range(1, NY)]
    ls = [ssend[0, 3:6]] + [srecv[k, 3:6] for k in range(1, NY)]
    top = functools.reduce(jnp.maximum, ms)
    ws = [jnp.exp2(m - top) for m in ms]
    total = sum(a * b for a, b in zip(ws, ls))
    outs = []
    for h in range(3):
        r0, r1 = head_rows[h]
        o = acc[r0:r1, 0:T] * ws[0][h : h + 1]
        for k in range(1, NY):
            o = o + orecv[k, r0:r1].astype(F32) * ws[k][h : h + 1]
        o = o / total[h : h + 1]
        outs.append(o * lax.rsqrt(jnp.mean(o * o, axis=0, keepdims=True) + EPS))
    heads = jnp.transpose(jnp.concatenate(outs, axis=0))
    mixed[x] = (heads * ogain_ref[...]).astype(BF16)
    for k in range(1, NX):
        send(mixed.at[x], mixed.at[x], mx_s.at[k], mx_r.at[NX - k], dev(xx=x + k))
    gap("mixw")
    phase("mixw")
    for k in range(1, NX):
        p = (x + k) % NX
        arrived(mixed.at[p], mx_r.at[k])
        arrived(resid.at[p], re_r.at[k])
    for slot in range(1, NX):
        arrived(wo.at[(x + offset_of(NX, slot) + 2 * NX) % NX, 1 - c], wop_r.at[slot])
    phase("proj")
    mixed_all = jnp.concatenate([mixed[k] for k in range(NX)], axis=1)

    def project(n, squares):
        cols = pl.ds(pl.multiple_of(n * 256, 256), 256)
        s = dot(mixed_all, wo[:, :, :, cols].reshape(NX * 256, 256))
        s = (s + resid[:, :, cols].reshape(T, 256).astype(F32)).astype(BF16)
        mid[n] = s
        s = s.astype(F32)
        return squares + jnp.sum(s * s, axis=1, keepdims=True)

    squares = lax.fori_loop(0, D // 256, project, jnp.zeros((T, 1), F32))
    factor = lax.rsqrt(squares / D + EPS)

    def scale(n, carry):
        cols = pl.ds(pl.multiple_of(n * 256, 256), 256)
        normed[n] = (mid[n].astype(F32) * factor * mgain_ref[:, cols]).astype(BF16)
        return carry

    lax.fori_loop(0, D // 256, scale, 0)

    phase("mlp0")
    def from_partner(m, slot):
        arrived(w.at[m, zpos(slot), :, 1 - c], wp_r.at[m, slot])

    accg[...] = jnp.zeros_like(accg)
    accu[...] = jnp.zeros_like(accu)
    F = accg.shape[1]

    def widen(k):
        for slot in slots_of(NZ, k):
            from_partner(0, slot)
            from_partner(1, slot)
        ring = slots_of(NZ, k)

        def one(i, carry):
            step = 0 if k == 0 else (k if len(ring) == 1 else (2 * i - 1) * k)
            p = (z + step + 2 * NZ) % NZ
            n = normed[p]
            accg[...] += dot(n, w[0, p].reshape(256, F))
            accu[...] += dot(n, w[1, p].reshape(256, F))
            return carry

        lax.fori_loop(0, len(ring), one, 0)

    for r in range(RZ + 1):
        gap(f"widen{r}")
        phase(f"widen#r={r}")
        widen(r)
    gap("hid")
    phase("hid")
    g = accg[...]
    hid[...] = (g / (1.0 + jnp.exp(-g)) * accu[...]).astype(BF16)

    def narrow(slot, carry):
        p = (z + ((slot + 1) // 2) * (1 - 2 * (slot % 2)) + 2 * NZ) % NZ
        s = dot_nt(hid[...], w[2, p].reshape(256, F)).astype(BF16)
        part[slot] = s.reshape(NX, R, 256)
        return carry

    def sums_rows(r):
        ring = slots_of(NZ, r)
        return pl.ds(ring[0], len(ring))

    for r in range(RZ + 1):
        gap(f"down{r}")
        phase(f"down#r={r}")
        ring = slots_of(NZ, r)
        for slot in ring:
            from_partner(2, slot)
        lax.fori_loop(ring[0], ring[0] + len(ring), narrow, 0)
        rows = sums_rows(r)
        for k in range(1, NX):
            p = (x + k) % NX
            send(part.at[rows, p], rsum.at[NX - k, rows], rs_s.at[r, k], rs_r.at[r, NX - k], dev(xx=x + k))
    gap("final")
    phase("final")
    for r in range(RZ + 1):
        for k in range(1, NX):
            arrived(rsum.at[k, sums_rows(r)], rs_r.at[r, k])
        for slot in slots_of(NZ, r):
            p = zpos(slot)
            s = part[slot, x].astype(F32)
            for k in range(1, NX):
                s = s + rsum[k, slot].astype(F32)
            s = s + mid[p, pl.ds(pl.multiple_of(x * R, R), R), :].astype(F32)
            out_ref[:, pl.ds(pl.multiple_of(p * 256, 256), 256)] = s.astype(BF16)

    phase("sendw")
    for d in pend:
        d.wait_send()

    for k in range(1, NX):
        arrived(wo.at[0, 0], wo_s.at[k])
        arrived(wo.at[0, 0], wop_s.at[k])
        arrived(resid.at[0], re_s.at[k])

    def sent_a(m):
        arrived(w.at[m, 0, pl.ds(0, NY - 1), 0], w_s1.at[m])
        arrived(w.at[m, pl.ds(0, NZ - 1), :, 0], w_s2.at[m])
        arrived(w.at[m, :, :, 0], wp_s.at[m])

    def sent_b(m):
        arrived(w.at[m, pl.ds(0, NZ - 1), 0, 1], w_s1.at[m])
        arrived(w.at[m, :, pl.ds(0, NY - 1), 1], w_s2.at[m])
        arrived(w.at[m, :, :, 1], wp_s.at[m])

    @pl.when(c == 0)
    def _():
        sent_a(0)
        sent_a(1)

    @pl.when(c == 1)
    def _():
        sent_b(0)
        sent_b(1)

    sent_b(2)

    phases.close()


def on_device(
    NZ,
    NX,
    residual,
    query_content,
    query_rotary,
    key_latent,
    rotary_key,
    latent_gain,
    key_weight,
    value_weight,
    output_gain,
    output_weight,
    mixer_gain,
    gate_weight,
    up_weight,
    down_weight,
):
    T = key_latent.shape[0]
    R, D = residual.shape
    F = gate_weight.shape[1]
    positions = lax.axis_index("sp") * T + lax.iota(jnp.int32, T)
    power = jnp.arange(0, ROT_DIM, 2, dtype=F32) / ROT_DIM
    inverse = 1.0 / jnp.power(ROPE_BASE, power)
    angles = positions.astype(F32)[None, :] * inverse[:, None]
    cos = jnp.cos(angles)
    sin = jnp.sin(angles)
    vm = pl.BlockSpec(memory_space=pltpu.VMEM)
    hbm = pl.BlockSpec(memory_space=pl.ANY)
    V = pltpu.VMEM
    S = pltpu.SemaphoreType.DMA
    scales = ((64 + ROT_DIM) ** -0.5,) * 2 + ((128 + ROT_DIM) ** -0.5,)
    return pl.pallas_call(
        functools.partial(kernel, NZ, NX, scales),
        out_shape=jax.ShapeDtypeStruct((R, D), BF16),
        in_specs=[vm] * 5 + [hbm] * 11,
        out_specs=vm,
        scratch_shapes=[
            V((T, key_latent.shape[1]), BF16),
            V(key_weight.shape, BF16),
            V(value_weight.shape, BF16),
            V((T, 256), BF16),
            V((query_rotary.shape[1], T), BF16),
            V((ROT_DIM, T), BF16),
            V((3, NZ, NY, 2, R, F), BF16),
            V((NZ, 2, T, 640), BF16),
            V((NY, T, 384), BF16),
            V((3, NY * T, 256), BF16),
            V((256, NY * T), F32),
            V((8, NY * T), F32),
            V((8, NY * T), F32),
            V((NY, 256, T), BF16),
            V((NY, 256, T), BF16),
            V((NY, 8, T), F32),
            V((NY, 8, T), F32),
            V((NX, T, 256), BF16),
            V((NX, 2, 128, D), BF16),
            V((NX, R, D), BF16),
            V((NZ, T, 256), BF16),
            V((NZ, T, 256), BF16),
            V((T, F), F32),
            V((T, F), F32),
            V((T, F), BF16),
            V((NZ, NX, R, 256), BF16),
            V((NX, NZ, R, 256), BF16),
            S((11,)),
            S((NZ,)),
            S((NZ,)),
            S((NZ,)),
            S((NZ,)),
            S((NY,)),
            S((NY,)),
            S((NY,)),
            S((NY,)),
            S((NY,)),
            S((NY,)),
            S((NX,)),
            S((NX,)),
            S((NX,)),
            S((NX,)),
            S((NX,)),
            S((NX,)),
            S((NX,)),
            S((NX,)),
            S((NZ // 2 + 1, NX)),
            S((NZ // 2 + 1, NX)),
            S((3,)),
            S((3,)),
            S((3,)),
            S((3, NZ)),
            S((3, NZ, NY)),
            S((3, NZ)),
        ],
        compiler_params=pltpu.CompilerParams(
            collective_id=0, has_side_effects=True, vmem_limit_bytes=60 * 1024 * 1024
        ),
    )(
        cos,
        sin,
        output_gain[None, :],
        mixer_gain[None, :],
        latent_gain[None, :],
        key_latent,
        key_weight,
        value_weight,
        query_content,
        query_rotary.T,
        rotary_key.T,
        residual,
        output_weight.reshape(2, 128, D),
        gate_weight,
        up_weight,
        down_weight.T,
    )


def solution(mesh):
    placed = (
        P(("sp", "tp"), None),
        P("sp", "tp"),
        P("sp", "tp"),
        P("sp", None),
        P("sp", None),
        P(),
        P(None, "tp"),
        P(None, "tp"),
        P("tp"),
        P("tp", None),
        P(),
        P("sp", "tp"),
        P("sp", "tp"),
        P("tp", "sp"),
    )
    NZ = mesh.shape["sp"] // (2 * NY)
    NX = mesh.shape["tp"]
    return jax.shard_map(
        functools.partial(on_device, NZ, NX),
        mesh=mesh,
        in_specs=placed,
        out_specs=P(("sp", "tp"), None),
        check_vma=False,
    )
```

```python
import contextlib
import functools

import jax
import jax.numpy as jnp
from jax import lax
from jax.experimental import pallas as pl
from jax.experimental.pallas import tpu as pltpu
from jax.sharding import PartitionSpec as P

NY = 4
ROT_DIM = 32
EPS = 1e-06
ROPE_BASE = 500000.0
LOG2E = 1.4426950408889634
MESH = pl.DeviceIdType.MESH
F32 = jnp.float32
BF16 = jnp.bfloat16

PARTS = (
    "kvw1",
    "q1",
    "q2",
    "att0",
    "kvw2",
    "att1",
    "kvw3",
    "att2",
    "kvw4",
    "att3",
    "att4",
    "owait",
    "mixw",
    "widen0",
    "widen1",
    "widen2",
    "widen3",
    "widen4",
    "hid",
    "down0",
    "down1",
    "down2",
    "down3",
    "down4",
    "final",
)
PLAN = (
    (
        (("ast", 0), ("by0", 2), ("ast", 1), ("bz0", 2),),
        (),
        (("zz", 2, 1), ("zy", 2, 1),),
        (("ay", 1, 1),),
        (("wo0",),),
        (("y", 2, 1, 1), ("ay", 1, 2),),
        (),
        (("y", 2, 0, 1), ("re",), ("az0", 1),),
        (("ay", 0, 1), ("zz", 2, 2), ("zy", 2, 2),),
        (("ay", 0, 2), ("az0", 0),),
        (("wo1",), ("az", 1, 1),),
        (("az", 0, 1), ("az", 1, 2), ("wo2",),),
        (("az", 0, 2), ("y", 2, 2, 1),),
        (),
        (("y", 2, 0, 2), ("zz", 2, 3), ("zy", 2, 3),),
        (("az", 1, 3),),
        (("y", 2, 2, 2), ("az", 0, 3),),
        (("zz", 2, 4), ("zy", 2, 4), ("y", 2, 3, 1), ("az", 1, 4), ("az", 0, 4),),
        (("y", 2, 1, 2),),
        (),
        (),
        (("y", 2, 4, 1),),
        (("y", 2, 3, 2),),
        (("y", 2, 4, 2),),
        (),
    ),
    (
        (("bz0", 0), ("bz0", 1), ("by0", 2), ("bz0", 2), ("wo0",), ("by0", 1),),
        (),
        (("by0", 0), ("zz", 1, 1), ("zy", 1, 1), ("zz", 0, 1), ("zy", 0, 1),),
        (("re",),),
        (("y", 2, 0, 1), ("y", 1, 0, 1),),
        (("wo1",),),
        (("zz", 0, 2), ("zy", 0, 2), ("zz", 2, 1), ("zy", 2, 1),),
        (("zz", 2, 2), ("zy", 2, 2),),
        (("y", 0, 0, 1),),
        (("y", 1, 1, 1), ("y", 2, 1, 1),),
        (("zz", 1, 2), ("zy", 1, 2),),
        (("y", 2, 0, 2), ("zz", 0, 3), ("zy", 0, 3), ("zz", 0, 4), ("zy", 0, 4), ("y", 0, 1, 1),),
        (("y", 2, 2, 1), ("y", 1, 2, 1), ("y", 0, 2, 1), ("zz", 1, 3), ("zy", 1, 3), ("zz", 1, 4), ("zy", 1, 4), ("wo2",),),
        (("y", 0, 3, 1), ("y", 0, 4, 1), ("y", 1, 3, 1), ("y", 1, 0, 2), ("y", 0, 0, 2),),
        (("y", 0, 1, 2), ("y", 1, 1, 2),),
        (("y", 1, 4, 1), ("y", 1, 2, 2), ("y", 0, 2, 2),),
        (("y", 2, 2, 2), ("y", 2, 1, 2), ("zz", 2, 3), ("zy", 2, 3), ("zz", 2, 4), ("zy", 2, 4), ("y", 0, 3, 2), ("y", 1, 3, 2),),
        (("y", 2, 3, 1), ("y", 0, 4, 2), ("y", 1, 4, 2),),
        (("y", 2, 4, 1),),
        (),
        (("y", 2, 3, 2),),
        (),
        (),
        (("y", 2, 4, 2),),
        (),
    ),
)


def dot(a, b):
    return lax.dot_general(a, b, (((1,), (0,)), ((), ())), preferred_element_type=F32)


def dot_nt(a, b):
    return lax.dot_general(a, b, (((1,), (1,)), ((), ())), preferred_element_type=F32)


def hops(n):
    both = list(range(1, (n - 1) // 2 + 1))
    return both, (n // 2 if n % 2 == 0 and n > 1 else None)


def kernel(
    NZ,
    NX,
    scales,
    cos_ref,
    sin_ref,
    ogain_hbm,
    mgain_hbm,
    lgain_hbm,
    lat_hbm,
    kw_hbm,
    vw_hbm,
    qc_hbm,
    qr_hbm,
    rk_hbm,
    resid_hbm,
    ow_hbm,
    gate_hbm,
    up_hbm,
    down_hbm,
    out_ref,
    ogain_ref,
    mgain_ref,
    lgain_ref,
    lat_ref,
    kw_ref,
    vw_ref,
    qc_ref,
    qr_ref,
    rk_ref,
    w,
    kv,
    qall,
    qx,
    acc,
    mrow,
    lrow,
    osend,
    orecv,
    ssend,
    srecv,
    mixed,
    wo,
    resid,
    mid,
    normed,
    accg,
    accu,
    hid,
    part,
    rsum,
    small_sem,
    loc_sem,
    kv_s,
    kv_r,
    kvp_s,
    kvp_r,
    q_s,
    q_r,
    o_s,
    o_r,
    st_s,
    st_r,
    mx_s,
    mx_r,
    wo_s,
    wo_r,
    wop_s,
    wop_r,
    re_s,
    re_r,
    rs_s,
    rs_r,
    w_s1,
    w_s2,
    wp_s,
    w_r1,
    w_r2,
    wp_r,
):
    sp = lax.axis_index("sp")
    x = lax.axis_index("tp")
    c = sp % 2
    y = (sp // 2) % NY
    z = sp // (2 * NY)
    T = qc_ref.shape[0]
    R = resid.shape[1]
    D = resid.shape[2]
    phases = contextlib.ExitStack()

    def phase(name):
        phases.close()
        phases.enter_context(jax.named_scope(name))

    def dev(zz=None, yy=None, cc=None, xx=None):
        zz = z if zz is None else (zz + 2 * NZ) % NZ
        yy = y if yy is None else (yy + 2 * NY) % NY
        cc = c if cc is None else cc
        xx = x if xx is None else (xx + 2 * NX) % NX
        return ((zz * NY + yy) * 2 + cc, xx)

    def send(src, dst, ssem, rsem, device):
        pltpu.make_async_remote_copy(
            src_ref=src, dst_ref=dst, send_sem=ssem, recv_sem=rsem, device_id=device, device_id_type=MESH
        ).start()

    def arrived(ref, sem):
        pltpu.make_async_copy(ref, ref, sem).wait()

    partner = dev(cc=1 - c)
    dirc = 1 - 2 * c
    zboth, zlast = hops(NZ)
    yboth, ylast = hops(NY)
    xboth, xlast = hops(NX)

    barrier = pltpu.get_barrier_semaphore()
    peers = [partner]
    peers += [dev(zz=z + 1)] + ([dev(zz=z - 1)] if NZ > 2 else [])
    peers += [dev(yy=y + k) for k in range(1, NY)]
    peers += [dev(xx=x + k) for k in range(1, NX)]
    for p in peers:
        pl.semaphore_signal(barrier, inc=1, device_id=p, device_id_type=MESH)

    small = [
        pltpu.make_async_copy(a, b, small_sem.at[k])
        for k, (a, b) in enumerate(
            [(lat_hbm, lat_ref), (lgain_hbm, lgain_ref), (kw_hbm, kw_ref), (vw_hbm, vw_ref), (qc_hbm, qc_ref), (qr_hbm, qr_ref), (rk_hbm, rk_ref)]
        )
    ]
    loc = [
        pltpu.make_async_copy(a, b, loc_sem.at[k])
        for k, (a, b) in enumerate(
            [
                (gate_hbm, w.at[0, z, y, c]),
                (up_hbm, w.at[1, z, y, c]),
                (down_hbm, w.at[2, z, y, c]),
                (ow_hbm, wo.at[x]),
                (resid_hbm, resid.at[x]),
                (ogain_hbm, ogain_ref),
                (mgain_hbm, mgain_ref),
            ]
        )
    ]
    for d in small + loc:
        d.start()
    phase("qkv")
    for d in small:
        d.wait()
    half = ROT_DIM // 2
    cos = cos_ref[...]
    sin = sin_ref[...]

    def turned(ref, count):
        rows = []
        for h in range(count):
            a = ref[h * ROT_DIM : h * ROT_DIM + half, :].astype(F32)
            b = ref[h * ROT_DIM + half : (h + 1) * ROT_DIM, :].astype(F32)
            rows += [a * cos - b * sin, b * cos + a * sin]
        return rows

    lat = lat_ref[...].astype(F32)
    lat = lat * lax.rsqrt(jnp.mean(lat * lat, axis=-1, keepdims=True) + EPS)
    lat = (lat * lgain_ref[...]).astype(BF16)
    keys = dot(lat, kw_ref[...]).astype(BF16)
    vals = jnp.transpose(dot(lat, vw_ref[...])).astype(BF16)
    kv[0, c, :, 0:128] = keys[:, 0:128]
    kv[0, c, :, 128:256] = jnp.transpose(jnp.concatenate(turned(rk_ref, 1) * 4, axis=0)).astype(BF16)
    kv[0, c, :, 256:384] = keys[:, 128:256]
    kv[0, c, :, 384:512] = vals[0:128, :]
    kv[0, c, :, 512:640] = vals[128:256, :]

    turned_q = turned(qr_ref, 3) + [jnp.zeros((ROT_DIM, T), F32)]
    qall[0, :, 0:128] = qc_ref[:, 0:128]
    qall[0, :, 128:256] = jnp.transpose(jnp.concatenate(turned_q, axis=0)).astype(BF16)
    qall[0, :, 256:384] = qc_ref[:, 128:256]

    phase("barrier")
    pl.semaphore_wait(barrier, len(peers))

    def kv_copy(src_slot, dst_slot, device):
        send(kv.at[src_slot, c], kv.at[dst_slot, c], kv_s, kv_r.at[(dst_slot + 1) // 2], device)

    def kv_partner(slot):
        send(kv.at[slot, c], kv.at[slot, c], kvp_s, kvp_r.at[(slot + 1) // 2], partner)

    def kv_send(r):
        if r in zboth:
            kv_copy(2 * r - 3 if r > 1 else 0, 2 * r - 1, dev(zz=z + 1))
            kv_copy(2 * r - 2 if r > 1 else 0, 2 * r, dev(zz=z - 1))
        elif r == zlast:
            kv_copy((2 * r - 3 + c) if r > 1 else 0, NZ - 1, dev(zz=z + dirc))

    def slots_of(n, r):
        if r == 0:
            return [0]
        return [2 * r - 1, 2 * r] if r <= (n - 1) // 2 else [n - 1]

    def offset_of(n, slot):
        if slot == 0:
            return 0
        return slot_r(n, slot) if slot % 2 == 0 else -slot_r(n, slot)

    def slot_r(n, slot):
        return (slot + 1) // 2

    def zpos(slot):
        return (z + offset_of(NZ, slot) + 2 * NZ) % NZ

    def ypos(slot):
        return (y + offset_of(NY, slot) + 2 * NY) % NY

    def wo_send(r):
        if r in xboth:
            send(wo.at[(x - r + 1 + NX) % NX, c], wo.at[(x - r + 1 + NX) % NX, c], wo_s, wo_r.at[r], dev(xx=x + 1))
            send(wo.at[(x + r - 1) % NX, c], wo.at[(x + r - 1) % NX, c], wo_s, wo_r.at[r], dev(xx=x - 1))
        elif r == xlast:
            p = (x - dirc * (r - 1) + 2 * NX) % NX
            send(wo.at[p, c], wo.at[p, c], wo_s, wo_r.at[r], dev(xx=x + dirc))

    def wo_wait(r):
        arrived(wo.at[pl.ds(0, len(slots_of(NX, r))), c], wo_r.at[r])
        for slot in slots_of(NX, r):
            p = (x + offset_of(NX, slot) + 2 * NX) % NX
            send(wo.at[p, c], wo.at[p, c], wop_s, wop_r, partner)

    def zdir(m):
        return dirc * (1 - 2 * (m % 2))

    def ring_y(m, zz, cc, r, ssem, rsem):
        if r in yboth:
            a, b = (y - r + 1 + NY) % NY, (y + r - 1) % NY
            send(w.at[m, zz, a, cc], w.at[m, zz, a, cc], ssem, rsem, dev(yy=y + 1))
            send(w.at[m, zz, b, cc], w.at[m, zz, b, cc], ssem, rsem, dev(yy=y - 1))
        elif r == ylast:
            p = (y - zdir(m) * (r - 1) + 2 * NY) % NY
            send(w.at[m, zz, p, cc], w.at[m, zz, p, cc], ssem, rsem, dev(yy=y + zdir(m)))

    def ring_z(m, view, r, ssem, rsem):
        if r in zboth:
            a, b = (z - r + 1 + NZ) % NZ, (z + r - 1) % NZ
            send(view(a), view(a), ssem, rsem, dev(zz=z + 1))
            send(view(b), view(b), ssem, rsem, dev(zz=z - 1))
        elif r == zlast:
            p = (z - zdir(m) * (r - 1) + 2 * NZ) % NZ
            send(view(p), view(p), ssem, rsem, dev(zz=z + zdir(m)))

    def a1_send(m, r):
        ring_y(m, z, 0, r, w_s1.at[m], w_r1.at[m, r])

    def a1_wait(m, r):
        arrived(w.at[m, 0, pl.ds(0, len(slots_of(NY, r))), 0], w_r1.at[m, r])

    def a_block(m, zz):
        return w.at[m, zz, :, 0]

    def a2_send(m, r):
        ring_z(m, lambda p: a_block(m, p), r, w_s2.at[m], w_r2.at[m, r, 0])

    def a_partner(m, slot):
        p = zpos(slot)
        send(a_block(m, p), a_block(m, p), wp_s.at[m], wp_r.at[m, (slot + 1) // 2], partner)

    def a2_wait(m, r):
        arrived(w.at[m, pl.ds(0, len(slots_of(NZ, r))), :, 0], w_r2.at[m, r, 0])

    def b1_send(m, r):
        ring_z(m, lambda p: w.at[m, p, y, c], r, w_s1.at[m], w_r1.at[m, r])

    def b1_wait(m, r):
        arrived(w.at[m, pl.ds(0, len(slots_of(NZ, r))), 0, 0], w_r1.at[m, r])

    def b2_send(m, slot, r):
        ring_y(m, zpos(slot), c, r, w_s2.at[m], w_r2.at[m, (slot + 1) // 2, r - 1])

    def b_partner(m, slot, yslot):
        p = w.at[m, zpos(slot), ypos(yslot), c]
        send(p, p, wp_s.at[m], wp_r.at[m, (slot + 1) // 2], partner)

    RZ = NZ // 2
    RY = NY // 2

    def b_first_y(m):
        b2_send(m, 0, 1)
        b_partner(m, 0, 0)

    def b_z(m, r):
        b1_wait(m, r)
        if r < RZ:
            b1_send(m, r + 1)

    def b_zy(m, r):
        for slot in slots_of(NZ, r):
            b2_send(m, slot, 1)
            b_partner(m, slot, 0)

    def b_y(m, r, k):
        arrived(w.at[m, pl.ds(0, len(slots_of(NZ, r))), pl.ds(0, len(slots_of(NY, k))), 0], w_r2.at[m, r, k - 1])
        for slot in slots_of(NZ, r):
            if k < RY:
                b2_send(m, slot, k + 1)
            for yslot in slots_of(NY, k):
                b_partner(m, slot, yslot)

    def a_y(m, k):
        a1_wait(m, k)
        if k < RY:
            a1_send(m, k + 1)

    def a_z(m, r):
        a2_wait(m, r)
        if r < RZ:
            a2_send(m, r + 1)
        for slot in slots_of(NZ, r):
            a_partner(m, slot)

    def a_first_z(m):
        a2_send(m, 1)
        a_partner(m, 0)

    def resid_send():
        for k in range(1, NX):
            send(resid.at[x], resid.at[x], re_s, re_r, dev(xx=x + k))

    def wo_pass(r):
        wo_wait(r)
        if r < NX // 2:
            wo_send(r + 1)

    steps = {
        "ast": lambda m: a1_send(m, 1),
        "ay": a_y,
        "az0": a_first_z,
        "az": a_z,
        "bz0": lambda m: b1_send(m, 1),
        "by0": b_first_y,
        "zz": b_z,
        "zy": b_zy,
        "y": b_y,
        "wo0": lambda: wo_send(1),
        "wo1": lambda: wo_pass(1),
        "wo2": lambda: wo_pass(2),
        "re": resid_send,
    }

    def on(core, *todo):
        def run():
            for f, *a in todo:
                steps[f](*a)

        pl.when(c == core)(run)

    def gap(name):
        phase("g_" + name)
        at = PARTS.index(name)
        for core in (0, 1):
            if PLAN[core][at]:
                on(core, *PLAN[core][at])

    phase("send0")

    def q_send(r):
        if r in yboth:
            left = 0 if r == 1 else offset_of(NY, 2 * r - 3) % NY
            right = 0 if r == 1 else offset_of(NY, 2 * r - 2) % NY
            send(qall.at[left], qall.at[(-r) % NY], q_s, q_r.at[r], dev(yy=y + 1))
            send(qall.at[right], qall.at[r], q_s, q_r.at[r], dev(yy=y - 1))
        elif r == ylast:
            member = 0 if r == 1 else (-dirc * (r - 1) + NY) % NY
            send(qall.at[member], qall.at[r], q_s, q_r.at[r], dev(yy=y + dirc))

    kv_send(1)
    kv_partner(0)
    q_send(1)
    for d in loc:
        d.wait()

    lane = lax.broadcasted_iota(jnp.int32, (T, 256), 1)
    own0 = (lane < 64) | ((lane >= 128) & (lane < 160))
    own1 = ((lane >= 64) & (lane < 128)) | ((lane >= 160) & (lane < 192))
    own2 = ((lane >= 64) & (lane < 96)) | (lane >= 128)

    def spread(k):
        narrow = qall[k, :, 0:256]
        wide = qall[k, :, 128:384]
        zero = jnp.zeros_like(narrow)
        qx[0, k * T : (k + 1) * T, :] = jnp.where(own0, narrow, zero)
        qx[1, k * T : (k + 1) * T, :] = jnp.where(own1, narrow, zero)
        qx[2, k * T : (k + 1) * T, :] = jnp.where(own2, wide, zero)

    def kv_wait(r):
        phase(f"kvw#r={r}")
        ring = slots_of(NZ, r)
        arrived(kv.at[pl.ds(ring[0], len(ring)), c], kv_r.at[r])
        if r < RZ:
            kv_send(r + 1)
        for slot in slots_of(NZ, r):
            kv_partner(slot)

    phase("spread0")
    spread(0)
    mrow[...] = jnp.full_like(mrow, -1e30)
    lrow[...] = jnp.zeros_like(lrow)
    acc[...] = jnp.zeros_like(acc)
    def q_wait(r):
        phase(f"qw#r={r}")
        arrived(qall.at[pl.ds(0, len(slots_of(NY, r)))], q_r.at[r])
        if r < RY:
            q_send(r + 1)
        for slot in slots_of(NY, r):
            spread(offset_of(NY, slot) % NY)

    gap("kvw1")
    kv_wait(1)
    gap("q1")
    q_wait(1)
    gap("q2")
    for r in range(2, RY + 1):
        q_wait(r)

    QB = min(256, NY * T)
    head_rows = ((0, 64), (64, 128), (128, 256))

    def attend(first, count):
        nk = count * 2 * T
        k_narrow = kv[first : first + count, :, :, 0:256].reshape(nk, 256)
        k_wide = kv[first : first + count, :, :, 128:384].reshape(nk, 256)

        def values(h):
            lo, hi = ((384, 512), (384, 512), (512, 640))[h]
            r0, r1 = ((0, 64), (64, 128), (0, 128))[h]
            return jnp.concatenate(
                [kv[first + s, cc, r0:r1, lo:hi] for s in range(count) for cc in range(2)], axis=1
            )

        def block(b, carry):
            cols = pl.ds(pl.multiple_of(b * QB, QB), QB)
            for h in range(3):
                s = dot_nt(k_narrow if h < 2 else k_wide, qx[h, cols, :]) * (scales[h] * LOG2E)
                old = mrow[h : h + 1, cols]
                new = jnp.maximum(old, jnp.max(s, axis=0, keepdims=True))
                shrink = jnp.exp2(old - new)
                p = jnp.exp2(s - new)
                lrow[h : h + 1, cols] = lrow[h : h + 1, cols] * shrink + jnp.sum(p, axis=0, keepdims=True)
                mrow[h : h + 1, cols] = new
                r0, r1 = head_rows[h]
                acc[r0:r1, cols] = acc[r0:r1, cols] * shrink + dot(values(h), p.astype(BF16))
            return carry

        lax.fori_loop(0, NY * T // QB, block, 0)

    def att(r):
        phase(f"attw#r={r}")
        ring = slots_of(NZ, r)
        arrived(kv.at[pl.ds(ring[0], len(ring)), 1 - c], kvp_r.at[r])
        phase(f"att#r={r}")
        attend(ring[0], len(ring))

    gap("att0")
    att(0)
    for r in range(1, RZ + 1):
        if r < RZ:
            gap(f"kvw{r + 1}")
            kv_wait(r + 1)
        gap(f"att{r}")
        att(r)

    phase("osend")
    for k in range(NY):
        cols = slice(k * T, (k + 1) * T)
        osend[k] = acc[:, cols].astype(BF16)
        ssend[k, 0:3] = mrow[0:3, cols]
        ssend[k, 3:6] = lrow[0:3, cols]
        ssend[k, 6:8] = jnp.zeros((2, T), F32)
    for k in range(1, NY):
        send(osend.at[k], orecv.at[NY - k], o_s, o_r, dev(yy=y + k))
        send(ssend.at[k], srecv.at[NY - k], st_s, st_r, dev(yy=y + k))
    gap("owait")
    phase("owait")
    arrived(orecv.at[pl.ds(1, NY - 1)], o_r)
    arrived(srecv.at[pl.ds(1, NY - 1)], st_r)
    phase("merge")
    ms = [ssend[0, 0:3]] + [srecv[k, 0:3] for k in range(1, NY)]
    ls = [ssend[0, 3:6]] + [srecv[k, 3:6] for k in range(1, NY)]
    top = functools.reduce(jnp.maximum, ms)
    ws = [jnp.exp2(m - top) for m in ms]
    total = sum(a * b for a, b in zip(ws, ls))
    outs = []
    for h in range(3):
        r0, r1 = head_rows[h]
        o = acc[r0:r1, 0:T] * ws[0][h : h + 1]
        for k in range(1, NY):
            o = o + orecv[k, r0:r1].astype(F32) * ws[k][h : h + 1]
        o = o / total[h : h + 1]
        outs.append(o * lax.rsqrt(jnp.mean(o * o, axis=0, keepdims=True) + EPS))
    heads = jnp.transpose(jnp.concatenate(outs, axis=0))
    mixed[x] = (heads * ogain_ref[...]).astype(BF16)
    for k in range(1, NX):
        send(mixed.at[x], mixed.at[x], mx_s, mx_r, dev(xx=x + k))
    gap("mixw")
    phase("mixw")
    arrived(mixed.at[pl.ds(0, NX - 1)], mx_r)
    arrived(resid.at[pl.ds(0, NX - 1)], re_r)
    arrived(wo.at[pl.ds(0, NX - 1), 0], wop_r)
    phase("proj")
    mixed_all = jnp.concatenate([mixed[k] for k in range(NX)], axis=1)

    def project(n, squares):
        cols = pl.ds(pl.multiple_of(n * 256, 256), 256)
        s = dot(mixed_all, wo[:, :, :, cols].reshape(NX * 256, 256))
        s = (s + resid[:, :, cols].reshape(T, 256).astype(F32)).astype(BF16)
        mid[n] = s
        s = s.astype(F32)
        return squares + jnp.sum(s * s, axis=1, keepdims=True)

    squares = lax.fori_loop(0, D // 256, project, jnp.zeros((T, 1), F32))
    factor = lax.rsqrt(squares / D + EPS)

    def scale(n, carry):
        cols = pl.ds(pl.multiple_of(n * 256, 256), 256)
        normed[n] = (mid[n].astype(F32) * factor * mgain_ref[:, cols]).astype(BF16)
        return carry

    lax.fori_loop(0, D // 256, scale, 0)

    phase("mlp0")
    def from_partner(m, r):
        arrived(w.at[m, pl.ds(0, len(slots_of(NZ, r))), :, 0], wp_r.at[m, r])

    accg[...] = jnp.zeros_like(accg)
    accu[...] = jnp.zeros_like(accu)
    F = accg.shape[1]

    def widen(k):
        from_partner(0, k)
        from_partner(1, k)
        ring = slots_of(NZ, k)

        def one(i, carry):
            step = 0 if k == 0 else (k if len(ring) == 1 else (2 * i - 1) * k)
            p = (z + step + 2 * NZ) % NZ
            n = normed[p]
            accg[...] += dot(n, w[0, p].reshape(256, F))
            accu[...] += dot(n, w[1, p].reshape(256, F))
            return carry

        lax.fori_loop(0, len(ring), one, 0)

    for r in range(RZ + 1):
        gap(f"widen{r}")
        phase(f"widen#r={r}")
        widen(r)
    gap("hid")
    phase("hid")
    g = accg[...]
    hid[...] = (g / (1.0 + jnp.exp(-g)) * accu[...]).astype(BF16)

    def narrow(slot, carry):
        p = (z + ((slot + 1) // 2) * (1 - 2 * (slot % 2)) + 2 * NZ) % NZ
        s = dot_nt(hid[...], w[2, p].reshape(256, F)).astype(BF16)
        part[slot] = s.reshape(NX, R, 256)
        return carry

    def sums_rows(r):
        ring = slots_of(NZ, r)
        return pl.ds(ring[0], len(ring))

    for r in range(RZ + 1):
        gap(f"down{r}")
        phase(f"down#r={r}")
        ring = slots_of(NZ, r)
        from_partner(2, r)
        lax.fori_loop(ring[0], ring[0] + len(ring), narrow, 0)
        rows = sums_rows(r)
        for k in range(1, NX):
            p = (x + k) % NX
            send(part.at[rows, p], rsum.at[NX - k, rows], rs_s, rs_r.at[r], dev(xx=x + k))
    gap("final")
    phase("final")
    for r in range(RZ + 1):
        arrived(rsum.at[pl.ds(1, NX - 1), sums_rows(r)], rs_r.at[r])
        for slot in slots_of(NZ, r):
            p = zpos(slot)
            s = part[slot, x].astype(F32)
            for k in range(1, NX):
                s = s + rsum[k, slot].astype(F32)
            s = s + mid[p, pl.ds(pl.multiple_of(x * R, R), R), :].astype(F32)
            out_ref[:, pl.ds(pl.multiple_of(p * 256, 256), 256)] = s.astype(BF16)

    phase("sendw")
    arrived(kv.at[pl.ds(0, NZ - 1), 0], kv_s)
    arrived(kv.at[:, 0], kvp_s)
    arrived(qall.at[pl.ds(0, NY - 1)], q_s)
    arrived(osend.at[pl.ds(1, NY - 1)], o_s)
    arrived(ssend.at[pl.ds(1, NY - 1)], st_s)
    arrived(mixed.at[pl.ds(0, NX - 1)], mx_s)
    arrived(wo.at[pl.ds(0, NX - 1), 0], wo_s)
    arrived(wo.at[pl.ds(0, NX - 1), 0], wop_s)
    arrived(resid.at[pl.ds(0, NX - 1)], re_s)
    arrived(part.at[:, pl.ds(0, NX - 1)], rs_s)

    def sent_a(m):
        arrived(w.at[m, 0, pl.ds(0, NY - 1), 0], w_s1.at[m])
        arrived(w.at[m, pl.ds(0, NZ - 1), :, 0], w_s2.at[m])
        arrived(w.at[m, :, :, 0], wp_s.at[m])

    def sent_b(m):
        arrived(w.at[m, pl.ds(0, NZ - 1), 0, 1], w_s1.at[m])
        arrived(w.at[m, :, pl.ds(0, NY - 1), 1], w_s2.at[m])
        arrived(w.at[m, :, :, 1], wp_s.at[m])

    @pl.when(c == 0)
    def _():
        sent_a(0)
        sent_a(1)

    @pl.when(c == 1)
    def _():
        sent_b(0)
        sent_b(1)

    sent_b(2)

    phases.close()


def on_device(
    NZ,
    NX,
    residual,
    query_content,
    query_rotary,
    key_latent,
    rotary_key,
    latent_gain,
    key_weight,
    value_weight,
    output_gain,
    output_weight,
    mixer_gain,
    gate_weight,
    up_weight,
    down_weight,
):
    T = key_latent.shape[0]
    R, D = residual.shape
    F = gate_weight.shape[1]
    positions = lax.axis_index("sp") * T + lax.iota(jnp.int32, T)
    power = jnp.arange(0, ROT_DIM, 2, dtype=F32) / ROT_DIM
    inverse = 1.0 / jnp.power(ROPE_BASE, power)
    angles = positions.astype(F32)[None, :] * inverse[:, None]
    cos = jnp.cos(angles)
    sin = jnp.sin(angles)
    vm = pl.BlockSpec(memory_space=pltpu.VMEM)
    hbm = pl.BlockSpec(memory_space=pl.ANY)
    V = pltpu.VMEM

    def pin(a):
        return pltpu.with_memory_space_constraint(a, pltpu.HBM)

    S = pltpu.SemaphoreType.DMA
    RZ = NZ // 2
    scales = ((64 + ROT_DIM) ** -0.5,) * 2 + ((128 + ROT_DIM) ** -0.5,)
    return pl.pallas_call(
        functools.partial(kernel, NZ, NX, scales),
        out_shape=jax.ShapeDtypeStruct((R, D), BF16),
        in_specs=[vm] * 2 + [hbm] * 14,
        out_specs=vm,
        scratch_shapes=[
            V((1, output_gain.shape[0]), F32),
            V((1, D), F32),
            V((1, key_latent.shape[1]), F32),
            V((T, key_latent.shape[1]), BF16),
            V(key_weight.shape, BF16),
            V(value_weight.shape, BF16),
            V((T, 256), BF16),
            V((query_rotary.shape[1], T), BF16),
            V((ROT_DIM, T), BF16),
            V((3, NZ, NY, 2, R, F), BF16),
            V((NZ, 2, T, 640), BF16),
            V((NY, T, 384), BF16),
            V((3, NY * T, 256), BF16),
            V((256, NY * T), F32),
            V((8, NY * T), F32),
            V((8, NY * T), F32),
            V((NY, 256, T), BF16),
            V((NY, 256, T), BF16),
            V((NY, 8, T), F32),
            V((NY, 8, T), F32),
            V((NX, T, 256), BF16),
            V((NX, 2, 128, D), BF16),
            V((NX, R, D), BF16),
            V((NZ, T, 256), BF16),
            V((NZ, T, 256), BF16),
            V((T, F), F32),
            V((T, F), F32),
            V((T, F), BF16),
            V((NZ, NX, R, 256), BF16),
            V((NX, NZ, R, 256), BF16),
            S((7,)),
            S((7,)),
            S(()),
            S((RZ + 1,)),
            S(()),
            S((RZ + 1,)),
            S(()),
            S((NY // 2 + 1,)),
            S(()),
            S(()),
            S(()),
            S(()),
            S(()),
            S(()),
            S(()),
            S((NX // 2 + 1,)),
            S(()),
            S(()),
            S(()),
            S(()),
            S(()),
            S((RZ + 1,)),
            S((3,)),
            S((3,)),
            S((3,)),
            S((3, RZ + 1)),
            S((3, RZ + 1, 2)),
            S((3, RZ + 1)),
        ],
        compiler_params=pltpu.CompilerParams(
            collective_id=0, has_side_effects=True, vmem_limit_bytes=44 * 1024 * 1024
        ),
    )(
        cos,
        sin,
        pin(output_gain[None, :]),
        pin(mixer_gain[None, :]),
        pin(latent_gain[None, :]),
        pin(key_latent),
        pin(key_weight),
        pin(value_weight),
        pin(query_content),
        pin(query_rotary.T),
        pin(rotary_key.T),
        pin(residual),
        pin(output_weight.reshape(2, 128, D)),
        pin(gate_weight),
        pin(up_weight),
        pin(down_weight.T),
    )


def solution(mesh):
    placed = (
        P(("sp", "tp"), None),
        P("sp", "tp"),
        P("sp", "tp"),
        P("sp", None),
        P("sp", None),
        P(),
        P(None, "tp"),
        P(None, "tp"),
        P("tp"),
        P("tp", None),
        P(),
        P("sp", "tp"),
        P("sp", "tp"),
        P("tp", "sp"),
    )
    NZ = mesh.shape["sp"] // (2 * NY)
    NX = mesh.shape["tp"]
    return jax.shard_map(
        functools.partial(on_device, NZ, NX),
        mesh=mesh,
        in_specs=placed,
        out_specs=P(("sp", "tp"), None),
        check_vma=False,
    )
```

```python
import contextlib
import functools

import jax
import jax.numpy as jnp
from jax import lax
from jax.experimental import pallas as pl
from jax.experimental.pallas import tpu as pltpu
from jax.sharding import PartitionSpec as P

NY = 4
ROT_DIM = 32
EPS = 1e-06
ROPE_BASE = 500000.0
LOG2E = 1.4426950408889634
MESH = pl.DeviceIdType.MESH
F32 = jnp.float32
BF16 = jnp.bfloat16

Y_FIRST = ((0, 1, 2), (2,))
ZDIR = ((1, -1, -1, -1), (-1, 1, 1, -1))
PARTS = (
    "kvw1",
    "kvw2",
    "q1",
    "q2",
    "kvw3",
    "kx1",
    "att0",
    "kvw4",
    "kx2",
    "att1",
    "kx3",
    "att2",
    "kx4",
    "att3",
    "att4",
    "owait",
    "mixw",
    "widen0",
    "widen1",
    "widen2",
    "widen3",
    "widen4",
    "hid",
    "down0",
    "down1",
    "down2",
    "down3",
    "down4",
    "final",
)
PLAN = (
    (
        (("ast", 1), ("ast", 0), ("re",),),
        (("ast", 2), ("by0", 3), ("bz0", 3), ("ay", 1, 1),),
        (("ay", 0, 1), ("zz", 3, 1),),
        (("ay", 1, 2), ("az0", 1),),
        (),
        (("ay", 0, 2), ("wo0",),),
        (("az0", 0), ("ay", 2, 1),),
        (("zz", 3, 2),),
        (),
        (("ay", 2, 2), ("az0", 2),),
        (("zy", 3, 2),),
        (("az", 0, 1),),
        (("az", 2, 1),),
        (),
        (("az", 1, 1), ("wo1",),),
        (("y", 3, 0, 1), ("az", 0, 2), ("y", 3, 2, 1), ("az", 2, 2), ("az", 1, 2), ("zz", 3, 3), ("zy", 3, 3),),
        (("az", 0, 3), ("zy", 3, 1), ("az", 2, 3), ("wo2",),),
        (("az", 1, 3),),
        (("zz", 3, 4), ("zy", 3, 4),),
        (("y", 3, 1, 1),),
        (("y", 3, 3, 1),),
        (("az", 2, 4), ("az", 0, 4), ("az", 1, 4),),
        (("y", 3, 4, 1),),
        (("y", 3, 0, 2),),
        (("y", 3, 1, 2),),
        (("y", 3, 2, 2),),
        (("y", 3, 3, 2),),
        (("y", 3, 4, 2),),
        (),
    ),
    (
        (("bz0", 1), ("ast", 2), ("bz0", 3), ("re",), ("bz0", 0),),
        (("zz", 1, 1), ("zz", 3, 1), ("zy", 3, 1), ("zz", 0, 1), ("by0", 3),),
        (),
        (("zz", 1, 2), ("zy", 1, 2), ("zz", 0, 2), ("zy", 0, 1), ("zz", 3, 2), ("zy", 3, 2), ("ay", 2, 1),),
        (("zy", 1, 1),),
        (("zz", 1, 3), ("zy", 1, 3), ("y", 1, 2, 1),),
        (("by0", 0), ("zy", 0, 2), ("y", 3, 0, 1), ("by0", 1),),
        (("zz", 0, 3), ("zz", 0, 4),),
        (("y", 0, 1, 1), ("ay", 2, 2), ("az0", 2),),
        (("zz", 1, 4), ("zy", 1, 4),),
        (("wo0",), ("y", 1, 1, 1),),
        (("zy", 0, 3), ("y", 0, 0, 1), ("y", 1, 2, 2),),
        (("az", 2, 1), ("y", 3, 1, 1),),
        (("y", 1, 3, 1), ("y", 1, 0, 1), ("zy", 0, 4), ("y", 0, 2, 1), ("y", 0, 1, 2), ("y", 1, 4, 1),),
        (("y", 0, 0, 2), ("y", 0, 3, 1), ("y", 1, 3, 2), ("y", 3, 1, 2), ("wo1",),),
        (("y", 3, 2, 1), ("az", 2, 2), ("az", 2, 3), ("wo2",), ("y", 0, 4, 1), ("y", 0, 2, 2), ("y", 1, 0, 2),),
        (("y", 0, 3, 2), ("y", 1, 4, 2), ("y", 1, 1, 2), ("y", 3, 2, 2), ("zz", 3, 3), ("zy", 3, 3), ("zz", 3, 4), ("zy", 3, 4), ("y", 0, 4, 2),),
        (("y", 3, 0, 2),),
        (("az", 2, 4), ("y", 3, 3, 1),),
        (("y", 3, 4, 1),),
        (),
        (),
        (),
        (),
        (),
        (("y", 3, 3, 2),),
        (("y", 3, 4, 2),),
        (),
        (),
    ),
)


def dot(a, b):
    return lax.dot_general(a, b, (((1,), (0,)), ((), ())), preferred_element_type=F32)


def dot_nt(a, b):
    return lax.dot_general(a, b, (((1,), (1,)), ((), ())), preferred_element_type=F32)


def hops(n):
    both = list(range(1, (n - 1) // 2 + 1))
    return both, (n // 2 if n % 2 == 0 and n > 1 else None)


def kernel(
    NZ,
    NX,
    scales,
    cos_ref,
    sin_ref,
    ogain_hbm,
    mgain_hbm,
    lgain_hbm,
    lat_hbm,
    kw_hbm,
    vw_hbm,
    qc_hbm,
    qr_hbm,
    rk_hbm,
    resid_hbm,
    ow_hbm,
    gate_hbm,
    up_hbm,
    down_hbm,
    out_ref,
    ogain_ref,
    mgain_ref,
    lgain_ref,
    lat_ref,
    kw_ref,
    vw_ref,
    qc_ref,
    qr_ref,
    rk_ref,
    w,
    lats,
    vwt,
    k_narrow,
    k_wide,
    v_turned,
    qall,
    qx,
    acc,
    mrow,
    lrow,
    osend,
    orecv,
    ssend,
    srecv,
    mixed,
    wo,
    resid,
    mid,
    normed,
    accg,
    accu,
    hid,
    part,
    rsum,
    small_sem,
    loc_sem,
    kv_s,
    kv_r,
    kvp_s,
    kvp_r,
    kx_s,
    kx_r,
    q_s,
    q_r,
    o_s,
    o_r,
    st_s,
    st_r,
    mx_s,
    mx_r,
    wo_s,
    wo_r,
    wop_s,
    wop_r,
    re_s,
    re_r,
    rs_s,
    rs_r,
    w_s1,
    w_s2,
    wp_s,
    w_r1,
    w_r2,
    wp_r,
):
    sp = lax.axis_index("sp")
    x = lax.axis_index("tp")
    c = sp % 2
    y = (sp // 2) % NY
    z = sp // (2 * NY)
    T = qc_ref.shape[0]
    R = resid.shape[1]
    D = resid.shape[2]
    phases = contextlib.ExitStack()

    def phase(name):
        phases.close()
        phases.enter_context(jax.named_scope(name))

    def dev(zz=None, yy=None, cc=None, xx=None):
        zz = z if zz is None else (zz + 2 * NZ) % NZ
        yy = y if yy is None else (yy + 2 * NY) % NY
        cc = c if cc is None else cc
        xx = x if xx is None else (xx + 2 * NX) % NX
        return ((zz * NY + yy) * 2 + cc, xx)

    def send(src, dst, ssem, rsem, device):
        pltpu.make_async_remote_copy(
            src_ref=src, dst_ref=dst, send_sem=ssem, recv_sem=rsem, device_id=device, device_id_type=MESH
        ).start()

    def arrived(ref, sem):
        pltpu.make_async_copy(ref, ref, sem).wait()

    partner = dev(cc=1 - c)
    dirc = 1 - 2 * c
    zboth, zlast = hops(NZ)
    yboth, ylast = hops(NY)
    xboth, xlast = hops(NX)

    barrier = pltpu.get_barrier_semaphore()
    peers = [partner]
    peers += [dev(zz=z + 1)] + ([dev(zz=z - 1)] if NZ > 2 else [])
    peers += [dev(yy=y + k) for k in range(1, NY)]
    peers += [dev(xx=x + k) for k in range(1, NX)]
    for p in peers:
        pl.semaphore_signal(barrier, inc=1, device_id=p, device_id_type=MESH)

    small = [
        pltpu.make_async_copy(a, b, small_sem.at[k])
        for k, (a, b) in enumerate(
            [(lat_hbm, lat_ref), (lgain_hbm, lgain_ref), (kw_hbm, kw_ref), (vw_hbm, vw_ref), (qc_hbm, qc_ref), (qr_hbm, qr_ref), (rk_hbm, rk_ref)]
        )
    ]
    loc = [
        pltpu.make_async_copy(a, b, loc_sem.at[k])
        for k, (a, b) in enumerate(
            [
                (gate_hbm, w.at[0, z, y, c]),
                (up_hbm, w.at[1, z, y, c]),
                (down_hbm, w.at[2, z, y, c]),
                (ow_hbm, wo.at[x]),
                (resid_hbm, resid.at[x]),
                (ogain_hbm, ogain_ref),
                (mgain_hbm, mgain_ref),
            ]
        )
    ]
    for d in small + loc:
        d.start()
    phase("qkv")
    for d in small:
        d.wait()
    half = ROT_DIM // 2
    cos = cos_ref[...]
    sin = sin_ref[...]

    def turned(ref, count):
        rows = []
        for h in range(count):
            a = ref[h * ROT_DIM : h * ROT_DIM + half, :].astype(F32)
            b = ref[h * ROT_DIM + half : (h + 1) * ROT_DIM, :].astype(F32)
            rows += [a * cos - b * sin, b * cos + a * sin]
        return rows

    lat = lat_ref[...].astype(F32)
    lat = lat * lax.rsqrt(jnp.mean(lat * lat, axis=-1, keepdims=True) + EPS)
    lat = (lat * lgain_ref[...]).astype(BF16)
    L = lat.shape[1]
    lats[0, c, :, :, 0:L] = lat.reshape(NX, T // NX, L)
    rot = jnp.transpose(jnp.concatenate(turned(rk_ref, 1) * 4, axis=0)).astype(BF16)
    lats[0, c, :, :, L : L + 128] = rot.reshape(NX, T // NX, 128)

    turned_q = turned(qr_ref, 3) + [jnp.zeros((ROT_DIM, T), F32)]
    qall[0, :, 0:128] = qc_ref[:, 0:128]
    qall[0, :, 128:256] = jnp.transpose(jnp.concatenate(turned_q, axis=0)).astype(BF16)
    qall[0, :, 256:384] = qc_ref[:, 128:256]

    phase("barrier")
    pl.semaphore_wait(barrier, len(peers))

    def kv_copy(src_slot, dst_slot, device):
        send(lats.at[src_slot, c, x], lats.at[dst_slot, c, x], kv_s, kv_r.at[(dst_slot + 1) // 2], device)

    def kv_partner(slot):
        send(lats.at[slot, c], lats.at[slot, c], kvp_s, kvp_r.at[(slot + 1) // 2], partner)

    def kv_send(r):
        if r in zboth:
            kv_copy(2 * r - 3 if r > 1 else 0, 2 * r - 1, dev(zz=z + 1))
            kv_copy(2 * r - 2 if r > 1 else 0, 2 * r, dev(zz=z - 1))
        elif r == zlast:
            kv_copy((2 * r - 3 + c) if r > 1 else 0, NZ - 1, dev(zz=z + dirc))

    def slots_of(n, r):
        if r == 0:
            return [0]
        return [2 * r - 1, 2 * r] if r <= (n - 1) // 2 else [n - 1]

    def offset_of(n, slot):
        if slot == 0:
            return 0
        return slot_r(n, slot) if slot % 2 == 0 else -slot_r(n, slot)

    def slot_r(n, slot):
        return (slot + 1) // 2

    def zpos(slot):
        return (z + offset_of(NZ, slot) + 2 * NZ) % NZ

    def ypos(slot):
        return (y + offset_of(NY, slot) + 2 * NY) % NY

    def wo_send(r):
        if r in xboth:
            send(wo.at[(x - r + 1 + NX) % NX, c], wo.at[(x - r + 1 + NX) % NX, c], wo_s, wo_r.at[r], dev(xx=x + 1))
            send(wo.at[(x + r - 1) % NX, c], wo.at[(x + r - 1) % NX, c], wo_s, wo_r.at[r], dev(xx=x - 1))
        elif r == xlast:
            p = (x - dirc * (r - 1) + 2 * NX) % NX
            send(wo.at[p, c], wo.at[p, c], wo_s, wo_r.at[r], dev(xx=x + dirc))

    def wo_wait(r):
        arrived(wo.at[pl.ds(0, len(slots_of(NX, r))), c], wo_r.at[r])
        for slot in slots_of(NX, r):
            p = (x + offset_of(NX, slot) + 2 * NX) % NX
            send(wo.at[p, c], wo.at[p, c], wop_s, wop_r, partner)

    cut = w.shape[5] // 256 * 128
    units = ((0, 0, w.shape[5]), (1, 0, cut), (1, cut, w.shape[5]), (2, 0, w.shape[5]))
    core = [0]

    def piece(u, zz, yy, cc):
        mat, lo, hi = units[u]
        return w.at[mat, zz, yy, cc, :, lo:hi]

    def some(u, nz, ny):
        return piece(u, pl.ds(0, nz), pl.ds(0, ny), 0)

    def ring_y(u, zz, r, d, ssem, rsem):
        if r in yboth:
            a, b = (y - r + 1 + NY) % NY, (y + r - 1) % NY
            send(piece(u, zz, a, core[0]), piece(u, zz, a, core[0]), ssem, rsem, dev(yy=y + 1))
            send(piece(u, zz, b, core[0]), piece(u, zz, b, core[0]), ssem, rsem, dev(yy=y - 1))
        elif r == ylast:
            p = (y - d * (r - 1) + 2 * NY) % NY
            send(piece(u, zz, p, core[0]), piece(u, zz, p, core[0]), ssem, rsem, dev(yy=y + d))

    def ring_z(u, yy, r, ssem, rsem):
        d = ZDIR[core[0]][u]
        if r in zboth:
            a, b = (z - r + 1 + NZ) % NZ, (z + r - 1) % NZ
            send(piece(u, a, yy, core[0]), piece(u, a, yy, core[0]), ssem, rsem, dev(zz=z + 1))
            send(piece(u, b, yy, core[0]), piece(u, b, yy, core[0]), ssem, rsem, dev(zz=z - 1))
        elif r == zlast:
            p = (z - d * (r - 1) + 2 * NZ) % NZ
            send(piece(u, p, yy, core[0]), piece(u, p, yy, core[0]), ssem, rsem, dev(zz=z + d))

    every = pl.ds(0, NY)

    def a1_send(u, r):
        ring_y(u, z, r, ZDIR[core[0]][u], w_s1.at[u], w_r1.at[u, r])

    def a1_wait(u, r):
        arrived(some(u, 1, len(slots_of(NY, r))), w_r1.at[u, r])

    def a2_send(u, r):
        ring_z(u, every, r, w_s2.at[u], w_r2.at[u, r, 0])

    def a_partner(u, slot):
        p = piece(u, zpos(slot), every, core[0])
        send(p, p, wp_s.at[u], wp_r.at[u, (slot + 1) // 2], partner)

    def a2_wait(u, r):
        arrived(some(u, len(slots_of(NZ, r)), NY), w_r2.at[u, r, 0])

    def b1_send(u, r):
        ring_z(u, y, r, w_s1.at[u], w_r1.at[u, r])

    def b1_wait(u, r):
        arrived(some(u, len(slots_of(NZ, r)), 1), w_r1.at[u, r])

    def b2_send(u, slot, r):
        d = (1 - 2 * core[0]) * (1 - 2 * (slot % 2))
        ring_y(u, zpos(slot), r, d, w_s2.at[u], w_r2.at[u, (slot + 1) // 2, r - 1])

    def b_partner(u, slot, yslot):
        p = piece(u, zpos(slot), ypos(yslot), core[0])
        send(p, p, wp_s.at[u], wp_r.at[u, (slot + 1) // 2], partner)

    RZ = NZ // 2
    RY = NY // 2

    def b_first_y(m):
        b2_send(m, 0, 1)
        b_partner(m, 0, 0)

    def b_z(m, r):
        b1_wait(m, r)
        if r < RZ:
            b1_send(m, r + 1)

    def b_zy(m, r):
        for slot in slots_of(NZ, r):
            b2_send(m, slot, 1)
            b_partner(m, slot, 0)

    def b_y(m, r, k):
        arrived(some(m, len(slots_of(NZ, r)), len(slots_of(NY, k))), w_r2.at[m, r, k - 1])
        for slot in slots_of(NZ, r):
            if k < RY:
                b2_send(m, slot, k + 1)
            for yslot in slots_of(NY, k):
                b_partner(m, slot, yslot)

    def a_y(m, k):
        a1_wait(m, k)
        if k < RY:
            a1_send(m, k + 1)

    def a_z(m, r):
        a2_wait(m, r)
        if r < RZ:
            a2_send(m, r + 1)
        for slot in slots_of(NZ, r):
            a_partner(m, slot)

    def a_first_z(m):
        a2_send(m, 1)
        a_partner(m, 0)

    def resid_send():
        for k in range(1, NX):
            send(resid.at[x], resid.at[x], re_s, re_r, dev(xx=x + k))

    def wo_pass(r):
        wo_wait(r)
        if r < NX // 2:
            wo_send(r + 1)

    steps = {
        "ast": lambda m: a1_send(m, 1),
        "ay": a_y,
        "az0": a_first_z,
        "az": a_z,
        "bz0": lambda m: b1_send(m, 1),
        "by0": b_first_y,
        "zz": b_z,
        "zy": b_zy,
        "y": b_y,
        "wo0": lambda: wo_send(1),
        "wo1": lambda: wo_pass(1),
        "wo2": lambda: wo_pass(2),
        "re": resid_send,
    }

    def on(which, *todo):
        def run():
            core[0] = which
            for f, *a in todo:
                steps[f](*a)

        pl.when(c == which)(run)

    def gap(name):
        phase("g_" + name)
        at = PARTS.index(name)
        for which in (0, 1):
            if PLAN[which][at]:
                on(which, *PLAN[which][at])

    phase("send0")

    def q_send(r):
        if r in yboth:
            left = 0 if r == 1 else offset_of(NY, 2 * r - 3) % NY
            right = 0 if r == 1 else offset_of(NY, 2 * r - 2) % NY
            send(qall.at[left], qall.at[(-r) % NY], q_s, q_r.at[r], dev(yy=y + 1))
            send(qall.at[right], qall.at[r], q_s, q_r.at[r], dev(yy=y - 1))
        elif r == ylast:
            member = 0 if r == 1 else (-dirc * (r - 1) + NY) % NY
            send(qall.at[member], qall.at[r], q_s, q_r.at[r], dev(yy=y + dirc))

    kv_send(1)
    kv_partner(0)
    q_send(1)
    for d in loc:
        d.wait()

    lane = lax.broadcasted_iota(jnp.int32, (T, 256), 1)
    own0 = (lane < 64) | ((lane >= 128) & (lane < 160))
    own1 = ((lane >= 64) & (lane < 128)) | ((lane >= 160) & (lane < 192))
    own2 = ((lane >= 64) & (lane < 96)) | (lane >= 128)

    def spread(k):
        narrow = qall[k, :, 0:256]
        wide = qall[k, :, 128:384]
        zero = jnp.zeros_like(narrow)
        qx[0, k * T : (k + 1) * T, :] = jnp.where(own0, narrow, zero)
        qx[1, k * T : (k + 1) * T, :] = jnp.where(own1, narrow, zero)
        qx[2, k * T : (k + 1) * T, :] = jnp.where(own2, wide, zero)

    def kv_wait(r):
        phase(f"kvw#r={r}")
        ring = slots_of(NZ, r)
        arrived(lats.at[pl.ds(ring[0], len(ring)), c, 0], kv_r.at[r])
        if r < RZ:
            kv_send(r + 1)
        for slot in ring:
            for k in range(1, NX):
                send(lats.at[slot, c, x], lats.at[slot, c, x], kx_s, kx_r.at[r], dev(xx=x + k))

    def kx_wait(r):
        phase(f"kx#r={r}")
        ring = slots_of(NZ, r)
        arrived(lats.at[pl.ds(ring[0], len(ring)), c, pl.ds(0, NX - 1)], kx_r.at[r])
        for slot in ring:
            kv_partner(slot)

    phase("spread0")
    vwt[...] = jnp.transpose(vw_ref[...].astype(F32)).astype(BF16)
    spread(0)
    mrow[...] = jnp.full_like(mrow, -1e30)
    lrow[...] = jnp.zeros_like(lrow)
    acc[...] = jnp.zeros_like(acc)
    def q_wait(r):
        phase(f"qw#r={r}")
        arrived(qall.at[pl.ds(0, len(slots_of(NY, r)))], q_r.at[r])
        if r < RY:
            q_send(r + 1)
        for slot in slots_of(NY, r):
            spread(offset_of(NY, slot) % NY)

    QB = min(256, NY * T)
    head_rows = ((0, 64), (64, 128), (128, 256))

    def attend(first, count):
        nk = count * 2 * T
        lat = lats[first : first + count, :, :, :, 0:L].reshape(nk, L)
        rot = lats[first : first + count, :, :, :, L : L + 128].reshape(nk, 128)
        keys = dot(lat, kw_ref[...]).astype(BF16)
        k_narrow[0:nk, 0:128] = keys[:, 0:128]
        k_narrow[0:nk, 128:256] = rot
        k_wide[0:nk, 0:128] = rot
        k_wide[0:nk, 128:256] = keys[:, 128:256]
        v_turned[:, 0:nk] = dot_nt(vwt[...], lat).astype(BF16)

        def block(b, carry):
            cols = pl.ds(pl.multiple_of(b * QB, QB), QB)
            for h in range(3):
                s = dot_nt((k_narrow if h < 2 else k_wide)[0:nk, :], qx[h, cols, :]) * (scales[h] * LOG2E)
                old = mrow[h : h + 1, cols]
                new = jnp.maximum(old, jnp.max(s, axis=0, keepdims=True))
                shrink = jnp.exp2(old - new)
                p = jnp.exp2(s - new)
                lrow[h : h + 1, cols] = lrow[h : h + 1, cols] * shrink + jnp.sum(p, axis=0, keepdims=True)
                mrow[h : h + 1, cols] = new
                r0, r1 = head_rows[h]
                acc[r0:r1, cols] = acc[r0:r1, cols] * shrink + dot(v_turned[r0:r1, 0:nk], p.astype(BF16))
            return carry

        lax.fori_loop(0, NY * T // QB, block, 0)

    def att(r):
        phase(f"attw#r={r}")
        ring = slots_of(NZ, r)
        arrived(lats.at[pl.ds(ring[0], len(ring)), 1 - c], kvp_r.at[r])
        phase(f"att#r={r}")
        attend(ring[0], len(ring))

    do = {"kvw": kv_wait, "kx": kx_wait, "q": q_wait, "att": att}
    for name in PARTS[: PARTS.index("owait")]:
        gap(name)
        do[name[:-1]](int(name[-1]))

    phase("osend")
    for k in range(NY):
        cols = slice(k * T, (k + 1) * T)
        osend[k] = acc[:, cols].astype(BF16)
        ssend[k, 0:3] = mrow[0:3, cols]
        ssend[k, 3:6] = lrow[0:3, cols]
        ssend[k, 6:8] = jnp.zeros((2, T), F32)
    for k in range(1, NY):
        send(osend.at[k], orecv.at[NY - k], o_s, o_r, dev(yy=y + k))
        send(ssend.at[k], srecv.at[NY - k], st_s, st_r, dev(yy=y + k))
    gap("owait")
    phase("owait")
    arrived(orecv.at[pl.ds(1, NY - 1)], o_r)
    arrived(srecv.at[pl.ds(1, NY - 1)], st_r)
    phase("merge")
    ms = [ssend[0, 0:3]] + [srecv[k, 0:3] for k in range(1, NY)]
    ls = [ssend[0, 3:6]] + [srecv[k, 3:6] for k in range(1, NY)]
    top = functools.reduce(jnp.maximum, ms)
    ws = [jnp.exp2(m - top) for m in ms]
    total = sum(a * b for a, b in zip(ws, ls))
    outs = []
    for h in range(3):
        r0, r1 = head_rows[h]
        o = acc[r0:r1, 0:T] * ws[0][h : h + 1]
        for k in range(1, NY):
            o = o + orecv[k, r0:r1].astype(F32) * ws[k][h : h + 1]
        o = o / total[h : h + 1]
        outs.append(o * lax.rsqrt(jnp.mean(o * o, axis=0, keepdims=True) + EPS))
    heads = jnp.transpose(jnp.concatenate(outs, axis=0))
    mixed[x] = (heads * ogain_ref[...]).astype(BF16)
    for k in range(1, NX):
        send(mixed.at[x], mixed.at[x], mx_s, mx_r, dev(xx=x + k))
    gap("mixw")
    phase("mixw")
    arrived(mixed.at[pl.ds(0, NX - 1)], mx_r)
    arrived(resid.at[pl.ds(0, NX - 1)], re_r)
    arrived(wo.at[pl.ds(0, NX - 1), 0], wop_r)
    phase("proj")
    mixed_all = jnp.concatenate([mixed[k] for k in range(NX)], axis=1)

    def project(n, squares):
        cols = pl.ds(pl.multiple_of(n * 256, 256), 256)
        s = dot(mixed_all, wo[:, :, :, cols].reshape(NX * 256, 256))
        s = (s + resid[:, :, cols].reshape(T, 256).astype(F32)).astype(BF16)
        mid[n] = s
        s = s.astype(F32)
        return squares + jnp.sum(s * s, axis=1, keepdims=True)

    squares = lax.fori_loop(0, D // 256, project, jnp.zeros((T, 1), F32))
    factor = lax.rsqrt(squares / D + EPS)

    def scale(n, carry):
        cols = pl.ds(pl.multiple_of(n * 256, 256), 256)
        normed[n] = (mid[n].astype(F32) * factor * mgain_ref[:, cols]).astype(BF16)
        return carry

    lax.fori_loop(0, D // 256, scale, 0)

    phase("mlp0")
    def from_partner(u, r):
        arrived(some(u, len(slots_of(NZ, r)), NY), wp_r.at[u, r])

    accg[...] = jnp.zeros_like(accg)
    accu[...] = jnp.zeros_like(accu)
    F = accg.shape[1]

    def widen(k):
        for u in range(3):
            from_partner(u, k)
        ring = slots_of(NZ, k)

        def one(i, carry):
            step = 0 if k == 0 else (k if len(ring) == 1 else (2 * i - 1) * k)
            p = (z + step + 2 * NZ) % NZ
            n = normed[p]
            accg[...] += dot(n, w[0, p].reshape(256, F))
            accu[...] += dot(n, w[1, p].reshape(256, F))
            return carry

        lax.fori_loop(0, len(ring), one, 0)

    for r in range(RZ + 1):
        gap(f"widen{r}")
        phase(f"widen#r={r}")
        widen(r)
    gap("hid")
    phase("hid")
    g = accg[...]
    hid[...] = (g / (1.0 + jnp.exp(-g)) * accu[...]).astype(BF16)

    def narrow(slot, carry):
        p = (z + ((slot + 1) // 2) * (1 - 2 * (slot % 2)) + 2 * NZ) % NZ
        s = dot_nt(hid[...], w[2, p].reshape(256, F)).astype(BF16)
        part[slot] = s.reshape(NX, R, 256)
        return carry

    def sums_rows(r):
        ring = slots_of(NZ, r)
        return pl.ds(ring[0], len(ring))

    for r in range(RZ + 1):
        gap(f"down{r}")
        phase(f"down#r={r}")
        ring = slots_of(NZ, r)
        from_partner(3, r)
        lax.fori_loop(ring[0], ring[0] + len(ring), narrow, 0)
        rows = sums_rows(r)
        for k in range(1, NX):
            p = (x + k) % NX
            send(part.at[rows, p], rsum.at[NX - k, rows], rs_s, rs_r.at[r], dev(xx=x + k))
    gap("final")
    phase("final")
    for r in range(RZ + 1):
        arrived(rsum.at[pl.ds(1, NX - 1), sums_rows(r)], rs_r.at[r])
        for slot in slots_of(NZ, r):
            p = zpos(slot)
            s = part[slot, x].astype(F32)
            for k in range(1, NX):
                s = s + rsum[k, slot].astype(F32)
            s = s + mid[p, pl.ds(pl.multiple_of(x * R, R), R), :].astype(F32)
            out_ref[:, pl.ds(pl.multiple_of(p * 256, 256), 256)] = s.astype(BF16)

    phase("sendw")
    arrived(lats.at[pl.ds(0, NZ - 1), 0, 0], kv_s)
    arrived(lats.at[:, 0], kvp_s)
    arrived(lats.at[pl.ds(0, NZ - 1), 0, pl.ds(0, NX - 1)], kx_s)
    arrived(qall.at[pl.ds(0, NY - 1)], q_s)
    arrived(osend.at[pl.ds(1, NY - 1)], o_s)
    arrived(ssend.at[pl.ds(1, NY - 1)], st_s)
    arrived(mixed.at[pl.ds(0, NX - 1)], mx_s)
    arrived(wo.at[pl.ds(0, NX - 1), 0], wo_s)
    arrived(wo.at[pl.ds(0, NX - 1), 0], wop_s)
    arrived(resid.at[pl.ds(0, NX - 1)], re_s)
    arrived(part.at[:, pl.ds(0, NX - 1)], rs_s)

    for which in (0, 1):

        @pl.when(c == which)
        def _():
            for u in range(4):
                first_y = u in Y_FIRST[which]
                arrived(some(u, 1, NY - 1) if first_y else some(u, NZ - 1, 1), w_s1.at[u])
                arrived(some(u, NZ - 1, NY) if first_y else some(u, NZ, NY - 1), w_s2.at[u])
                arrived(some(u, NZ, NY), wp_s.at[u])

    phases.close()


def on_device(
    NZ,
    NX,
    residual,
    query_content,
    query_rotary,
    key_latent,
    rotary_key,
    latent_gain,
    key_weight,
    value_weight,
    output_gain,
    output_weight,
    mixer_gain,
    gate_weight,
    up_weight,
    down_weight,
):
    T = key_latent.shape[0]
    R, D = residual.shape
    F = gate_weight.shape[1]
    positions = lax.axis_index("sp") * T + lax.iota(jnp.int32, T)
    power = jnp.arange(0, ROT_DIM, 2, dtype=F32) / ROT_DIM
    inverse = 1.0 / jnp.power(ROPE_BASE, power)
    angles = positions.astype(F32)[None, :] * inverse[:, None]
    cos = jnp.cos(angles)
    sin = jnp.sin(angles)
    vm = pl.BlockSpec(memory_space=pltpu.VMEM)
    hbm = pl.BlockSpec(memory_space=pl.ANY)
    V = pltpu.VMEM

    def pin(a):
        return pltpu.with_memory_space_constraint(a, pltpu.HBM)

    S = pltpu.SemaphoreType.DMA
    RZ = NZ // 2
    scales = ((64 + ROT_DIM) ** -0.5,) * 2 + ((128 + ROT_DIM) ** -0.5,)
    return pl.pallas_call(
        functools.partial(kernel, NZ, NX, scales),
        out_shape=jax.ShapeDtypeStruct((R, D), BF16),
        in_specs=[vm] * 2 + [hbm] * 14,
        out_specs=vm,
        scratch_shapes=[
            V((1, output_gain.shape[0]), F32),
            V((1, D), F32),
            V((1, key_latent.shape[1]), F32),
            V((T, key_latent.shape[1]), BF16),
            V(key_weight.shape, BF16),
            V(value_weight.shape, BF16),
            V((T, 256), BF16),
            V((query_rotary.shape[1], T), BF16),
            V((ROT_DIM, T), BF16),
            V((3, NZ, NY, 2, R, F), BF16),
            V((NZ, 2, NX, T // NX, key_latent.shape[1] + 128), BF16),
            V(value_weight.shape[::-1], BF16),
            V((4 * T, 256), BF16),
            V((4 * T, 256), BF16),
            V((256, 4 * T), BF16),
            V((NY, T, 384), BF16),
            V((3, NY * T, 256), BF16),
            V((256, NY * T), F32),
            V((8, NY * T), F32),
            V((8, NY * T), F32),
            V((NY, 256, T), BF16),
            V((NY, 256, T), BF16),
            V((NY, 8, T), F32),
            V((NY, 8, T), F32),
            V((NX, T, 256), BF16),
            V((NX, 2, 128, D), BF16),
            V((NX, R, D), BF16),
            V((NZ, T, 256), BF16),
            V((NZ, T, 256), BF16),
            V((T, F), F32),
            V((T, F), F32),
            V((T, F), BF16),
            V((NZ, NX, R, 256), BF16),
            V((NX, NZ, R, 256), BF16),
            S((7,)),
            S((7,)),
            S(()),
            S((RZ + 1,)),
            S(()),
            S((RZ + 1,)),
            S(()),
            S((RZ + 1,)),
            S(()),
            S((NY // 2 + 1,)),
            S(()),
            S(()),
            S(()),
            S(()),
            S(()),
            S(()),
            S(()),
            S((NX // 2 + 1,)),
            S(()),
            S(()),
            S(()),
            S(()),
            S(()),
            S((RZ + 1,)),
            S((4,)),
            S((4,)),
            S((4,)),
            S((4, RZ + 1)),
            S((4, RZ + 1, 2)),
            S((4, RZ + 1)),
        ],
        compiler_params=pltpu.CompilerParams(
            collective_id=0, has_side_effects=True, vmem_limit_bytes=44 * 1024 * 1024
        ),
    )(
        cos,
        sin,
        pin(output_gain[None, :]),
        pin(mixer_gain[None, :]),
        pin(latent_gain[None, :]),
        pin(key_latent),
        pin(key_weight),
        pin(value_weight),
        pin(query_content),
        pin(query_rotary.T),
        pin(rotary_key.T),
        pin(residual),
        pin(output_weight.reshape(2, 128, D)),
        pin(gate_weight),
        pin(up_weight),
        pin(down_weight.T),
    )


def solution(mesh):
    placed = (
        P(("sp", "tp"), None),
        P("sp", "tp"),
        P("sp", "tp"),
        P("sp", None),
        P("sp", None),
        P(),
        P(None, "tp"),
        P(None, "tp"),
        P("tp"),
        P("tp", None),
        P(),
        P("sp", "tp"),
        P("sp", "tp"),
        P("tp", "sp"),
    )
    NZ = mesh.shape["sp"] // (2 * NY)
    NX = mesh.shape["tp"]
    return jax.shard_map(
        functools.partial(on_device, NZ, NX),
        mesh=mesh,
        in_specs=placed,
        out_specs=P(("sp", "tp"), None),
        check_vma=False,
    )
```

```python
import contextlib
import functools

import jax
import jax.numpy as jnp
from jax import lax
from jax.experimental import pallas as pl
from jax.experimental.pallas import tpu as pltpu
from jax.sharding import PartitionSpec as P

NY = 4
ROT_DIM = 32
EPS = 1e-06
ROPE_BASE = 500000.0
LOG2E = 1.4426950408889634
MESH = pl.DeviceIdType.MESH
F32 = jnp.float32
BF16 = jnp.bfloat16

Y_FIRST = ((0, 1, 2), (2,))
ZDIR = ((1, -1, -1, -1), (-1, 1, 1, -1))
PARTS = (
    "kvw1",
    "kvw2",
    "q1",
    "q2",
    "kvw3",
    "kx1",
    "att0",
    "kvw4",
    "kx2",
    "att1",
    "kx3",
    "att2",
    "kx4",
    "att3",
    "att4",
    "owait",
    "mixw",
    "widen0",
    "widen1",
    "widen2",
    "widen3",
    "widen4",
    "hid",
    "down0",
    "down1",
    "down2",
    "down3",
    "down4",
    "final",
)
PLAN = (
    (
        (("ast", 1), ("re",), ("ast", 0), ("bz0", 3),),
        (("by0", 3), ("ast", 2), ("zz", 3, 1), ("ay", 1, 1),),
        (("ay", 0, 1), ("ay", 1, 2), ("az0", 1), ("ay", 2, 1),),
        (),
        (),
        (("ay", 0, 2), ("az0", 0),),
        (("wo0",),),
        (),
        (("ay", 2, 2), ("az0", 2),),
        (("zz", 3, 2), ("zy", 3, 2),),
        (("y", 3, 0, 1), ("az", 0, 1),),
        (),
        (("az", 2, 1),),
        (("wo1",),),
        (("az", 1, 1),),
        (("az", 0, 2), ("az", 2, 2), ("az", 1, 2), ("y", 3, 2, 1), ("wo2",),),
        (("zy", 3, 1), ("zz", 3, 3), ("zy", 3, 3), ("az", 2, 3), ("y", 3, 0, 2), ("az", 0, 3),),
        (("az", 1, 3),),
        (("y", 3, 1, 1), ("zz", 3, 4), ("zy", 3, 4),),
        (("y", 3, 3, 1),),
        (),
        (("az", 2, 4), ("az", 0, 4), ("az", 1, 4),),
        (("y", 3, 1, 2),),
        (),
        (("y", 3, 2, 2), ("y", 3, 4, 1),),
        (),
        (("y", 3, 3, 2),),
        (("y", 3, 4, 2),),
        (),
    ),
    (
        (("bz0", 1), ("re",), ("bz0", 3), ("ast", 2), ("bz0", 0),),
        (("zz", 1, 1), ("zz", 3, 1), ("zy", 3, 1), ("zz", 0, 1),),
        (),
        (("by0", 1), ("zz", 3, 2), ("zy", 3, 2), ("zz", 0, 2), ("zy", 0, 2), ("by0", 0), ("zz", 1, 2),),
        (("ay", 2, 1), ("by0", 3),),
        (),
        (("zz", 0, 3), ("zz", 1, 3), ("zy", 1, 3),),
        (("zy", 1, 1), ("ay", 2, 2), ("az0", 2),),
        (("y", 0, 0, 1), ("y", 3, 0, 1),),
        (("zy", 0, 3), ("zz", 1, 4), ("zy", 1, 4),),
        (("y", 3, 2, 1), ("zy", 1, 2),),
        (("wo0",), ("zy", 0, 1),),
        (("y", 1, 1, 1),),
        (("y", 3, 1, 1), ("zz", 0, 4), ("zy", 0, 4), ("az", 2, 1),),
        (("y", 1, 2, 1), ("y", 0, 3, 1), ("y", 3, 0, 2),),
        (("az", 2, 2), ("y", 0, 1, 1), ("wo1",), ("y", 0, 4, 1),),
        (("y", 1, 3, 1), ("y", 0, 2, 1), ("y", 1, 0, 1), ("wo2",), ("y", 1, 4, 1), ("zz", 3, 3), ("zy", 3, 3), ("az", 2, 3),),
        (("y", 0, 4, 2), ("y", 0, 1, 2), ("y", 0, 0, 2), ("y", 1, 0, 2),),
        (("zz", 3, 4), ("zy", 3, 4), ("y", 1, 1, 2),),
        (("y", 0, 3, 2), ("y", 3, 2, 2), ("y", 3, 1, 2), ("y", 0, 2, 2), ("y", 1, 2, 2),),
        (("az", 2, 4), ("y", 1, 3, 2),),
        (("y", 1, 4, 2), ("y", 3, 3, 1), ("y", 3, 4, 1),),
        (),
        (),
        (),
        (("y", 3, 3, 2),),
        (("y", 3, 4, 2),),
        (),
        (),
    ),
)


def dot(a, b):
    return lax.dot_general(a, b, (((1,), (0,)), ((), ())), preferred_element_type=F32)


def dot_nt(a, b):
    return lax.dot_general(a, b, (((1,), (1,)), ((), ())), preferred_element_type=F32)


def hops(n):
    both = list(range(1, (n - 1) // 2 + 1))
    return both, (n // 2 if n % 2 == 0 and n > 1 else None)


def kernel(
    NZ,
    NX,
    scales,
    cos_ref,
    sin_ref,
    ogain_hbm,
    mgain_hbm,
    lgain_hbm,
    lat_hbm,
    kw_hbm,
    vw_hbm,
    qc_hbm,
    qr_hbm,
    rk_hbm,
    resid_hbm,
    ow_hbm,
    gate_hbm,
    up_hbm,
    down_hbm,
    out_ref,
    ogain_ref,
    mgain_ref,
    lgain_ref,
    lat_ref,
    kw_ref,
    vw_ref,
    qc_ref,
    qr_ref,
    rk_ref,
    w,
    lats,
    vwt,
    k_narrow,
    k_wide,
    v_turned,
    qall,
    qx,
    acc,
    mrow,
    lrow,
    osend,
    orecv,
    ssend,
    srecv,
    mixed,
    wo,
    resid,
    mid,
    normed,
    accg,
    accu,
    hid,
    part,
    rsum,
    small_sem,
    loc_sem,
    kv_s,
    kv_r,
    kvp_s,
    kvp_r,
    kx_s,
    kx_r,
    q_s,
    q_r,
    o_s,
    o_r,
    st_s,
    st_r,
    mx_s,
    mx_r,
    wo_s,
    wo_r,
    wop_s,
    wop_r,
    re_s,
    re_r,
    rs_s,
    rs_r,
    w_s1,
    w_s2,
    wp_s,
    w_r1,
    w_r2,
    wp_r,
):
    sp = lax.axis_index("sp")
    x = lax.axis_index("tp")
    c = sp % 2
    y = (sp // 2) % NY
    z = sp // (2 * NY)
    T = qc_ref.shape[0]
    R = resid.shape[1]
    D = resid.shape[2]
    phases = contextlib.ExitStack()

    def phase(name):
        phases.close()
        phases.enter_context(jax.named_scope(name))

    def dev(zz=None, yy=None, cc=None, xx=None):
        zz = z if zz is None else (zz + 2 * NZ) % NZ
        yy = y if yy is None else (yy + 2 * NY) % NY
        cc = c if cc is None else cc
        xx = x if xx is None else (xx + 2 * NX) % NX
        return ((zz * NY + yy) * 2 + cc, xx)

    def send(src, dst, ssem, rsem, device):
        pltpu.make_async_remote_copy(
            src_ref=src, dst_ref=dst, send_sem=ssem, recv_sem=rsem, device_id=device, device_id_type=MESH
        ).start()

    def arrived(ref, sem):
        pltpu.make_async_copy(ref, ref, sem).wait()

    partner = dev(cc=1 - c)
    dirc = 1 - 2 * c
    zboth, zlast = hops(NZ)
    yboth, ylast = hops(NY)
    xboth, xlast = hops(NX)

    barrier = pltpu.get_barrier_semaphore()
    peers = [partner]
    peers += [dev(zz=z + 1)] + ([dev(zz=z - 1)] if NZ > 2 else [])
    peers += [dev(yy=y + k) for k in range(1, NY)]
    peers += [dev(xx=x + k) for k in range(1, NX)]
    for p in peers:
        pl.semaphore_signal(barrier, inc=1, device_id=p, device_id_type=MESH)

    small = [
        pltpu.make_async_copy(a, b, small_sem.at[k])
        for k, (a, b) in enumerate(
            [(lat_hbm, lat_ref), (lgain_hbm, lgain_ref), (kw_hbm, kw_ref), (vw_hbm, vw_ref), (qc_hbm, qc_ref), (qr_hbm, qr_ref), (rk_hbm, rk_ref)]
        )
    ]
    loc = [
        pltpu.make_async_copy(a, b, loc_sem.at[k])
        for k, (a, b) in enumerate(
            [
                (gate_hbm, w.at[0, z, y, c]),
                (up_hbm, w.at[1, z, y, c]),
                (down_hbm, w.at[2, z, y, c]),
                (ow_hbm, wo.at[x]),
                (resid_hbm, resid.at[x]),
                (ogain_hbm, ogain_ref),
                (mgain_hbm, mgain_ref),
            ]
        )
    ]
    for d in small + loc:
        d.start()
    phase("qkv")
    for d in small:
        d.wait()
    half = ROT_DIM // 2
    cos = cos_ref[...]
    sin = sin_ref[...]

    def turned(ref, count):
        rows = []
        for h in range(count):
            a = ref[h * ROT_DIM : h * ROT_DIM + half, :].astype(F32)
            b = ref[h * ROT_DIM + half : (h + 1) * ROT_DIM, :].astype(F32)
            rows += [a * cos - b * sin, b * cos + a * sin]
        return rows

    lat = lat_ref[...].astype(F32)
    lat = lat * lax.rsqrt(jnp.mean(lat * lat, axis=-1, keepdims=True) + EPS)
    lat = (lat * lgain_ref[...]).astype(BF16)
    L = lat.shape[1]
    lats[0, c, :, :, 0:L] = lat.reshape(NX, T // NX, L)
    rot = jnp.transpose(jnp.concatenate(turned(rk_ref, 1) * 4, axis=0)).astype(BF16)
    lats[0, c, :, :, L : L + 128] = rot.reshape(NX, T // NX, 128)

    turned_q = turned(qr_ref, 3) + [jnp.zeros((ROT_DIM, T), F32)]
    qall[0, :, 0:128] = qc_ref[:, 0:128]
    qall[0, :, 128:256] = jnp.transpose(jnp.concatenate(turned_q, axis=0)).astype(BF16)
    qall[0, :, 256:384] = qc_ref[:, 128:256]

    phase("barrier")
    pl.semaphore_wait(barrier, len(peers))

    def kv_copy(src_slot, dst_slot, device):
        send(lats.at[src_slot, c, x], lats.at[dst_slot, c, x], kv_s, kv_r.at[(dst_slot + 1) // 2], device)

    def kv_partner(slot):
        send(lats.at[slot, c], lats.at[slot, c], kvp_s, kvp_r.at[(slot + 1) // 2], partner)

    def kv_send(r):
        if r in zboth:
            kv_copy(2 * r - 3 if r > 1 else 0, 2 * r - 1, dev(zz=z + 1))
            kv_copy(2 * r - 2 if r > 1 else 0, 2 * r, dev(zz=z - 1))
        elif r == zlast:
            kv_copy((2 * r - 3 + c) if r > 1 else 0, NZ - 1, dev(zz=z + dirc))

    def slots_of(n, r):
        if r == 0:
            return [0]
        return [2 * r - 1, 2 * r] if r <= (n - 1) // 2 else [n - 1]

    def offset_of(n, slot):
        if slot == 0:
            return 0
        return slot_r(n, slot) if slot % 2 == 0 else -slot_r(n, slot)

    def slot_r(n, slot):
        return (slot + 1) // 2

    def zpos(slot):
        return (z + offset_of(NZ, slot) + 2 * NZ) % NZ

    def ypos(slot):
        return (y + offset_of(NY, slot) + 2 * NY) % NY

    def wo_send(r):
        if r in xboth:
            send(wo.at[(x - r + 1 + NX) % NX, c], wo.at[(x - r + 1 + NX) % NX, c], wo_s, wo_r.at[r], dev(xx=x + 1))
            send(wo.at[(x + r - 1) % NX, c], wo.at[(x + r - 1) % NX, c], wo_s, wo_r.at[r], dev(xx=x - 1))
        elif r == xlast:
            p = (x - dirc * (r - 1) + 2 * NX) % NX
            send(wo.at[p, c], wo.at[p, c], wo_s, wo_r.at[r], dev(xx=x + dirc))

    def wo_wait(r):
        arrived(wo.at[pl.ds(0, len(slots_of(NX, r))), c], wo_r.at[r])
        for slot in slots_of(NX, r):
            p = (x + offset_of(NX, slot) + 2 * NX) % NX
            send(wo.at[p, c], wo.at[p, c], wop_s, wop_r, partner)

    cut = w.shape[5] // 256 * 128
    units = ((0, 0, w.shape[5]), (1, 0, cut), (1, cut, w.shape[5]), (2, 0, w.shape[5]))
    core = [0]

    def piece(u, zz, yy, cc):
        mat, lo, hi = units[u]
        return w.at[mat, zz, yy, cc, :, lo:hi]

    def some(u, nz, ny):
        return piece(u, pl.ds(0, nz), pl.ds(0, ny), 0)

    def ring_y(u, zz, r, d, ssem, rsem):
        if r in yboth:
            a, b = (y - r + 1 + NY) % NY, (y + r - 1) % NY
            send(piece(u, zz, a, core[0]), piece(u, zz, a, core[0]), ssem, rsem, dev(yy=y + 1))
            send(piece(u, zz, b, core[0]), piece(u, zz, b, core[0]), ssem, rsem, dev(yy=y - 1))
        elif r == ylast:
            p = (y - d * (r - 1) + 2 * NY) % NY
            send(piece(u, zz, p, core[0]), piece(u, zz, p, core[0]), ssem, rsem, dev(yy=y + d))

    def ring_z(u, yy, r, ssem, rsem):
        d = ZDIR[core[0]][u]
        if r in zboth:
            a, b = (z - r + 1 + NZ) % NZ, (z + r - 1) % NZ
            send(piece(u, a, yy, core[0]), piece(u, a, yy, core[0]), ssem, rsem, dev(zz=z + 1))
            send(piece(u, b, yy, core[0]), piece(u, b, yy, core[0]), ssem, rsem, dev(zz=z - 1))
        elif r == zlast:
            p = (z - d * (r - 1) + 2 * NZ) % NZ
            send(piece(u, p, yy, core[0]), piece(u, p, yy, core[0]), ssem, rsem, dev(zz=z + d))

    every = pl.ds(0, NY)

    def a1_send(u, r):
        ring_y(u, z, r, ZDIR[core[0]][u], w_s1.at[u], w_r1.at[u, r])

    def a1_wait(u, r):
        arrived(some(u, 1, len(slots_of(NY, r))), w_r1.at[u, r])

    def a2_send(u, r):
        ring_z(u, every, r, w_s2.at[u], w_r2.at[u, r, 0])

    def a_partner(u, slot):
        p = piece(u, zpos(slot), every, core[0])
        send(p, p, wp_s.at[u], wp_r.at[u, (slot + 1) // 2], partner)

    def a2_wait(u, r):
        arrived(some(u, len(slots_of(NZ, r)), NY), w_r2.at[u, r, 0])

    def b1_send(u, r):
        ring_z(u, y, r, w_s1.at[u], w_r1.at[u, r])

    def b1_wait(u, r):
        arrived(some(u, len(slots_of(NZ, r)), 1), w_r1.at[u, r])

    def b2_send(u, slot, r):
        d = (1 - 2 * core[0]) * (1 - 2 * (slot % 2))
        ring_y(u, zpos(slot), r, d, w_s2.at[u], w_r2.at[u, (slot + 1) // 2, r - 1])

    def b_partner(u, slot, yslot):
        p = piece(u, zpos(slot), ypos(yslot), core[0])
        send(p, p, wp_s.at[u], wp_r.at[u, (slot + 1) // 2], partner)

    RZ = NZ // 2
    RY = NY // 2

    def b_first_y(m):
        b2_send(m, 0, 1)
        b_partner(m, 0, 0)

    def b_z(m, r):
        b1_wait(m, r)
        if r < RZ:
            b1_send(m, r + 1)

    def b_zy(m, r):
        for slot in slots_of(NZ, r):
            b2_send(m, slot, 1)
            b_partner(m, slot, 0)

    def b_y(m, r, k):
        arrived(some(m, len(slots_of(NZ, r)), len(slots_of(NY, k))), w_r2.at[m, r, k - 1])
        for slot in slots_of(NZ, r):
            if k < RY:
                b2_send(m, slot, k + 1)
            for yslot in slots_of(NY, k):
                b_partner(m, slot, yslot)

    def a_y(m, k):
        a1_wait(m, k)
        if k < RY:
            a1_send(m, k + 1)

    def a_z(m, r):
        a2_wait(m, r)
        if r < RZ:
            a2_send(m, r + 1)
        for slot in slots_of(NZ, r):
            a_partner(m, slot)

    def a_first_z(m):
        a2_send(m, 1)
        a_partner(m, 0)

    def resid_send():
        for k in range(1, NX):
            send(resid.at[x], resid.at[x], re_s, re_r, dev(xx=x + k))

    def wo_pass(r):
        wo_wait(r)
        if r < NX // 2:
            wo_send(r + 1)

    steps = {
        "ast": lambda m: a1_send(m, 1),
        "ay": a_y,
        "az0": a_first_z,
        "az": a_z,
        "bz0": lambda m: b1_send(m, 1),
        "by0": b_first_y,
        "zz": b_z,
        "zy": b_zy,
        "y": b_y,
        "wo0": lambda: wo_send(1),
        "wo1": lambda: wo_pass(1),
        "wo2": lambda: wo_pass(2),
        "re": resid_send,
    }

    def on(which, *todo):
        def run():
            core[0] = which
            for f, *a in todo:
                steps[f](*a)

        pl.when(c == which)(run)

    def gap(name):
        phase("g_" + name)
        at = PARTS.index(name)
        for which in (0, 1):
            if PLAN[which][at]:
                on(which, *PLAN[which][at])

    phase("send0")

    def q_send(r):
        if r in yboth:
            left = 0 if r == 1 else offset_of(NY, 2 * r - 3) % NY
            right = 0 if r == 1 else offset_of(NY, 2 * r - 2) % NY
            send(qall.at[left], qall.at[(-r) % NY], q_s, q_r.at[r], dev(yy=y + 1))
            send(qall.at[right], qall.at[r], q_s, q_r.at[r], dev(yy=y - 1))
        elif r == ylast:
            member = 0 if r == 1 else (-dirc * (r - 1) + NY) % NY
            send(qall.at[member], qall.at[r], q_s, q_r.at[r], dev(yy=y + dirc))

    kv_send(1)
    kv_partner(0)
    q_send(1)
    for d in loc:
        d.wait()

    lane = lax.broadcasted_iota(jnp.int32, (T, 256), 1)
    own0 = (lane < 64) | ((lane >= 128) & (lane < 160))
    own1 = ((lane >= 64) & (lane < 128)) | ((lane >= 160) & (lane < 192))
    own2 = ((lane >= 64) & (lane < 96)) | (lane >= 128)

    def spread(k):
        narrow = qall[k, :, 0:256]
        wide = qall[k, :, 128:384]
        zero = jnp.zeros_like(narrow)
        qx[0, k * T : (k + 1) * T, :] = jnp.where(own0, narrow, zero)
        qx[1, k * T : (k + 1) * T, :] = jnp.where(own1, narrow, zero)
        qx[2, k * T : (k + 1) * T, :] = jnp.where(own2, wide, zero)

    def kv_wait(r):
        phase(f"kvw#r={r}")
        ring = slots_of(NZ, r)
        arrived(lats.at[pl.ds(ring[0], len(ring)), c, 0], kv_r.at[r])
        if r < RZ:
            kv_send(r + 1)
        for slot in ring:
            for k in range(1, NX):
                send(lats.at[slot, c, x], lats.at[slot, c, x], kx_s, kx_r.at[r], dev(xx=x + k))

    def kx_wait(r):
        phase(f"kx#r={r}")
        ring = slots_of(NZ, r)
        arrived(lats.at[pl.ds(ring[0], len(ring)), c, pl.ds(0, NX - 1)], kx_r.at[r])
        for slot in ring:
            kv_partner(slot)

    phase("spread0")
    vwt[...] = jnp.transpose(vw_ref[...].astype(F32)).astype(BF16)
    spread(0)
    mrow[...] = jnp.full_like(mrow, -1e30)
    lrow[...] = jnp.zeros_like(lrow)
    acc[...] = jnp.zeros_like(acc)
    accg[...] = jnp.zeros_like(accg)
    accu[...] = jnp.zeros_like(accu)
    def q_wait(r):
        phase(f"qw#r={r}")
        arrived(qall.at[pl.ds(0, len(slots_of(NY, r)))], q_r.at[r])
        if r < RY:
            q_send(r + 1)
        for slot in slots_of(NY, r):
            spread(offset_of(NY, slot) % NY)

    QB = min(256, NY * T)
    head_rows = ((0, 64), (64, 128), (128, 256))

    def attend(first, count):
        nk = count * 2 * T
        lat = lats[first : first + count, :, :, :, 0:L].reshape(nk, L)
        rot = lats[first : first + count, :, :, :, L : L + 128].reshape(nk, 128)
        keys = dot(lat, kw_ref[...]).astype(BF16)
        k_narrow[0:nk, 0:128] = keys[:, 0:128]
        k_narrow[0:nk, 128:256] = rot
        k_wide[0:nk, 0:128] = rot
        k_wide[0:nk, 128:256] = keys[:, 128:256]
        v_turned[:, 0:nk] = dot_nt(vwt[...], lat).astype(BF16)

        def block(b, carry):
            cols = pl.ds(pl.multiple_of(b * QB, QB), QB)
            for h in range(3):
                s = dot_nt((k_narrow if h < 2 else k_wide)[0:nk, :], qx[h, cols, :]) * (scales[h] * LOG2E)
                old = mrow[h : h + 1, cols]
                new = jnp.maximum(old, jnp.max(s, axis=0, keepdims=True))
                shrink = jnp.exp2(old - new)
                p = jnp.exp2(s - new)
                lrow[h : h + 1, cols] = lrow[h : h + 1, cols] * shrink + jnp.sum(p, axis=0, keepdims=True)
                mrow[h : h + 1, cols] = new
                r0, r1 = head_rows[h]
                acc[r0:r1, cols] = acc[r0:r1, cols] * shrink + dot(v_turned[r0:r1, 0:nk], p.astype(BF16))
            return carry

        lax.fori_loop(0, NY * T // QB, block, 0, unroll=True)

    def att(r):
        phase(f"attw#r={r}")
        ring = slots_of(NZ, r)
        arrived(lats.at[pl.ds(ring[0], len(ring)), 1 - c], kvp_r.at[r])
        phase(f"att#r={r}")
        attend(ring[0], len(ring))

    do = {"kvw": kv_wait, "kx": kx_wait, "q": q_wait, "att": att}
    for name in PARTS[: PARTS.index("owait")]:
        gap(name)
        do[name[:-1]](int(name[-1]))

    phase("osend")
    for k in range(NY):
        cols = slice(k * T, (k + 1) * T)
        osend[k] = acc[:, cols].astype(BF16)
        ssend[k, 0:3] = mrow[0:3, cols]
        ssend[k, 3:6] = lrow[0:3, cols]
        ssend[k, 6:8] = jnp.zeros((2, T), F32)
    for k in range(1, NY):
        send(osend.at[k], orecv.at[NY - k], o_s, o_r, dev(yy=y + k))
        send(ssend.at[k], srecv.at[NY - k], st_s, st_r, dev(yy=y + k))
    gap("owait")
    phase("owait")
    arrived(orecv.at[pl.ds(1, NY - 1)], o_r)
    arrived(srecv.at[pl.ds(1, NY - 1)], st_r)
    phase("merge")
    ms = [ssend[0, 0:3]] + [srecv[k, 0:3] for k in range(1, NY)]
    ls = [ssend[0, 3:6]] + [srecv[k, 3:6] for k in range(1, NY)]
    top = functools.reduce(jnp.maximum, ms)
    ws = [jnp.exp2(m - top) for m in ms]
    total = sum(a * b for a, b in zip(ws, ls))
    outs = []
    for h in range(3):
        r0, r1 = head_rows[h]
        o = acc[r0:r1, 0:T] * ws[0][h : h + 1]
        for k in range(1, NY):
            o = o + orecv[k, r0:r1].astype(F32) * ws[k][h : h + 1]
        o = o / total[h : h + 1]
        outs.append(o * lax.rsqrt(jnp.mean(o * o, axis=0, keepdims=True) + EPS))
    heads = jnp.transpose(jnp.concatenate(outs, axis=0))
    mixed[x] = (heads * ogain_ref[...]).astype(BF16)
    for k in range(1, NX):
        send(mixed.at[x], mixed.at[x], mx_s, mx_r, dev(xx=x + k))
    gap("mixw")
    phase("mixw")
    arrived(mixed.at[pl.ds(0, NX - 1)], mx_r)
    arrived(resid.at[pl.ds(0, NX - 1)], re_r)
    arrived(wo.at[pl.ds(0, NX - 1), 0], wop_r)
    phase("proj")
    mixed_all = jnp.concatenate([mixed[k] for k in range(NX)], axis=1)

    def project(n, squares):
        cols = pl.ds(pl.multiple_of(n * 256, 256), 256)
        s = dot(mixed_all, wo[:, :, :, cols].reshape(NX * 256, 256))
        s = (s + resid[:, :, cols].reshape(T, 256).astype(F32)).astype(BF16)
        mid[n] = s
        s = s.astype(F32)
        return squares + s * s

    squares = lax.fori_loop(0, D // 256, project, jnp.zeros((T, 256), F32), unroll=4)
    factor = lax.rsqrt(jnp.sum(squares, axis=1, keepdims=True) / D + EPS)

    def scale(n, carry):
        cols = pl.ds(pl.multiple_of(n * 256, 256), 256)
        normed[n] = (mid[n].astype(F32) * factor * mgain_ref[:, cols]).astype(BF16)
        return carry

    lax.fori_loop(0, D // 256, scale, 0, unroll=4)

    phase("mlp0")
    def from_partner(u, r):
        arrived(some(u, len(slots_of(NZ, r)), NY), wp_r.at[u, r])

    F = accg.shape[1]

    def widen(k):
        for u in range(3):
            from_partner(u, k)
        ring = slots_of(NZ, k)

        def one(i, carry):
            step = 0 if k == 0 else (k if len(ring) == 1 else (2 * i - 1) * k)
            p = (z + step + 2 * NZ) % NZ
            n = normed[p]
            accg[...] += dot(n, w[0, p].reshape(256, F))
            accu[...] += dot(n, w[1, p].reshape(256, F))
            return carry

        lax.fori_loop(0, len(ring), one, 0, unroll=True)

    for r in range(RZ + 1):
        gap(f"widen{r}")
        phase(f"widen#r={r}")
        widen(r)
    gap("hid")
    phase("hid")
    g = accg[...]
    hid[...] = (g / (1.0 + jnp.exp(-g)) * accu[...]).astype(BF16)

    def narrow(slot, carry):
        p = (z + ((slot + 1) // 2) * (1 - 2 * (slot % 2)) + 2 * NZ) % NZ
        s = dot_nt(hid[...], w[2, p].reshape(256, F)).astype(BF16)
        part[slot] = s.reshape(NX, R, 256)
        return carry

    def sums_rows(r):
        ring = slots_of(NZ, r)
        return pl.ds(ring[0], len(ring))

    for r in range(RZ + 1):
        gap(f"down{r}")
        phase(f"down#r={r}")
        ring = slots_of(NZ, r)
        from_partner(3, r)
        lax.fori_loop(ring[0], ring[0] + len(ring), narrow, 0, unroll=True)
        rows = sums_rows(r)
        for k in range(1, NX):
            p = (x + k) % NX
            send(part.at[rows, p], rsum.at[NX - k, rows], rs_s, rs_r.at[r], dev(xx=x + k))
    gap("final")
    phase("final")
    for r in range(RZ + 1):
        arrived(rsum.at[pl.ds(1, NX - 1), sums_rows(r)], rs_r.at[r])
        for slot in slots_of(NZ, r):
            p = zpos(slot)
            s = part[slot, x].astype(F32)
            for k in range(1, NX):
                s = s + rsum[k, slot].astype(F32)
            s = s + mid[p, pl.ds(pl.multiple_of(x * R, R), R), :].astype(F32)
            out_ref[:, pl.ds(pl.multiple_of(p * 256, 256), 256)] = s.astype(BF16)

    phase("sendw")
    arrived(lats.at[pl.ds(0, NZ - 1), 0, 0], kv_s)
    arrived(lats.at[:, 0], kvp_s)
    arrived(lats.at[pl.ds(0, NZ - 1), 0, pl.ds(0, NX - 1)], kx_s)
    arrived(qall.at[pl.ds(0, NY - 1)], q_s)
    arrived(osend.at[pl.ds(1, NY - 1)], o_s)
    arrived(ssend.at[pl.ds(1, NY - 1)], st_s)
    arrived(mixed.at[pl.ds(0, NX - 1)], mx_s)
    arrived(wo.at[pl.ds(0, NX - 1), 0], wo_s)
    arrived(wo.at[pl.ds(0, NX - 1), 0], wop_s)
    arrived(resid.at[pl.ds(0, NX - 1)], re_s)
    arrived(part.at[:, pl.ds(0, NX - 1)], rs_s)

    for which in (0, 1):

        @pl.when(c == which)
        def _():
            for u in range(4):
                first_y = u in Y_FIRST[which]
                arrived(some(u, 1, NY - 1) if first_y else some(u, NZ - 1, 1), w_s1.at[u])
                arrived(some(u, NZ - 1, NY) if first_y else some(u, NZ, NY - 1), w_s2.at[u])
                arrived(some(u, NZ, NY), wp_s.at[u])

    phases.close()


def on_device(
    NZ,
    NX,
    residual,
    query_content,
    query_rotary,
    key_latent,
    rotary_key,
    latent_gain,
    key_weight,
    value_weight,
    output_gain,
    output_weight,
    mixer_gain,
    gate_weight,
    up_weight,
    down_weight,
):
    T = key_latent.shape[0]
    R, D = residual.shape
    F = gate_weight.shape[1]
    positions = lax.axis_index("sp") * T + lax.iota(jnp.int32, T)
    power = jnp.arange(0, ROT_DIM, 2, dtype=F32) / ROT_DIM
    inverse = 1.0 / jnp.power(ROPE_BASE, power)
    angles = positions.astype(F32)[None, :] * inverse[:, None]
    cos = jnp.cos(angles)
    sin = jnp.sin(angles)
    vm = pl.BlockSpec(memory_space=pltpu.VMEM)
    hbm = pl.BlockSpec(memory_space=pl.ANY)
    V = pltpu.VMEM

    def pin(a):
        return pltpu.with_memory_space_constraint(a, pltpu.HBM)

    S = pltpu.SemaphoreType.DMA
    RZ = NZ // 2
    scales = ((64 + ROT_DIM) ** -0.5,) * 2 + ((128 + ROT_DIM) ** -0.5,)
    return pl.pallas_call(
        functools.partial(kernel, NZ, NX, scales),
        out_shape=jax.ShapeDtypeStruct((R, D), BF16),
        in_specs=[vm] * 2 + [hbm] * 14,
        out_specs=vm,
        scratch_shapes=[
            V((1, output_gain.shape[0]), F32),
            V((1, D), F32),
            V((1, key_latent.shape[1]), F32),
            V((T, key_latent.shape[1]), BF16),
            V(key_weight.shape, BF16),
            V(value_weight.shape, BF16),
            V((T, 256), BF16),
            V((query_rotary.shape[1], T), BF16),
            V((ROT_DIM, T), BF16),
            V((3, NZ, NY, 2, R, F), BF16),
            V((NZ, 2, NX, T // NX, key_latent.shape[1] + 128), BF16),
            V(value_weight.shape[::-1], BF16),
            V((4 * T, 256), BF16),
            V((4 * T, 256), BF16),
            V((256, 4 * T), BF16),
            V((NY, T, 384), BF16),
            V((3, NY * T, 256), BF16),
            V((256, NY * T), F32),
            V((8, NY * T), F32),
            V((8, NY * T), F32),
            V((NY, 256, T), BF16),
            V((NY, 256, T), BF16),
            V((NY, 8, T), F32),
            V((NY, 8, T), F32),
            V((NX, T, 256), BF16),
            V((NX, 2, 128, D), BF16),
            V((NX, R, D), BF16),
            V((NZ, T, 256), BF16),
            V((NZ, T, 256), BF16),
            V((T, F), F32),
            V((T, F), F32),
            V((T, F), BF16),
            V((NZ, NX, R, 256), BF16),
            V((NX, NZ, R, 256), BF16),
            S((7,)),
            S((7,)),
            S(()),
            S((RZ + 1,)),
            S(()),
            S((RZ + 1,)),
            S(()),
            S((RZ + 1,)),
            S(()),
            S((NY // 2 + 1,)),
            S(()),
            S(()),
            S(()),
            S(()),
            S(()),
            S(()),
            S(()),
            S((NX // 2 + 1,)),
            S(()),
            S(()),
            S(()),
            S(()),
            S(()),
            S((RZ + 1,)),
            S((4,)),
            S((4,)),
            S((4,)),
            S((4, RZ + 1)),
            S((4, RZ + 1, 2)),
            S((4, RZ + 1)),
        ],
        compiler_params=pltpu.CompilerParams(
            collective_id=0, has_side_effects=True, vmem_limit_bytes=44 * 1024 * 1024
        ),
    )(
        cos,
        sin,
        pin(output_gain[None, :]),
        pin(mixer_gain[None, :]),
        pin(latent_gain[None, :]),
        pin(key_latent),
        pin(key_weight),
        pin(value_weight),
        pin(query_content),
        pin(query_rotary.T),
        pin(rotary_key.T),
        pin(residual),
        pin(output_weight.reshape(2, 128, D)),
        pin(gate_weight),
        pin(up_weight),
        pin(down_weight.T),
    )


def solution(mesh):
    placed = (
        P(("sp", "tp"), None),
        P("sp", "tp"),
        P("sp", "tp"),
        P("sp", None),
        P("sp", None),
        P(),
        P(None, "tp"),
        P(None, "tp"),
        P("tp"),
        P("tp", None),
        P(),
        P("sp", "tp"),
        P("sp", "tp"),
        P("tp", "sp"),
    )
    NZ = mesh.shape["sp"] // (2 * NY)
    NX = mesh.shape["tp"]
    return jax.shard_map(
        functools.partial(on_device, NZ, NX),
        mesh=mesh,
        in_specs=placed,
        out_specs=P(("sp", "tp"), None),
        check_vma=False,
    )
```

```python
import contextlib
import functools

import jax
import jax.numpy as jnp
from jax import lax
from jax.experimental import pallas as pl
from jax.experimental.pallas import tpu as pltpu
from jax.sharding import PartitionSpec as P

NY = 4
ROT_DIM = 32
EPS = 1e-06
ROPE_BASE = 500000.0
LOG2E = 1.4426950408889634
MESH = pl.DeviceIdType.MESH
F32 = jnp.float32
BF16 = jnp.bfloat16

Y_FIRST = ((0, 1, 2), (2,))
ZDIR = ((1, -1, -1, -1), (-1, 1, 1, -1))
PARTS = (
    "kvw1",
    "kvw2",
    "q1",
    "q2",
    "kvw3",
    "kx1",
    "att0",
    "kvw4",
    "kx2",
    "att1",
    "kx3",
    "att2",
    "kx4",
    "att3",
    "att4",
    "owait",
    "mixw",
    "widen0",
    "widen1",
    "widen2",
    "widen3",
    "widen4",
    "hid",
    "down0",
    "down1",
    "down2",
    "down3",
    "down4",
    "final",
)
PLAN = (
    (
        (("ast", 1), ("ast", 0), ("re",),),
        (("ast", 2), ("by0", 3), ("bz0", 3), ("ay", 1, 1),),
        (("ay", 0, 1), ("zz", 3, 1),),
        (("ay", 1, 2), ("az0", 1),),
        (),
        (("ay", 0, 2), ("wo0",),),
        (("az0", 0), ("ay", 2, 1),),
        (("zz", 3, 2),),
        (),
        (("ay", 2, 2), ("az0", 2),),
        (("zy", 3, 2),),
        (("az", 0, 1),),
        (("az", 2, 1),),
        (),
        (("az", 1, 1), ("wo1",),),
        (("y", 3, 0, 1), ("az", 0, 2), ("y", 3, 2, 1), ("az", 2, 2), ("az", 1, 2), ("zz", 3, 3), ("zy", 3, 3),),
        (("az", 0, 3), ("zy", 3, 1), ("az", 2, 3), ("wo2",),),
        (("az", 1, 3),),
        (("zz", 3, 4), ("zy", 3, 4),),
        (("y", 3, 1, 1),),
        (("y", 3, 3, 1),),
        (("az", 2, 4), ("az", 0, 4), ("az", 1, 4),),
        (("y", 3, 4, 1),),
        (("y", 3, 0, 2),),
        (("y", 3, 1, 2),),
        (("y", 3, 2, 2),),
        (("y", 3, 3, 2),),
        (("y", 3, 4, 2),),
        (),
    ),
    (
        (("bz0", 1), ("ast", 2), ("bz0", 3), ("re",), ("bz0", 0),),
        (("zz", 1, 1), ("zz", 3, 1), ("zy", 3, 1), ("zz", 0, 1), ("by0", 3),),
        (),
        (("zz", 1, 2), ("zy", 1, 2), ("zz", 0, 2), ("zy", 0, 1), ("zz", 3, 2), ("zy", 3, 2), ("ay", 2, 1),),
        (("zy", 1, 1),),
        (("zz", 1, 3), ("zy", 1, 3), ("y", 1, 2, 1),),
        (("by0", 0), ("zy", 0, 2), ("y", 3, 0, 1), ("by0", 1),),
        (("zz", 0, 3), ("zz", 0, 4),),
        (("y", 0, 1, 1), ("ay", 2, 2), ("az0", 2),),
        (("zz", 1, 4), ("zy", 1, 4),),
        (("wo0",), ("y", 1, 1, 1),),
        (("zy", 0, 3), ("y", 0, 0, 1), ("y", 1, 2, 2),),
        (("az", 2, 1), ("y", 3, 1, 1),),
        (("y", 1, 3, 1), ("y", 1, 0, 1), ("zy", 0, 4), ("y", 0, 2, 1), ("y", 0, 1, 2), ("y", 1, 4, 1),),
        (("y", 0, 0, 2), ("y", 0, 3, 1), ("y", 1, 3, 2), ("y", 3, 1, 2), ("wo1",),),
        (("y", 3, 2, 1), ("az", 2, 2), ("az", 2, 3), ("wo2",), ("y", 0, 4, 1), ("y", 0, 2, 2), ("y", 1, 0, 2),),
        (("y", 0, 3, 2), ("y", 1, 4, 2), ("y", 1, 1, 2), ("y", 3, 2, 2), ("zz", 3, 3), ("zy", 3, 3), ("zz", 3, 4), ("zy", 3, 4), ("y", 0, 4, 2),),
        (("y", 3, 0, 2),),
        (("az", 2, 4), ("y", 3, 3, 1),),
        (("y", 3, 4, 1),),
        (),
        (),
        (),
        (),
        (),
        (("y", 3, 3, 2),),
        (("y", 3, 4, 2),),
        (),
        (),
    ),
)


def dot(a, b):
    return lax.dot_general(a, b, (((1,), (0,)), ((), ())), preferred_element_type=F32)


def dot_nt(a, b):
    return lax.dot_general(a, b, (((1,), (1,)), ((), ())), preferred_element_type=F32)


def hops(n):
    both = list(range(1, (n - 1) // 2 + 1))
    return both, (n // 2 if n % 2 == 0 and n > 1 else None)


def kernel(
    NZ,
    NX,
    scales,
    cos_ref,
    sin_ref,
    ogain_hbm,
    mgain_hbm,
    lgain_hbm,
    lat_hbm,
    kw_hbm,
    vw_hbm,
    qc_hbm,
    qr_hbm,
    rk_hbm,
    resid_hbm,
    ow_hbm,
    gate_hbm,
    up_hbm,
    down_hbm,
    out_ref,
    ogain_ref,
    mgain_ref,
    lgain_ref,
    lat_ref,
    kw_ref,
    vw_ref,
    qc_ref,
    qr_ref,
    rk_ref,
    w,
    lats,
    vwt,
    k_narrow,
    k_wide,
    v_turned,
    qall,
    qx,
    acc,
    mrow,
    lrow,
    osend,
    orecv,
    ssend,
    srecv,
    mixed,
    wo,
    resid,
    mid,
    normed,
    accg,
    accu,
    hid,
    part,
    rsum,
    small_sem,
    loc_sem,
    kv_s,
    kv_r,
    kvp_s,
    kvp_r,
    kx_s,
    kx_r,
    q_s,
    q_r,
    o_s,
    o_r,
    st_s,
    st_r,
    mx_s,
    mx_r,
    wo_s,
    wo_r,
    wop_s,
    wop_r,
    re_s,
    re_r,
    rs_s,
    rs_r,
    w_s1,
    w_s2,
    wp_s,
    w_r1,
    w_r2,
    wp_r,
):
    sp = lax.axis_index("sp")
    x = lax.axis_index("tp")
    c = sp % 2
    y = (sp // 2) % NY
    z = sp // (2 * NY)
    T = qc_ref.shape[0]
    R = resid.shape[1]
    D = resid.shape[2]
    phases = contextlib.ExitStack()

    def phase(name):
        phases.close()
        phases.enter_context(jax.named_scope(name))

    def dev(zz=None, yy=None, cc=None, xx=None):
        zz = z if zz is None else (zz + 2 * NZ) % NZ
        yy = y if yy is None else (yy + 2 * NY) % NY
        cc = c if cc is None else cc
        xx = x if xx is None else (xx + 2 * NX) % NX
        return ((zz * NY + yy) * 2 + cc, xx)

    def send(src, dst, ssem, rsem, device):
        pltpu.make_async_remote_copy(
            src_ref=src, dst_ref=dst, send_sem=ssem, recv_sem=rsem, device_id=device, device_id_type=MESH
        ).start()

    def arrived(ref, sem):
        pltpu.make_async_copy(ref, ref, sem).wait()

    partner = dev(cc=1 - c)
    dirc = 1 - 2 * c
    zboth, zlast = hops(NZ)
    yboth, ylast = hops(NY)
    xboth, xlast = hops(NX)

    barrier = pltpu.get_barrier_semaphore()
    peers = [partner]
    peers += [dev(zz=z + 1)] + ([dev(zz=z - 1)] if NZ > 2 else [])
    peers += [dev(yy=y + k) for k in range(1, NY)]
    peers += [dev(xx=x + k) for k in range(1, NX)]
    for p in peers:
        pl.semaphore_signal(barrier, inc=1, device_id=p, device_id_type=MESH)

    small = [
        pltpu.make_async_copy(a, b, small_sem.at[k])
        for k, (a, b) in enumerate(
            [(lat_hbm, lat_ref), (lgain_hbm, lgain_ref), (kw_hbm, kw_ref), (vw_hbm, vw_ref), (qc_hbm, qc_ref), (qr_hbm, qr_ref), (rk_hbm, rk_ref)]
        )
    ]
    loc = [
        pltpu.make_async_copy(a, b, loc_sem.at[k])
        for k, (a, b) in enumerate(
            [
                (gate_hbm, w.at[0, z, y, c]),
                (up_hbm, w.at[1, z, y, c]),
                (down_hbm, w.at[2, z, y, c]),
                (ow_hbm, wo.at[x]),
                (resid_hbm, resid.at[x]),
                (ogain_hbm, ogain_ref),
                (mgain_hbm, mgain_ref),
            ]
        )
    ]
    for d in small + loc:
        d.start()
    phase("qkv")
    for d in small:
        d.wait()
    half = ROT_DIM // 2
    cos = cos_ref[...]
    sin = sin_ref[...]

    def turned(ref, count):
        rows = []
        for h in range(count):
            a = ref[h * ROT_DIM : h * ROT_DIM + half, :].astype(F32)
            b = ref[h * ROT_DIM + half : (h + 1) * ROT_DIM, :].astype(F32)
            rows += [a * cos - b * sin, b * cos + a * sin]
        return rows

    lat = lat_ref[...].astype(F32)
    lat = lat * lax.rsqrt(jnp.mean(lat * lat, axis=-1, keepdims=True) + EPS)
    lat = (lat * lgain_ref[...]).astype(BF16)
    L = lat.shape[1]
    lats[0, c, :, :, 0:L] = lat.reshape(NX, T // NX, L)
    rot = jnp.transpose(jnp.concatenate(turned(rk_ref, 1) * 4, axis=0)).astype(BF16)
    lats[0, c, :, :, L : L + 128] = rot.reshape(NX, T // NX, 128)

    turned_q = turned(qr_ref, 3) + [jnp.zeros((ROT_DIM, T), F32)]
    qall[0, :, 0:128] = qc_ref[:, 0:128]
    qall[0, :, 128:256] = jnp.transpose(jnp.concatenate(turned_q, axis=0)).astype(BF16)
    qall[0, :, 256:384] = qc_ref[:, 128:256]

    phase("barrier")
    pl.semaphore_wait(barrier, len(peers))

    def kv_copy(src_slot, dst_slot, device):
        send(lats.at[src_slot, c, x], lats.at[dst_slot, c, x], kv_s, kv_r.at[(dst_slot + 1) // 2], device)

    def kv_partner(slot):
        send(lats.at[slot, c], lats.at[slot, c], kvp_s, kvp_r.at[(slot + 1) // 2], partner)

    def kv_send(r):
        if r in zboth:
            kv_copy(2 * r - 3 if r > 1 else 0, 2 * r - 1, dev(zz=z + 1))
            kv_copy(2 * r - 2 if r > 1 else 0, 2 * r, dev(zz=z - 1))
        elif r == zlast:
            kv_copy((2 * r - 3 + c) if r > 1 else 0, NZ - 1, dev(zz=z + dirc))

    def slots_of(n, r):
        if r == 0:
            return [0]
        return [2 * r - 1, 2 * r] if r <= (n - 1) // 2 else [n - 1]

    def offset_of(n, slot):
        if slot == 0:
            return 0
        return slot_r(n, slot) if slot % 2 == 0 else -slot_r(n, slot)

    def slot_r(n, slot):
        return (slot + 1) // 2

    def zpos(slot):
        return (z + offset_of(NZ, slot) + 2 * NZ) % NZ

    def ypos(slot):
        return (y + offset_of(NY, slot) + 2 * NY) % NY

    def wo_send(r):
        if r in xboth:
            send(wo.at[(x - r + 1 + NX) % NX, c], wo.at[(x - r + 1 + NX) % NX, c], wo_s, wo_r.at[r], dev(xx=x + 1))
            send(wo.at[(x + r - 1) % NX, c], wo.at[(x + r - 1) % NX, c], wo_s, wo_r.at[r], dev(xx=x - 1))
        elif r == xlast:
            p = (x - dirc * (r - 1) + 2 * NX) % NX
            send(wo.at[p, c], wo.at[p, c], wo_s, wo_r.at[r], dev(xx=x + dirc))

    def wo_wait(r):
        arrived(wo.at[pl.ds(0, len(slots_of(NX, r))), c], wo_r.at[r])
        for slot in slots_of(NX, r):
            p = (x + offset_of(NX, slot) + 2 * NX) % NX
            send(wo.at[p, c], wo.at[p, c], wop_s, wop_r, partner)

    cut = w.shape[5] // 256 * 128
    units = ((0, 0, w.shape[5]), (1, 0, cut), (1, cut, w.shape[5]), (2, 0, w.shape[5]))
    core = [0]

    def piece(u, zz, yy, cc):
        mat, lo, hi = units[u]
        return w.at[mat, zz, yy, cc, :, lo:hi]

    def some(u, nz, ny):
        return piece(u, pl.ds(0, nz), pl.ds(0, ny), 0)

    def ring_y(u, zz, r, d, ssem, rsem):
        if r in yboth:
            a, b = (y - r + 1 + NY) % NY, (y + r - 1) % NY
            send(piece(u, zz, a, core[0]), piece(u, zz, a, core[0]), ssem, rsem, dev(yy=y + 1))
            send(piece(u, zz, b, core[0]), piece(u, zz, b, core[0]), ssem, rsem, dev(yy=y - 1))
        elif r == ylast:
            p = (y - d * (r - 1) + 2 * NY) % NY
            send(piece(u, zz, p, core[0]), piece(u, zz, p, core[0]), ssem, rsem, dev(yy=y + d))

    def ring_z(u, yy, r, ssem, rsem):
        d = ZDIR[core[0]][u]
        if r in zboth:
            a, b = (z - r + 1 + NZ) % NZ, (z + r - 1) % NZ
            send(piece(u, a, yy, core[0]), piece(u, a, yy, core[0]), ssem, rsem, dev(zz=z + 1))
            send(piece(u, b, yy, core[0]), piece(u, b, yy, core[0]), ssem, rsem, dev(zz=z - 1))
        elif r == zlast:
            p = (z - d * (r - 1) + 2 * NZ) % NZ
            send(piece(u, p, yy, core[0]), piece(u, p, yy, core[0]), ssem, rsem, dev(zz=z + d))

    every = pl.ds(0, NY)

    def a1_send(u, r):
        ring_y(u, z, r, ZDIR[core[0]][u], w_s1.at[u], w_r1.at[u, r])

    def a1_wait(u, r):
        arrived(some(u, 1, len(slots_of(NY, r))), w_r1.at[u, r])

    def a2_send(u, r):
        ring_z(u, every, r, w_s2.at[u], w_r2.at[u, r, 0])

    def a_partner(u, slot):
        p = piece(u, zpos(slot), every, core[0])
        send(p, p, wp_s.at[u], wp_r.at[u, (slot + 1) // 2], partner)

    def a2_wait(u, r):
        arrived(some(u, len(slots_of(NZ, r)), NY), w_r2.at[u, r, 0])

    def b1_send(u, r):
        ring_z(u, y, r, w_s1.at[u], w_r1.at[u, r])

    def b1_wait(u, r):
        arrived(some(u, len(slots_of(NZ, r)), 1), w_r1.at[u, r])

    def b2_send(u, slot, r):
        d = (1 - 2 * core[0]) * (1 - 2 * (slot % 2))
        ring_y(u, zpos(slot), r, d, w_s2.at[u], w_r2.at[u, (slot + 1) // 2, r - 1])

    def b_partner(u, slot, yslot):
        p = piece(u, zpos(slot), ypos(yslot), core[0])
        send(p, p, wp_s.at[u], wp_r.at[u, (slot + 1) // 2], partner)

    RZ = NZ // 2
    RY = NY // 2

    def b_first_y(m):
        b2_send(m, 0, 1)
        b_partner(m, 0, 0)

    def b_z(m, r):
        b1_wait(m, r)
        if r < RZ:
            b1_send(m, r + 1)

    def b_zy(m, r):
        for slot in slots_of(NZ, r):
            b2_send(m, slot, 1)
            b_partner(m, slot, 0)

    def b_y(m, r, k):
        arrived(some(m, len(slots_of(NZ, r)), len(slots_of(NY, k))), w_r2.at[m, r, k - 1])
        for slot in slots_of(NZ, r):
            if k < RY:
                b2_send(m, slot, k + 1)
            for yslot in slots_of(NY, k):
                b_partner(m, slot, yslot)

    def a_y(m, k):
        a1_wait(m, k)
        if k < RY:
            a1_send(m, k + 1)

    def a_z(m, r):
        a2_wait(m, r)
        if r < RZ:
            a2_send(m, r + 1)
        for slot in slots_of(NZ, r):
            a_partner(m, slot)

    def a_first_z(m):
        a2_send(m, 1)
        a_partner(m, 0)

    def resid_send():
        for k in range(1, NX):
            send(resid.at[x], resid.at[x], re_s, re_r, dev(xx=x + k))

    def wo_pass(r):
        wo_wait(r)
        if r < NX // 2:
            wo_send(r + 1)

    steps = {
        "ast": lambda m: a1_send(m, 1),
        "ay": a_y,
        "az0": a_first_z,
        "az": a_z,
        "bz0": lambda m: b1_send(m, 1),
        "by0": b_first_y,
        "zz": b_z,
        "zy": b_zy,
        "y": b_y,
        "wo0": lambda: wo_send(1),
        "wo1": lambda: wo_pass(1),
        "wo2": lambda: wo_pass(2),
        "re": resid_send,
    }

    def on(which, *todo):
        def run():
            core[0] = which
            for f, *a in todo:
                steps[f](*a)

        pl.when(c == which)(run)

    def gap(name):
        phase("g_" + name)
        at = PARTS.index(name)
        for which in (0, 1):
            if PLAN[which][at]:
                on(which, *PLAN[which][at])

    phase("send0")

    def q_send(r):
        if r in yboth:
            left = 0 if r == 1 else offset_of(NY, 2 * r - 3) % NY
            right = 0 if r == 1 else offset_of(NY, 2 * r - 2) % NY
            send(qall.at[left], qall.at[(-r) % NY], q_s, q_r.at[r], dev(yy=y + 1))
            send(qall.at[right], qall.at[r], q_s, q_r.at[r], dev(yy=y - 1))
        elif r == ylast:
            member = 0 if r == 1 else (-dirc * (r - 1) + NY) % NY
            send(qall.at[member], qall.at[r], q_s, q_r.at[r], dev(yy=y + dirc))

    kv_send(1)
    kv_partner(0)
    q_send(1)
    for d in loc:
        d.wait()

    lane = lax.broadcasted_iota(jnp.int32, (T, 256), 1)
    own0 = (lane < 64) | ((lane >= 128) & (lane < 160))
    own1 = ((lane >= 64) & (lane < 128)) | ((lane >= 160) & (lane < 192))
    own2 = ((lane >= 64) & (lane < 96)) | (lane >= 128)

    def spread(k):
        narrow = qall[k, :, 0:256]
        wide = qall[k, :, 128:384]
        zero = jnp.zeros_like(narrow)
        qx[0, k * T : (k + 1) * T, :] = jnp.where(own0, narrow, zero)
        qx[1, k * T : (k + 1) * T, :] = jnp.where(own1, narrow, zero)
        qx[2, k * T : (k + 1) * T, :] = jnp.where(own2, wide, zero)

    def kv_wait(r):
        phase(f"kvw#r={r}")
        ring = slots_of(NZ, r)
        arrived(lats.at[pl.ds(ring[0], len(ring)), c, 0], kv_r.at[r])
        if r < RZ:
            kv_send(r + 1)
        for slot in ring:
            for k in range(1, NX):
                send(lats.at[slot, c, x], lats.at[slot, c, x], kx_s, kx_r.at[r], dev(xx=x + k))

    def kx_wait(r):
        phase(f"kx#r={r}")
        ring = slots_of(NZ, r)
        arrived(lats.at[pl.ds(ring[0], len(ring)), c, pl.ds(0, NX - 1)], kx_r.at[r])
        for slot in ring:
            kv_partner(slot)

    phase("spread0")
    vwt[...] = jnp.transpose(vw_ref[...].astype(F32)).astype(BF16)
    spread(0)
    mrow[...] = jnp.full_like(mrow, -1e30)
    lrow[...] = jnp.zeros_like(lrow)
    acc[...] = jnp.zeros_like(acc)
    accg[...] = jnp.zeros_like(accg)
    accu[...] = jnp.zeros_like(accu)
    def q_wait(r):
        phase(f"qw#r={r}")
        arrived(qall.at[pl.ds(0, len(slots_of(NY, r)))], q_r.at[r])
        if r < RY:
            q_send(r + 1)
        for slot in slots_of(NY, r):
            spread(offset_of(NY, slot) % NY)

    QB = min(256, NY * T)
    head_rows = ((0, 64), (64, 128), (128, 256))

    def attend(first, count):
        nk = count * 2 * T
        lat = lats[first : first + count, :, :, :, 0:L].reshape(nk, L)
        rot = lats[first : first + count, :, :, :, L : L + 128].reshape(nk, 128)
        keys = dot(lat, kw_ref[...]).astype(BF16)
        k_narrow[0:nk, 0:128] = keys[:, 0:128]
        k_narrow[0:nk, 128:256] = rot
        k_wide[0:nk, 0:128] = rot
        k_wide[0:nk, 128:256] = keys[:, 128:256]
        v_turned[:, 0:nk] = dot_nt(vwt[...], lat).astype(BF16)

        def block(b, carry):
            cols = pl.ds(pl.multiple_of(b * QB, QB), QB)
            for h in range(3):
                s = dot_nt((k_narrow if h < 2 else k_wide)[0:nk, :], qx[h, cols, :]) * (scales[h] * LOG2E)
                old = mrow[h : h + 1, cols]
                new = jnp.maximum(old, jnp.max(s, axis=0, keepdims=True))
                shrink = jnp.exp2(old - new)
                p = jnp.exp2(s - new)
                lrow[h : h + 1, cols] = lrow[h : h + 1, cols] * shrink + jnp.sum(p, axis=0, keepdims=True)
                mrow[h : h + 1, cols] = new
                r0, r1 = head_rows[h]
                acc[r0:r1, cols] = acc[r0:r1, cols] * shrink + dot(v_turned[r0:r1, 0:nk], p.astype(BF16))
            return carry

        lax.fori_loop(0, NY * T // QB, block, 0, unroll=True)

    def att(r):
        phase(f"attw#r={r}")
        ring = slots_of(NZ, r)
        arrived(lats.at[pl.ds(ring[0], len(ring)), 1 - c], kvp_r.at[r])
        phase(f"att#r={r}")
        attend(ring[0], len(ring))

    do = {"kvw": kv_wait, "kx": kx_wait, "q": q_wait, "att": att}
    for name in PARTS[: PARTS.index("owait")]:
        gap(name)
        do[name[:-1]](int(name[-1]))

    phase("osend")
    for k in range(NY):
        cols = slice(k * T, (k + 1) * T)
        osend[k] = acc[:, cols].astype(BF16)
        ssend[k, 0:3] = mrow[0:3, cols]
        ssend[k, 3:6] = lrow[0:3, cols]
        ssend[k, 6:8] = jnp.zeros((2, T), F32)
    for k in range(1, NY):
        send(osend.at[k], orecv.at[NY - k], o_s, o_r, dev(yy=y + k))
        send(ssend.at[k], srecv.at[NY - k], st_s, st_r, dev(yy=y + k))
    gap("owait")
    phase("owait")
    arrived(orecv.at[pl.ds(1, NY - 1)], o_r)
    arrived(srecv.at[pl.ds(1, NY - 1)], st_r)
    phase("merge")
    ms = [ssend[0, 0:3]] + [srecv[k, 0:3] for k in range(1, NY)]
    ls = [ssend[0, 3:6]] + [srecv[k, 3:6] for k in range(1, NY)]
    top = functools.reduce(jnp.maximum, ms)
    ws = [jnp.exp2(m - top) for m in ms]
    total = sum(a * b for a, b in zip(ws, ls))
    outs = []
    for h in range(3):
        r0, r1 = head_rows[h]
        o = acc[r0:r1, 0:T] * ws[0][h : h + 1]
        for k in range(1, NY):
            o = o + orecv[k, r0:r1].astype(F32) * ws[k][h : h + 1]
        o = o / total[h : h + 1]
        outs.append(o * lax.rsqrt(jnp.mean(o * o, axis=0, keepdims=True) + EPS))
    heads = jnp.transpose(jnp.concatenate(outs, axis=0))
    mixed[x] = (heads * ogain_ref[...]).astype(BF16)
    for k in range(1, NX):
        send(mixed.at[x], mixed.at[x], mx_s, mx_r, dev(xx=x + k))
    gap("mixw")
    phase("mixw")
    arrived(mixed.at[pl.ds(0, NX - 1)], mx_r)
    arrived(resid.at[pl.ds(0, NX - 1)], re_r)
    arrived(wo.at[pl.ds(0, NX - 1), 0], wop_r)
    phase("proj")
    mixed_all = jnp.concatenate([mixed[k] for k in range(NX)], axis=1)

    def project(n, squares):
        cols = pl.ds(pl.multiple_of(n * 256, 256), 256)
        s = dot(mixed_all, wo[:, :, :, cols].reshape(NX * 256, 256))
        s = (s + resid[:, :, cols].reshape(T, 256).astype(F32)).astype(BF16)
        mid[n] = s
        s = s.astype(F32)
        return squares + s * s

    squares = lax.fori_loop(0, D // 256, project, jnp.zeros((T, 256), F32), unroll=4)
    factor = lax.rsqrt(jnp.sum(squares, axis=1, keepdims=True) / D + EPS)

    def scale(n, carry):
        cols = pl.ds(pl.multiple_of(n * 256, 256), 256)
        normed[n] = (mid[n].astype(F32) * factor * mgain_ref[:, cols]).astype(BF16)
        return carry

    lax.fori_loop(0, D // 256, scale, 0, unroll=4)

    phase("mlp0")
    def from_partner(u, r):
        arrived(some(u, len(slots_of(NZ, r)), NY), wp_r.at[u, r])

    F = accg.shape[1]

    def widen(k):
        for u in range(3):
            from_partner(u, k)
        ring = slots_of(NZ, k)

        def one(i, carry):
            step = 0 if k == 0 else (k if len(ring) == 1 else (2 * i - 1) * k)
            p = (z + step + 2 * NZ) % NZ
            n = normed[p]
            accg[...] += dot(n, w[0, p].reshape(256, F))
            accu[...] += dot(n, w[1, p].reshape(256, F))
            return carry

        lax.fori_loop(0, len(ring), one, 0, unroll=True)

    for r in range(RZ + 1):
        gap(f"widen{r}")
        phase(f"widen#r={r}")
        widen(r)
    gap("hid")
    phase("hid")
    g = accg[...]
    hid[...] = (g / (1.0 + jnp.exp(-g)) * accu[...]).astype(BF16)

    def narrow(slot, carry):
        p = (z + ((slot + 1) // 2) * (1 - 2 * (slot % 2)) + 2 * NZ) % NZ
        s = dot_nt(hid[...], w[2, p].reshape(256, F)).astype(BF16)
        part[slot] = s.reshape(NX, R, 256)
        return carry

    def sums_rows(r):
        ring = slots_of(NZ, r)
        return pl.ds(ring[0], len(ring))

    for r in range(RZ + 1):
        gap(f"down{r}")
        phase(f"down#r={r}")
        ring = slots_of(NZ, r)
        from_partner(3, r)
        lax.fori_loop(ring[0], ring[0] + len(ring), narrow, 0, unroll=True)
        rows = sums_rows(r)
        for k in range(1, NX):
            p = (x + k) % NX
            send(part.at[rows, p], rsum.at[NX - k, rows], rs_s, rs_r.at[r], dev(xx=x + k))
    gap("final")
    phase("final")
    for r in range(RZ + 1):
        arrived(rsum.at[pl.ds(1, NX - 1), sums_rows(r)], rs_r.at[r])
        for slot in slots_of(NZ, r):
            p = zpos(slot)
            s = part[slot, x].astype(F32)
            for k in range(1, NX):
                s = s + rsum[k, slot].astype(F32)
            s = s + mid[p, pl.ds(pl.multiple_of(x * R, R), R), :].astype(F32)
            out_ref[:, pl.ds(pl.multiple_of(p * 256, 256), 256)] = s.astype(BF16)

    phase("sendw")
    arrived(lats.at[pl.ds(0, NZ - 1), 0, 0], kv_s)
    arrived(lats.at[:, 0], kvp_s)
    arrived(lats.at[pl.ds(0, NZ - 1), 0, pl.ds(0, NX - 1)], kx_s)
    arrived(qall.at[pl.ds(0, NY - 1)], q_s)
    arrived(osend.at[pl.ds(1, NY - 1)], o_s)
    arrived(ssend.at[pl.ds(1, NY - 1)], st_s)
    arrived(mixed.at[pl.ds(0, NX - 1)], mx_s)
    arrived(wo.at[pl.ds(0, NX - 1), 0], wo_s)
    arrived(wo.at[pl.ds(0, NX - 1), 0], wop_s)
    arrived(resid.at[pl.ds(0, NX - 1)], re_s)
    arrived(part.at[:, pl.ds(0, NX - 1)], rs_s)

    for which in (0, 1):

        @pl.when(c == which)
        def _():
            for u in range(4):
                first_y = u in Y_FIRST[which]
                arrived(some(u, 1, NY - 1) if first_y else some(u, NZ - 1, 1), w_s1.at[u])
                arrived(some(u, NZ - 1, NY) if first_y else some(u, NZ, NY - 1), w_s2.at[u])
                arrived(some(u, NZ, NY), wp_s.at[u])

    phases.close()


def on_device(
    NZ,
    NX,
    residual,
    query_content,
    query_rotary,
    key_latent,
    rotary_key,
    latent_gain,
    key_weight,
    value_weight,
    output_gain,
    output_weight,
    mixer_gain,
    gate_weight,
    up_weight,
    down_weight,
):
    T = key_latent.shape[0]
    R, D = residual.shape
    F = gate_weight.shape[1]
    positions = lax.axis_index("sp") * T + lax.iota(jnp.int32, T)
    power = jnp.arange(0, ROT_DIM, 2, dtype=F32) / ROT_DIM
    inverse = 1.0 / jnp.power(ROPE_BASE, power)
    angles = positions.astype(F32)[None, :] * inverse[:, None]
    cos = jnp.cos(angles)
    sin = jnp.sin(angles)
    vm = pl.BlockSpec(memory_space=pltpu.VMEM)
    hbm = pl.BlockSpec(memory_space=pl.ANY)
    V = pltpu.VMEM

    def pin(a):
        return pltpu.with_memory_space_constraint(a, pltpu.HBM)

    S = pltpu.SemaphoreType.DMA
    RZ = NZ // 2
    scales = ((64 + ROT_DIM) ** -0.5,) * 2 + ((128 + ROT_DIM) ** -0.5,)
    return pl.pallas_call(
        functools.partial(kernel, NZ, NX, scales),
        out_shape=jax.ShapeDtypeStruct((R, D), BF16),
        in_specs=[vm] * 2 + [hbm] * 14,
        out_specs=vm,
        scratch_shapes=[
            V((1, output_gain.shape[0]), F32),
            V((1, D), F32),
            V((1, key_latent.shape[1]), F32),
            V((T, key_latent.shape[1]), BF16),
            V(key_weight.shape, BF16),
            V(value_weight.shape, BF16),
            V((T, 256), BF16),
            V((query_rotary.shape[1], T), BF16),
            V((ROT_DIM, T), BF16),
            V((3, NZ, NY, 2, R, F), BF16),
            V((NZ, 2, NX, T // NX, key_latent.shape[1] + 128), BF16),
            V(value_weight.shape[::-1], BF16),
            V((4 * T, 256), BF16),
            V((4 * T, 256), BF16),
            V((256, 4 * T), BF16),
            V((NY, T, 384), BF16),
            V((3, NY * T, 256), BF16),
            V((256, NY * T), F32),
            V((8, NY * T), F32),
            V((8, NY * T), F32),
            V((NY, 256, T), BF16),
            V((NY, 256, T), BF16),
            V((NY, 8, T), F32),
            V((NY, 8, T), F32),
            V((NX, T, 256), BF16),
            V((NX, 2, 128, D), BF16),
            V((NX, R, D), BF16),
            V((NZ, T, 256), BF16),
            V((NZ, T, 256), BF16),
            V((T, F), F32),
            V((T, F), F32),
            V((T, F), BF16),
            V((NZ, NX, R, 256), BF16),
            V((NX, NZ, R, 256), BF16),
            S((7,)),
            S((7,)),
            S(()),
            S((RZ + 1,)),
            S(()),
            S((RZ + 1,)),
            S(()),
            S((RZ + 1,)),
            S(()),
            S((NY // 2 + 1,)),
            S(()),
            S(()),
            S(()),
            S(()),
            S(()),
            S(()),
            S(()),
            S((NX // 2 + 1,)),
            S(()),
            S(()),
            S(()),
            S(()),
            S(()),
            S((RZ + 1,)),
            S((4,)),
            S((4,)),
            S((4,)),
            S((4, RZ + 1)),
            S((4, RZ + 1, 2)),
            S((4, RZ + 1)),
        ],
        compiler_params=pltpu.CompilerParams(
            collective_id=0, has_side_effects=True, vmem_limit_bytes=44 * 1024 * 1024
        ),
    )(
        cos,
        sin,
        pin(output_gain[None, :]),
        pin(mixer_gain[None, :]),
        pin(latent_gain[None, :]),
        pin(key_latent),
        pin(key_weight),
        pin(value_weight),
        pin(query_content),
        pin(query_rotary.T),
        pin(rotary_key.T),
        pin(residual),
        pin(output_weight.reshape(2, 128, D)),
        pin(gate_weight),
        pin(up_weight),
        pin(down_weight.T),
    )


def solution(mesh):
    placed = (
        P(("sp", "tp"), None),
        P("sp", "tp"),
        P("sp", "tp"),
        P("sp", None),
        P("sp", None),
        P(),
        P(None, "tp"),
        P(None, "tp"),
        P("tp"),
        P("tp", None),
        P(),
        P("sp", "tp"),
        P("sp", "tp"),
        P("tp", "sp"),
    )
    NZ = mesh.shape["sp"] // (2 * NY)
    NX = mesh.shape["tp"]
    return jax.shard_map(
        functools.partial(on_device, NZ, NX),
        mesh=mesh,
        in_specs=placed,
        out_specs=P(("sp", "tp"), None),
        check_vma=False,
    )
```

```python
import contextlib
import functools

import jax
import jax.numpy as jnp
from jax import lax
from jax.experimental import pallas as pl
from jax.experimental.pallas import tpu as pltpu
from jax.sharding import PartitionSpec as P

NY = 4
ROT_DIM = 32
EPS = 1e-06
ROPE_BASE = 500000.0
LOG2E = 1.4426950408889634
MESH = pl.DeviceIdType.MESH
F32 = jnp.float32
BF16 = jnp.bfloat16

Y_FIRST = ((0, 1, 2), (2,))
ZDIR = ((1, -1, -1, -1), (-1, 1, 1, -1))
PARTS = (
    "kvw1",
    "kvw2",
    "q1",
    "q2",
    "kvw3",
    "kx1",
    "att0",
    "kvw4",
    "kx2",
    "att1",
    "kx3",
    "att2",
    "kx4",
    "att3",
    "att4",
    "owait",
    "mixw",
    "widen0",
    "widen1",
    "widen2",
    "widen3",
    "widen4",
    "hid",
    "down0",
    "down1",
    "down2",
    "down3",
    "down4",
    "final",
)
PLAN = (
    (
        (("bz0", 3), ("re",), ("ast", 1), ("ast", 0), ("ast", 2),),
        (("by0", 3), ("zz", 3, 1), ("ay", 1, 1),),
        (("ay", 2, 1),),
        (("ay", 0, 1), ("ay", 1, 2), ("az0", 1),),
        (),
        (),
        (("ay", 0, 2), ("az0", 0),),
        (),
        (),
        (("wo0",), ("y", 3, 0, 1), ("ay", 2, 2), ("az0", 2), ("az", 1, 1),),
        (("az", 0, 1),),
        (),
        (("zy", 3, 1), ("az", 2, 1),),
        (),
        (("zz", 3, 2), ("zy", 3, 2),),
        (("wo1",), ("az", 0, 2), ("az", 2, 2), ("az", 1, 2),),
        (("y", 3, 2, 1), ("zz", 3, 3), ("zy", 3, 3), ("az", 0, 3), ("y", 3, 1, 1), ("az", 2, 3), ("wo2",),),
        (("az", 1, 3), ("y", 3, 3, 1),),
        (("y", 3, 0, 2), ("zz", 3, 4), ("zy", 3, 4),),
        (("y", 3, 1, 2),),
        (("y", 3, 2, 2),),
        (("az", 2, 4), ("az", 0, 4), ("az", 1, 4),),
        (),
        (),
        (("y", 3, 4, 1),),
        (),
        (("y", 3, 3, 2),),
        (("y", 3, 4, 2),),
        (),
    ),
    (
        (("bz0", 1), ("bz0", 3), ("re",), ("ast", 2), ("bz0", 0),),
        (("zz", 1, 1), ("zz", 3, 1), ("zy", 3, 1), ("zz", 0, 1),),
        (("ay", 2, 1),),
        (("zz", 3, 2), ("zy", 3, 2), ("zz", 0, 2), ("zy", 0, 2),),
        (("zz", 1, 2), ("zy", 1, 2), ("by0", 3),),
        (("zy", 0, 1),),
        (("zy", 1, 1),),
        (("zz", 1, 3), ("zy", 1, 3),),
        (("ay", 2, 2), ("az0", 2),),
        (("zz", 0, 3), ("zy", 0, 3),),
        (("y", 0, 2, 1), ("y", 0, 1, 1),),
        (("wo0",),),
        (("by0", 0), ("y", 3, 0, 1), ("zz", 0, 4), ("zy", 0, 4),),
        (("az", 2, 1), ("y", 0, 2, 2),),
        (("by0", 1), ("wo1",), ("zz", 1, 4), ("zy", 1, 4), ("az", 2, 2), ("y", 1, 1, 1), ("y", 1, 0, 1), ("y", 1, 3, 1), ("y", 0, 3, 1), ("y", 0, 0, 1), ("y", 0, 4, 1),),
        (("y", 3, 1, 1), ("y", 1, 4, 1), ("y", 1, 4, 2), ("y", 1, 1, 2), ("az", 2, 3), ("wo2",), ("y", 0, 3, 2),),
        (("y", 3, 0, 2), ("y", 1, 2, 1), ("y", 0, 0, 2), ("y", 3, 2, 1), ("y", 0, 1, 2), ("y", 1, 3, 2), ("zz", 3, 3), ("zy", 3, 3), ("zz", 3, 4), ("zy", 3, 4), ("y", 1, 2, 2), ("y", 1, 0, 2),),
        (("az", 2, 4), ("y", 0, 4, 2), ("y", 3, 3, 1),),
        (("y", 3, 1, 2),),
        (),
        (("y", 3, 2, 2), ("y", 3, 4, 1),),
        (),
        (),
        (),
        (),
        (("y", 3, 3, 2),),
        (("y", 3, 4, 2),),
        (),
        (),
    ),
)


def dot(a, b):
    return lax.dot_general(a, b, (((1,), (0,)), ((), ())), preferred_element_type=F32)


def dot_nt(a, b):
    return lax.dot_general(a, b, (((1,), (1,)), ((), ())), preferred_element_type=F32)


def hops(n):
    both = list(range(1, (n - 1) // 2 + 1))
    return both, (n // 2 if n % 2 == 0 and n > 1 else None)


def kernel(
    NZ,
    NX,
    scales,
    cos_ref,
    sin_ref,
    ogain_hbm,
    mgain_hbm,
    lgain_hbm,
    lat_hbm,
    kw_hbm,
    vw_hbm,
    qc_hbm,
    qr_hbm,
    rk_hbm,
    resid_hbm,
    ow_hbm,
    gate_hbm,
    up_hbm,
    down_hbm,
    out_ref,
    ogain_ref,
    mgain_ref,
    lgain_ref,
    lat_ref,
    kw_ref,
    vw_ref,
    qc_ref,
    qr_ref,
    rk_ref,
    w,
    lats,
    vwt,
    k_narrow,
    k_wide,
    v_turned,
    qall,
    qx,
    acc,
    mrow,
    lrow,
    osend,
    orecv,
    ssend,
    srecv,
    mixed,
    wo,
    resid,
    mid,
    normed,
    accg,
    accu,
    hid,
    part,
    rsum,
    small_sem,
    loc_sem,
    kv_s,
    kv_r,
    kvp_s,
    kvp_r,
    kx_s,
    kx_r,
    q_s,
    q_r,
    o_s,
    o_r,
    st_s,
    st_r,
    mx_s,
    mx_r,
    wo_s,
    wo_r,
    wop_s,
    wop_r,
    re_s,
    re_r,
    rs_s,
    rs_r,
    w_s1,
    w_s2,
    wp_s,
    w_r1,
    w_r2,
    wp_r,
):
    sp = lax.axis_index("sp")
    x = lax.axis_index("tp")
    c = sp % 2
    y = (sp // 2) % NY
    z = sp // (2 * NY)
    T = qc_ref.shape[0]
    R = resid.shape[1]
    D = resid.shape[2]
    phases = contextlib.ExitStack()

    def phase(name):
        phases.close()
        phases.enter_context(jax.named_scope(name))

    def dev(zz=None, yy=None, cc=None, xx=None):
        zz = z if zz is None else (zz + 2 * NZ) % NZ
        yy = y if yy is None else (yy + 2 * NY) % NY
        cc = c if cc is None else cc
        xx = x if xx is None else (xx + 2 * NX) % NX
        return ((zz * NY + yy) * 2 + cc, xx)

    def send(src, dst, ssem, rsem, device):
        pltpu.make_async_remote_copy(
            src_ref=src, dst_ref=dst, send_sem=ssem, recv_sem=rsem, device_id=device, device_id_type=MESH
        ).start()

    def arrived(ref, sem):
        pltpu.make_async_copy(ref, ref, sem).wait()

    partner = dev(cc=1 - c)
    dirc = 1 - 2 * c
    zboth, zlast = hops(NZ)
    yboth, ylast = hops(NY)
    xboth, xlast = hops(NX)

    barrier = pltpu.get_barrier_semaphore()
    peers = [partner]
    peers += [dev(zz=z + 1)] + ([dev(zz=z - 1)] if NZ > 2 else [])
    peers += [dev(yy=y + k) for k in range(1, NY)]
    peers += [dev(xx=x + k) for k in range(1, NX)]
    for p in peers:
        pl.semaphore_signal(barrier, inc=1, device_id=p, device_id_type=MESH)

    small = [
        pltpu.make_async_copy(a, b, small_sem.at[k])
        for k, (a, b) in enumerate(
            [(lat_hbm, lat_ref), (lgain_hbm, lgain_ref), (kw_hbm, kw_ref), (vw_hbm, vw_ref), (qc_hbm, qc_ref), (qr_hbm, qr_ref), (rk_hbm, rk_ref)]
        )
    ]
    loc = [
        pltpu.make_async_copy(a, b, loc_sem.at[k])
        for k, (a, b) in enumerate(
            [
                (gate_hbm, w.at[0, z, y, c]),
                (up_hbm, w.at[1, z, y, c]),
                (down_hbm, w.at[2, z, y, c]),
                (ow_hbm, wo.at[x]),
                (resid_hbm, resid.at[x]),
                (ogain_hbm, ogain_ref),
                (mgain_hbm, mgain_ref),
            ]
        )
    ]
    for d in small + loc:
        d.start()
    phase("qkv")
    for d in small:
        d.wait()
    half = ROT_DIM // 2
    cos = cos_ref[...]
    sin = sin_ref[...]

    def turned(ref, count):
        rows = []
        for h in range(count):
            a = ref[h * ROT_DIM : h * ROT_DIM + half, :].astype(F32)
            b = ref[h * ROT_DIM + half : (h + 1) * ROT_DIM, :].astype(F32)
            rows += [a * cos - b * sin, b * cos + a * sin]
        return rows

    lat = lat_ref[...].astype(F32)
    lat = lat * lax.rsqrt(jnp.mean(lat * lat, axis=-1, keepdims=True) + EPS)
    lat = (lat * lgain_ref[...]).astype(BF16)
    L = lat.shape[1]
    lats[0, c, :, :, 0:L] = lat.reshape(NX, T // NX, L)
    rot = jnp.transpose(jnp.concatenate(turned(rk_ref, 1) * 4, axis=0)).astype(BF16)
    lats[0, c, :, :, L : L + 128] = rot.reshape(NX, T // NX, 128)

    turned_q = turned(qr_ref, 3) + [jnp.zeros((ROT_DIM, T), F32)]
    qall[0, :, 0:128] = qc_ref[:, 0:128]
    qall[0, :, 128:256] = jnp.transpose(jnp.concatenate(turned_q, axis=0)).astype(BF16)
    qall[0, :, 256:384] = qc_ref[:, 128:256]

    phase("barrier")
    pl.semaphore_wait(barrier, len(peers))

    def kv_copy(src_slot, dst_slot, device):
        send(lats.at[src_slot, c, x], lats.at[dst_slot, c, x], kv_s, kv_r.at[(dst_slot + 1) // 2], device)

    def kv_partner(slot):
        send(lats.at[slot, c], lats.at[slot, c], kvp_s, kvp_r.at[(slot + 1) // 2], partner)

    def kv_send(r):
        if r in zboth:
            kv_copy(2 * r - 3 if r > 1 else 0, 2 * r - 1, dev(zz=z + 1))
            kv_copy(2 * r - 2 if r > 1 else 0, 2 * r, dev(zz=z - 1))
        elif r == zlast:
            kv_copy((2 * r - 3 + c) if r > 1 else 0, NZ - 1, dev(zz=z + dirc))

    def slots_of(n, r):
        if r == 0:
            return [0]
        return [2 * r - 1, 2 * r] if r <= (n - 1) // 2 else [n - 1]

    def offset_of(n, slot):
        if slot == 0:
            return 0
        return slot_r(n, slot) if slot % 2 == 0 else -slot_r(n, slot)

    def slot_r(n, slot):
        return (slot + 1) // 2

    def zpos(slot):
        return (z + offset_of(NZ, slot) + 2 * NZ) % NZ

    def ypos(slot):
        return (y + offset_of(NY, slot) + 2 * NY) % NY

    def wo_send(r):
        if r in xboth:
            send(wo.at[(x - r + 1 + NX) % NX, c], wo.at[(x - r + 1 + NX) % NX, c], wo_s, wo_r.at[r], dev(xx=x + 1))
            send(wo.at[(x + r - 1) % NX, c], wo.at[(x + r - 1) % NX, c], wo_s, wo_r.at[r], dev(xx=x - 1))
        elif r == xlast:
            p = (x - dirc * (r - 1) + 2 * NX) % NX
            send(wo.at[p, c], wo.at[p, c], wo_s, wo_r.at[r], dev(xx=x + dirc))

    def wo_wait(r):
        arrived(wo.at[pl.ds(0, len(slots_of(NX, r))), c], wo_r.at[r])
        for slot in slots_of(NX, r):
            p = (x + offset_of(NX, slot) + 2 * NX) % NX
            send(wo.at[p, c], wo.at[p, c], wop_s, wop_r, partner)

    cut = w.shape[5] // 256 * 128
    units = ((0, 0, w.shape[5]), (1, 0, cut), (1, cut, w.shape[5]), (2, 0, w.shape[5]))
    core = [0]

    def piece(u, zz, yy, cc):
        mat, lo, hi = units[u]
        return w.at[mat, zz, yy, cc, :, lo:hi]

    def some(u, nz, ny):
        return piece(u, pl.ds(0, nz), pl.ds(0, ny), 0)

    def ring_y(u, zz, r, d, ssem, rsem):
        if r in yboth:
            a, b = (y - r + 1 + NY) % NY, (y + r - 1) % NY
            send(piece(u, zz, a, core[0]), piece(u, zz, a, core[0]), ssem, rsem, dev(yy=y + 1))
            send(piece(u, zz, b, core[0]), piece(u, zz, b, core[0]), ssem, rsem, dev(yy=y - 1))
        elif r == ylast:
            p = (y - d * (r - 1) + 2 * NY) % NY
            send(piece(u, zz, p, core[0]), piece(u, zz, p, core[0]), ssem, rsem, dev(yy=y + d))

    def ring_z(u, yy, r, ssem, rsem):
        d = ZDIR[core[0]][u]
        if r in zboth:
            a, b = (z - r + 1 + NZ) % NZ, (z + r - 1) % NZ
            send(piece(u, a, yy, core[0]), piece(u, a, yy, core[0]), ssem, rsem, dev(zz=z + 1))
            send(piece(u, b, yy, core[0]), piece(u, b, yy, core[0]), ssem, rsem, dev(zz=z - 1))
        elif r == zlast:
            p = (z - d * (r - 1) + 2 * NZ) % NZ
            send(piece(u, p, yy, core[0]), piece(u, p, yy, core[0]), ssem, rsem, dev(zz=z + d))

    every = pl.ds(0, NY)

    def a1_send(u, r):
        ring_y(u, z, r, ZDIR[core[0]][u], w_s1.at[u], w_r1.at[u, r])

    def a1_wait(u, r):
        arrived(some(u, 1, len(slots_of(NY, r))), w_r1.at[u, r])

    def a2_send(u, r):
        ring_z(u, every, r, w_s2.at[u], w_r2.at[u, r, 0])

    def a_partner(u, slot):
        p = piece(u, zpos(slot), every, core[0])
        send(p, p, wp_s.at[u], wp_r.at[u, (slot + 1) // 2], partner)

    def a2_wait(u, r):
        arrived(some(u, len(slots_of(NZ, r)), NY), w_r2.at[u, r, 0])

    def b1_send(u, r):
        ring_z(u, y, r, w_s1.at[u], w_r1.at[u, r])

    def b1_wait(u, r):
        arrived(some(u, len(slots_of(NZ, r)), 1), w_r1.at[u, r])

    def b2_send(u, slot, r):
        d = (1 - 2 * core[0]) * (1 - 2 * (slot % 2))
        ring_y(u, zpos(slot), r, d, w_s2.at[u], w_r2.at[u, (slot + 1) // 2, r - 1])

    def b_partner(u, slot, yslot):
        p = piece(u, zpos(slot), ypos(yslot), core[0])
        send(p, p, wp_s.at[u], wp_r.at[u, (slot + 1) // 2], partner)

    RZ = NZ // 2
    RY = NY // 2

    def b_first_y(m):
        b2_send(m, 0, 1)
        b_partner(m, 0, 0)

    def b_z(m, r):
        b1_wait(m, r)
        if r < RZ:
            b1_send(m, r + 1)

    def b_zy(m, r):
        for slot in slots_of(NZ, r):
            b2_send(m, slot, 1)
            b_partner(m, slot, 0)

    def b_y(m, r, k):
        arrived(some(m, len(slots_of(NZ, r)), len(slots_of(NY, k))), w_r2.at[m, r, k - 1])
        for slot in slots_of(NZ, r):
            if k < RY:
                b2_send(m, slot, k + 1)
            for yslot in slots_of(NY, k):
                b_partner(m, slot, yslot)

    def a_y(m, k):
        a1_wait(m, k)
        if k < RY:
            a1_send(m, k + 1)

    def a_z(m, r):
        a2_wait(m, r)
        if r < RZ:
            a2_send(m, r + 1)
        for slot in slots_of(NZ, r):
            a_partner(m, slot)

    def a_first_z(m):
        a2_send(m, 1)
        a_partner(m, 0)

    def resid_send():
        for k in range(1, NX):
            send(resid.at[x], resid.at[x], re_s, re_r, dev(xx=x + k))

    def wo_pass(r):
        wo_wait(r)
        if r < NX // 2:
            wo_send(r + 1)

    steps = {
        "ast": lambda m: a1_send(m, 1),
        "ay": a_y,
        "az0": a_first_z,
        "az": a_z,
        "bz0": lambda m: b1_send(m, 1),
        "by0": b_first_y,
        "zz": b_z,
        "zy": b_zy,
        "y": b_y,
        "wo0": lambda: wo_send(1),
        "wo1": lambda: wo_pass(1),
        "wo2": lambda: wo_pass(2),
        "re": resid_send,
    }

    def on(which, *todo):
        def run():
            core[0] = which
            for f, *a in todo:
                steps[f](*a)

        pl.when(c == which)(run)

    def gap(name):
        phase("g_" + name)
        at = PARTS.index(name)
        for which in (0, 1):
            if PLAN[which][at]:
                on(which, *PLAN[which][at])

    phase("send0")

    def q_send(r):
        if r in yboth:
            left = 0 if r == 1 else offset_of(NY, 2 * r - 3) % NY
            right = 0 if r == 1 else offset_of(NY, 2 * r - 2) % NY
            send(qall.at[left], qall.at[(-r) % NY], q_s, q_r.at[r], dev(yy=y + 1))
            send(qall.at[right], qall.at[r], q_s, q_r.at[r], dev(yy=y - 1))
        elif r == ylast:
            member = 0 if r == 1 else (-dirc * (r - 1) + NY) % NY
            send(qall.at[member], qall.at[r], q_s, q_r.at[r], dev(yy=y + dirc))

    kv_send(1)
    kv_partner(0)
    q_send(1)
    for d in loc:
        d.wait()

    lane = lax.broadcasted_iota(jnp.int32, (T, 256), 1)
    own0 = (lane < 64) | ((lane >= 128) & (lane < 160))
    own1 = ((lane >= 64) & (lane < 128)) | ((lane >= 160) & (lane < 192))
    own2 = ((lane >= 64) & (lane < 96)) | (lane >= 128)

    def spread(k):
        narrow = qall[k, :, 0:256]
        wide = qall[k, :, 128:384]
        zero = jnp.zeros_like(narrow)
        qx[0, k * T : (k + 1) * T, :] = jnp.where(own0, narrow, zero)
        qx[1, k * T : (k + 1) * T, :] = jnp.where(own1, narrow, zero)
        qx[2, k * T : (k + 1) * T, :] = jnp.where(own2, wide, zero)

    def kv_wait(r):
        phase(f"kvw#r={r}")
        ring = slots_of(NZ, r)
        arrived(lats.at[pl.ds(ring[0], len(ring)), c, 0], kv_r.at[r])
        if r < RZ:
            kv_send(r + 1)
        for slot in ring:
            for k in range(1, NX):
                send(lats.at[slot, c, x], lats.at[slot, c, x], kx_s, kx_r.at[r], dev(xx=x + k))

    def kx_wait(r):
        phase(f"kx#r={r}")
        ring = slots_of(NZ, r)
        arrived(lats.at[pl.ds(ring[0], len(ring)), c, pl.ds(0, NX - 1)], kx_r.at[r])
        for slot in ring:
            kv_partner(slot)

    phase("spread0")
    vwt[...] = jnp.transpose(vw_ref[...].astype(F32)).astype(BF16)
    spread(0)
    mrow[...] = jnp.full_like(mrow, -1e30)
    lrow[...] = jnp.zeros_like(lrow)
    acc[...] = jnp.zeros_like(acc)
    accg[...] = jnp.zeros_like(accg)
    accu[...] = jnp.zeros_like(accu)
    def q_wait(r):
        phase(f"qw#r={r}")
        arrived(qall.at[pl.ds(0, len(slots_of(NY, r)))], q_r.at[r])
        if r < RY:
            q_send(r + 1)
        for slot in slots_of(NY, r):
            spread(offset_of(NY, slot) % NY)

    QB = min(256, NY * T)
    head_rows = ((0, 64), (64, 128), (128, 256))

    def attend(first, count):
        nk = count * 2 * T
        lat = lats[first : first + count, :, :, :, 0:L].reshape(nk, L)
        rot = lats[first : first + count, :, :, :, L : L + 128].reshape(nk, 128)
        keys = dot(lat, kw_ref[...]).astype(BF16)
        k_narrow[0:nk, 0:128] = keys[:, 0:128]
        k_narrow[0:nk, 128:256] = rot
        k_wide[0:nk, 0:128] = rot
        k_wide[0:nk, 128:256] = keys[:, 128:256]
        v_turned[:, 0:nk] = dot_nt(vwt[...], lat).astype(BF16)

        def block(b, carry):
            cols = pl.ds(pl.multiple_of(b * QB, QB), QB)
            for h in range(3):
                s = dot_nt((k_narrow if h < 2 else k_wide)[0:nk, :], qx[h, cols, :]) * (scales[h] * LOG2E)
                old = mrow[h : h + 1, cols]
                new = jnp.maximum(old, jnp.max(s, axis=0, keepdims=True))
                shrink = jnp.exp2(old - new)
                p = jnp.exp2(s - new)
                lrow[h : h + 1, cols] = lrow[h : h + 1, cols] * shrink + jnp.sum(p, axis=0, keepdims=True)
                mrow[h : h + 1, cols] = new
                r0, r1 = head_rows[h]
                acc[r0:r1, cols] = acc[r0:r1, cols] * shrink + dot(v_turned[r0:r1, 0:nk], p.astype(BF16))
            return carry

        lax.fori_loop(0, NY * T // QB, block, 0, unroll=True)

    def att(r):
        phase(f"attw#r={r}")
        ring = slots_of(NZ, r)
        arrived(lats.at[pl.ds(ring[0], len(ring)), 1 - c], kvp_r.at[r])
        phase(f"att#r={r}")
        attend(ring[0], len(ring))

    do = {"kvw": kv_wait, "kx": kx_wait, "q": q_wait, "att": att}
    for name in PARTS[: PARTS.index("owait")]:
        gap(name)
        do[name[:-1]](int(name[-1]))

    phase("osend")
    for k in range(NY):
        cols = slice(k * T, (k + 1) * T)
        osend[k] = acc[:, cols].astype(BF16)
        ssend[k, 0:3] = mrow[0:3, cols]
        ssend[k, 3:6] = lrow[0:3, cols]
        ssend[k, 6:8] = jnp.zeros((2, T), F32)
    for k in range(1, NY):
        send(osend.at[k], orecv.at[NY - k], o_s, o_r, dev(yy=y + k))
        send(ssend.at[k], srecv.at[NY - k], st_s, st_r, dev(yy=y + k))
    gap("owait")
    phase("owait")
    arrived(orecv.at[pl.ds(1, NY - 1)], o_r)
    arrived(srecv.at[pl.ds(1, NY - 1)], st_r)
    phase("merge")
    ms = [ssend[0, 0:3]] + [srecv[k, 0:3] for k in range(1, NY)]
    ls = [ssend[0, 3:6]] + [srecv[k, 3:6] for k in range(1, NY)]
    top = functools.reduce(jnp.maximum, ms)
    ws = [jnp.exp2(m - top) for m in ms]
    total = sum(a * b for a, b in zip(ws, ls))
    outs = []
    for h in range(3):
        r0, r1 = head_rows[h]
        o = acc[r0:r1, 0:T] * ws[0][h : h + 1]
        for k in range(1, NY):
            o = o + orecv[k, r0:r1].astype(F32) * ws[k][h : h + 1]
        o = o / total[h : h + 1]
        outs.append(o * lax.rsqrt(jnp.mean(o * o, axis=0, keepdims=True) + EPS))
    heads = jnp.transpose(jnp.concatenate(outs, axis=0))
    mixed[x] = (heads * ogain_ref[...]).astype(BF16)
    for k in range(1, NX):
        send(mixed.at[x], mixed.at[x], mx_s, mx_r, dev(xx=x + k))
    gap("mixw")
    phase("mixw")
    arrived(mixed.at[pl.ds(0, NX - 1)], mx_r)
    arrived(resid.at[pl.ds(0, NX - 1)], re_r)
    arrived(wo.at[pl.ds(0, NX - 1), 0], wop_r)
    phase("proj")
    mixed_all = jnp.concatenate([mixed[k] for k in range(NX)], axis=1)

    def project(n, squares):
        cols = pl.ds(pl.multiple_of(n * 256, 256), 256)
        s = dot(mixed_all, wo[:, :, :, cols].reshape(NX * 256, 256))
        s = (s + resid[:, :, cols].reshape(T, 256).astype(F32)).astype(BF16)
        mid[n] = s
        s = s.astype(F32)
        return squares + s * s

    squares = lax.fori_loop(0, D // 256, project, jnp.zeros((T, 256), F32), unroll=4)
    factor = lax.rsqrt(jnp.sum(squares, axis=1, keepdims=True) / D + EPS)

    def scale(n, carry):
        cols = pl.ds(pl.multiple_of(n * 256, 256), 256)
        normed[n] = (mid[n].astype(F32) * factor * mgain_ref[:, cols]).astype(BF16)
        return carry

    lax.fori_loop(0, D // 256, scale, 0, unroll=4)

    phase("mlp0")
    def from_partner(u, r):
        arrived(some(u, len(slots_of(NZ, r)), NY), wp_r.at[u, r])

    F = accg.shape[1]

    def widen(k):
        for u in range(3):
            from_partner(u, k)
        ring = slots_of(NZ, k)

        def one(i, carry):
            step = 0 if k == 0 else (k if len(ring) == 1 else (2 * i - 1) * k)
            p = (z + step + 2 * NZ) % NZ
            n = normed[p]
            accg[...] += dot(n, w[0, p].reshape(256, F))
            accu[...] += dot(n, w[1, p].reshape(256, F))
            return carry

        lax.fori_loop(0, len(ring), one, 0, unroll=True)

    for r in range(RZ + 1):
        gap(f"widen{r}")
        phase(f"widen#r={r}")
        widen(r)
    gap("hid")
    phase("hid")
    g = accg[...]
    hid[...] = (g / (1.0 + jnp.exp(-g)) * accu[...]).astype(BF16)

    def narrow(slot, carry):
        p = (z + ((slot + 1) // 2) * (1 - 2 * (slot % 2)) + 2 * NZ) % NZ
        s = dot_nt(hid[...], w[2, p].reshape(256, F)).astype(BF16)
        part[slot] = s.reshape(NX, R, 256)
        return carry

    def sums_rows(r):
        ring = slots_of(NZ, r)
        return pl.ds(ring[0], len(ring))

    for r in range(RZ + 1):
        gap(f"down{r}")
        phase(f"down#r={r}")
        ring = slots_of(NZ, r)
        from_partner(3, r)
        lax.fori_loop(ring[0], ring[0] + len(ring), narrow, 0, unroll=True)
        rows = sums_rows(r)
        for k in range(1, NX):
            p = (x + k) % NX
            send(part.at[rows, p], rsum.at[NX - k, rows], rs_s, rs_r.at[r], dev(xx=x + k))
    gap("final")
    phase("final")
    for r in range(RZ + 1):
        arrived(rsum.at[pl.ds(1, NX - 1), sums_rows(r)], rs_r.at[r])
        for slot in slots_of(NZ, r):
            p = zpos(slot)
            s = part[slot, x].astype(F32)
            for k in range(1, NX):
                s = s + rsum[k, slot].astype(F32)
            s = s + mid[p, pl.ds(pl.multiple_of(x * R, R), R), :].astype(F32)
            out_ref[:, pl.ds(pl.multiple_of(p * 256, 256), 256)] = s.astype(BF16)

    phase("sendw")
    arrived(lats.at[pl.ds(0, NZ - 1), 0, 0], kv_s)
    arrived(lats.at[:, 0], kvp_s)
    arrived(lats.at[pl.ds(0, NZ - 1), 0, pl.ds(0, NX - 1)], kx_s)
    arrived(qall.at[pl.ds(0, NY - 1)], q_s)
    arrived(osend.at[pl.ds(1, NY - 1)], o_s)
    arrived(ssend.at[pl.ds(1, NY - 1)], st_s)
    arrived(mixed.at[pl.ds(0, NX - 1)], mx_s)
    arrived(wo.at[pl.ds(0, NX - 1), 0], wo_s)
    arrived(wo.at[pl.ds(0, NX - 1), 0], wop_s)
    arrived(resid.at[pl.ds(0, NX - 1)], re_s)
    arrived(part.at[:, pl.ds(0, NX - 1)], rs_s)

    for which in (0, 1):

        @pl.when(c == which)
        def _():
            for u in range(4):
                first_y = u in Y_FIRST[which]
                arrived(some(u, 1, NY - 1) if first_y else some(u, NZ - 1, 1), w_s1.at[u])
                arrived(some(u, NZ - 1, NY) if first_y else some(u, NZ, NY - 1), w_s2.at[u])
                arrived(some(u, NZ, NY), wp_s.at[u])

    phases.close()


def on_device(
    NZ,
    NX,
    residual,
    query_content,
    query_rotary,
    key_latent,
    rotary_key,
    latent_gain,
    key_weight,
    value_weight,
    output_gain,
    output_weight,
    mixer_gain,
    gate_weight,
    up_weight,
    down_weight,
):
    T = key_latent.shape[0]
    R, D = residual.shape
    F = gate_weight.shape[1]
    positions = lax.axis_index("sp") * T + lax.iota(jnp.int32, T)
    power = jnp.arange(0, ROT_DIM, 2, dtype=F32) / ROT_DIM
    inverse = 1.0 / jnp.power(ROPE_BASE, power)
    angles = positions.astype(F32)[None, :] * inverse[:, None]
    cos = jnp.cos(angles)
    sin = jnp.sin(angles)
    vm = pl.BlockSpec(memory_space=pltpu.VMEM)
    hbm = pl.BlockSpec(memory_space=pl.ANY)
    V = pltpu.VMEM

    def pin(a):
        return pltpu.with_memory_space_constraint(a, pltpu.HBM)

    S = pltpu.SemaphoreType.DMA
    RZ = NZ // 2
    scales = ((64 + ROT_DIM) ** -0.5,) * 2 + ((128 + ROT_DIM) ** -0.5,)
    return pl.pallas_call(
        functools.partial(kernel, NZ, NX, scales),
        out_shape=jax.ShapeDtypeStruct((R, D), BF16),
        in_specs=[vm] * 2 + [hbm] * 14,
        out_specs=vm,
        scratch_shapes=[
            V((1, output_gain.shape[0]), F32),
            V((1, D), F32),
            V((1, key_latent.shape[1]), F32),
            V((T, key_latent.shape[1]), BF16),
            V(key_weight.shape, BF16),
            V(value_weight.shape, BF16),
            V((T, 256), BF16),
            V((query_rotary.shape[1], T), BF16),
            V((ROT_DIM, T), BF16),
            V((3, NZ, NY, 2, R, F), BF16),
            V((NZ, 2, NX, T // NX, key_latent.shape[1] + 128), BF16),
            V(value_weight.shape[::-1], BF16),
            V((4 * T, 256), BF16),
            V((4 * T, 256), BF16),
            V((256, 4 * T), BF16),
            V((NY, T, 384), BF16),
            V((3, NY * T, 256), BF16),
            V((256, NY * T), F32),
            V((8, NY * T), F32),
            V((8, NY * T), F32),
            V((NY, 256, T), BF16),
            V((NY, 256, T), BF16),
            V((NY, 8, T), F32),
            V((NY, 8, T), F32),
            V((NX, T, 256), BF16),
            V((NX, 2, 128, D), BF16),
            V((NX, R, D), BF16),
            V((NZ, T, 256), BF16),
            V((NZ, T, 256), BF16),
            V((T, F), F32),
            V((T, F), F32),
            V((T, F), BF16),
            V((NZ, NX, R, 256), BF16),
            V((NX, NZ, R, 256), BF16),
            S((7,)),
            S((7,)),
            S(()),
            S((RZ + 1,)),
            S(()),
            S((RZ + 1,)),
            S(()),
            S((RZ + 1,)),
            S(()),
            S((NY // 2 + 1,)),
            S(()),
            S(()),
            S(()),
            S(()),
            S(()),
            S(()),
            S(()),
            S((NX // 2 + 1,)),
            S(()),
            S(()),
            S(()),
            S(()),
            S(()),
            S((RZ + 1,)),
            S((4,)),
            S((4,)),
            S((4,)),
            S((4, RZ + 1)),
            S((4, RZ + 1, 2)),
            S((4, RZ + 1)),
        ],
        compiler_params=pltpu.CompilerParams(
            collective_id=0, has_side_effects=True, vmem_limit_bytes=44 * 1024 * 1024
        ),
    )(
        cos,
        sin,
        pin(output_gain[None, :]),
        pin(mixer_gain[None, :]),
        pin(latent_gain[None, :]),
        pin(key_latent),
        pin(key_weight),
        pin(value_weight),
        pin(query_content),
        pin(query_rotary.T),
        pin(rotary_key.T),
        pin(residual),
        pin(output_weight.reshape(2, 128, D)),
        pin(gate_weight),
        pin(up_weight),
        pin(down_weight.T),
    )


def solution(mesh):
    placed = (
        P(("sp", "tp"), None),
        P("sp", "tp"),
        P("sp", "tp"),
        P("sp", None),
        P("sp", None),
        P(),
        P(None, "tp"),
        P(None, "tp"),
        P("tp"),
        P("tp", None),
        P(),
        P("sp", "tp"),
        P("sp", "tp"),
        P("tp", "sp"),
    )
    NZ = mesh.shape["sp"] // (2 * NY)
    NX = mesh.shape["tp"]
    return jax.shard_map(
        functools.partial(on_device, NZ, NX),
        mesh=mesh,
        in_specs=placed,
        out_specs=P(("sp", "tp"), None),
        check_vma=False,
    )
```
